32 devices in a mesh: sp: 8 (over z, y), tp: 4 (over x, core).
Axes of the slice: x: 2, y: 2, z: 4, core: 2. Of those that a mesh axis runs over, the one named last changes fastest.
Arguments:
- queries: bfloat16 [6144, 1024], P('sp', 'tp'), may hold values from -8 to 8
- keys: bfloat16 [6144, 256], P('sp', 'tp'), may hold values from -8 to 8
- values: bfloat16 [6144, 256], P('sp', 'tp'), may hold values from -18 to 18
- query_gain: float32 [64], replicated, may hold values from 0.4 to 5.5
- key_gain: float32 [64], replicated, may hold values from 0.4 to 5.5
- sink_logits: float32 [16], P('tp'), may hold values from 2 to 5
- out_weight: bfloat16 [1024, 2048], P('tp'), may hold values from -0.1875 to 0.1875
- residual: bfloat16 [6144, 2048], P('sp', 'tp'), may hold values from -21 to 21
- norm_gain: float32 [2048], P('tp'), may hold values from 0.1 to 1.9
- gate_weight: bfloat16 [2048, 5632], P('sp', 'tp'), may hold values from -0.125 to 0.125
- up_weight: bfloat16 [2048, 5632], P('sp', 'tp'), may hold values from -0.125 to 0.125
- down_weight: bfloat16 [5632, 2048], P('tp', 'sp'), may hold values from -0.078125 to 0.078125
Outputs:
- layer_out: bfloat16 [6144, 2048], P('sp', 'tp')
The draws below stay inside these ranges and needn't reach their ends.
All inputs are finite; a program needn't handle non-finite values.
Results may differ from the reference program's by a relative error of at most 0.0095.
The reference program's roundings to bfloat16 on the way count: a program that leaves them out, or rounds other values in their place, can miss the bound.
Values may be sent and summed in bfloat16 or wider, within the bound.
A program may use at most 192 MiB of HBM per device.

```python
import jax
import jax.numpy as jnp
from jax import lax

D = 2048
FF = 5632
HEAD_DIM = 64
Q_HEADS = 16
KV_HEADS = 4
WINDOW = 128
TOKENS = 6144
N_TP = 4


def shared_fields(key):
    key_rows = jnp.clip(jax.random.normal(jax.random.fold_in(key, 101), (TOKENS, KV_HEADS * HEAD_DIM), jnp.float32), -6.0, 6.0)
    query_rows = jnp.clip(jax.random.normal(jax.random.fold_in(key, 102), (TOKENS, Q_HEADS * HEAD_DIM), jnp.float32), -6.0, 6.0)
    return (key_rows, query_rows)


def draw_keys(key, part):
    return shared_fields(key)[0].astype(jnp.bfloat16)


def draw_queries(key, part):
    return shared_fields(key)[1].astype(jnp.bfloat16)


def gain_draw(key):
    return 1.0 + 0.18 * jnp.clip(jax.random.normal(key, (HEAD_DIM,), jnp.float32), -3.0, 3.0)


def draw_query_gain(key, part):
    return gain_draw(jax.random.fold_in(key, 104))


def draw_key_gain(key, part):
    return gain_draw(jax.random.fold_in(key, 105))


def draw_residual(key, part):
    columns = jnp.arange(D).astype(jnp.float32)
    col_scale = 3.0 ** (columns / (D - 1))
    base = jnp.clip(jax.random.normal(jax.random.fold_in(key, 106), (TOKENS, D), jnp.float32), -6.0, 6.0)
    return (base * col_scale).astype(jnp.bfloat16)


def shard_levels(own_key, shape, pieces, low, top_value):
    factor_of, own = 1.0, jax.random.fold_in(own_key, 6)
    for dim, blocks in pieces:
        steps = jnp.exp(jax.random.uniform(jax.random.fold_in(own, dim), (blocks,), jnp.float32, low / len(pieces), top_value / len(pieces)))
        factor_of = factor_of * jnp.repeat(steps, shape[dim] // blocks).reshape([-1 if axis == dim else 1 for axis in range(len(shape))])
    return factor_of


def bell_draw(own_key, extent, scale, reach, pieces=(), kind=jnp.bfloat16):
    result = jax.random.normal(own_key, extent, jnp.float32) * scale
    if len(pieces) > 0:
        result = shard_levels(own_key, extent, pieces, -0.22, 0.18) * result
    return jnp.clip(result, min=-reach, max=reach).astype(kind)


def setup_inputs(seed: int = 0) -> dict:
    splits = jax.random.split(jax.random.key(seed), 13)
    return {
        "queries": draw_queries(jax.random.fold_in(splits[12], 71), 0),
        "keys": draw_keys(jax.random.fold_in(splits[12], 71), 0),
        "values": bell_draw(splits[2], (TOKENS, KV_HEADS * HEAD_DIM), 3.0, 18.0, ((0, 8), (1, 4))),
        "query_gain": draw_query_gain(jax.random.fold_in(splits[12], 71), 0),
        "key_gain": draw_key_gain(jax.random.fold_in(splits[12], 71), 0),
        "sink_logits": jnp.clip(2.0 + 3.0 * jax.random.uniform(splits[5], (Q_HEADS,), jnp.float32) ** shard_levels(splits[5], (Q_HEADS,), ((0, 4),), -0.2, 0.2), 2.0, 5.0),
        "out_weight": bell_draw(splits[6], (Q_HEADS * HEAD_DIM, D), (Q_HEADS * HEAD_DIM) ** -0.5, 0.1875, ((0, 4),)),
        "residual": draw_residual(jax.random.fold_in(splits[12], 71), 0),
        "norm_gain": jnp.clip(1.0 + 0.18 * jax.random.normal(splits[8], (D,), jnp.float32), 0.1, 1.9),
        "gate_weight": bell_draw(splits[9], (D, FF), D ** -0.5, 0.125, ((0, 8), (1, 4))),
        "up_weight": bell_draw(splits[10], (D, FF), D ** -0.5, 0.125, ((0, 8), (1, 4))),
        "down_weight": bell_draw(splits[11], (FF, D), FF ** -0.5, 0.078125, ((0, 4), (1, 8))),
    }


def norm_heads(flat, gain, heads):
    row_count = flat.shape[0]
    head_width = gain.shape[0]
    data = flat.astype(jnp.float32).reshape(row_count, heads, head_width)
    scaled = data * lax.rsqrt(lax.optimization_barrier(jnp.mean(data * data, axis=-1, keepdims=True)) + 1e-06) * gain
    return scaled.astype(jnp.bfloat16)

def reference(queries, keys, values, query_gain, key_gain, sink_logits, out_weight, residual, norm_gain, gate_weight, up_weight, down_weight):
    seq_len = queries.shape[0]
    group_size = Q_HEADS // KV_HEADS
    block_count = seq_len // WINDOW
    query_heads = norm_heads(queries, query_gain, Q_HEADS).reshape(seq_len, KV_HEADS, group_size, HEAD_DIM).transpose(1, 0, 2, 3)
    key_heads = norm_heads(keys, key_gain, KV_HEADS).transpose(1, 0, 2)
    value_heads = values.reshape(seq_len, KV_HEADS, HEAD_DIM).transpose(1, 0, 2)
    sink_rows = sink_logits.reshape(KV_HEADS, group_size)
    query_index = jnp.arange(WINDOW)[:, None]
    key_index = jnp.arange(2 * WINDOW)[None, :]
    offset_lag = WINDOW + query_index - key_index
    inband = (offset_lag >= 0) & (offset_lag < WINDOW)
    leading = (jnp.arange(block_count)[:, None, None] > 0) | (key_index[None] >= WINDOW)
    valid = inband[None] & leading

    def one_head(operands):
        query_h, key_h, value_h, sink_h = operands
        zero_rows = jnp.zeros((WINDOW, HEAD_DIM), jnp.bfloat16)
        key_prev = jnp.concatenate([zero_rows, key_h[:seq_len - WINDOW]], axis=0)
        value_prev = jnp.concatenate([zero_rows, value_h[:seq_len - WINDOW]], axis=0)
        key_blocks = jnp.concatenate([key_prev.reshape(block_count, WINDOW, HEAD_DIM), key_h.reshape(block_count, WINDOW, HEAD_DIM)], axis=1).astype(jnp.float32)
        value_blocks = jnp.concatenate([value_prev.reshape(block_count, WINDOW, HEAD_DIM), value_h.reshape(block_count, WINDOW, HEAD_DIM)], axis=1).astype(jnp.float32)
        query_blocks = query_h.reshape(block_count, WINDOW, group_size, HEAD_DIM).astype(jnp.float32)
        scores = jnp.einsum('nqgd,nkd->ngqk', query_blocks, key_blocks) * HEAD_DIM ** (-0.5)
        scores = jnp.where(valid[:, None], scores, -1e+30)
        sink_b = sink_h[None, :, None]
        row_peak = jnp.maximum(lax.optimization_barrier(jnp.max(scores, axis=-1)), sink_b)
        exp_terms = jnp.exp(scores - row_peak[..., None])
        denom_sum = lax.optimization_barrier(jnp.sum(exp_terms, axis=-1)) + jnp.exp(sink_b - row_peak)
        weights = (exp_terms / denom_sum[..., None]).astype(jnp.bfloat16)
        attended = jnp.einsum('ngqk,nkd->nqgd', weights.astype(jnp.float32), value_blocks).astype(jnp.bfloat16)
        return attended.reshape(seq_len, group_size, HEAD_DIM)
    heads_out = lax.map(one_head, (query_heads, key_heads, value_heads, sink_rows))
    attended = heads_out.transpose(1, 0, 2, 3).reshape(seq_len, Q_HEADS * HEAD_DIM)
    slice_width = Q_HEADS * HEAD_DIM // N_TP
    mixed = jnp.zeros((seq_len, D), jnp.float32)
    for member in range(N_TP):
        lower = member * slice_width
        product = jnp.dot(attended[:, lower:lower + slice_width], out_weight[lower:lower + slice_width], preferred_element_type=jnp.float32)
        mixed = mixed + product.astype(jnp.bfloat16).astype(jnp.float32)
    middle = (residual.astype(jnp.float32) + mixed).astype(jnp.bfloat16)
    middle_wide = middle.astype(jnp.float32)
    normed = (middle_wide * lax.rsqrt(lax.optimization_barrier(jnp.mean(middle_wide * middle_wide, axis=1, keepdims=True)) + 1e-06) * norm_gain).astype(jnp.bfloat16)
    hidden_width = FF // N_TP
    feed = jnp.zeros((seq_len, D), jnp.float32)
    for member in range(N_TP):
        lower = member * hidden_width
        gate_acts = jnp.dot(normed, gate_weight[:, lower:lower + hidden_width], preferred_element_type=jnp.float32)
        up_acts = jnp.dot(normed, up_weight[:, lower:lower + hidden_width], preferred_element_type=jnp.float32)
        hidden = (jax.nn.silu(gate_acts) * up_acts).astype(jnp.bfloat16)
        product = jnp.dot(hidden, down_weight[lower:lower + hidden_width], preferred_element_type=jnp.float32)
        feed = feed + product.astype(jnp.bfloat16).astype(jnp.float32)
    return (middle_wide + 0.5 * feed).astype(jnp.bfloat16)
```

```python
import functools

import jax
import jax.numpy as jnp
from jax import lax
from jax.experimental import pallas as pl
from jax.experimental.pallas import tpu as pltpu
from jax.sharding import PartitionSpec as P

WINDOW = 128
PAIR = 2
LANES = 128
EPS = 1e-06
MESH = pl.DeviceIdType.MESH


def swap(block, axis, flip):
    return lax.ppermute(block, axis, [(i, i ^ flip) for i in range(lax.axis_size(axis))])


def from_behind(block, axis, distance):
    devices = range(lax.axis_size(axis))
    route = [(i - distance, i) for i in devices if i - distance in devices]
    return lax.ppermute(block, axis, route)


def gather_flips(block, axis):
    found = {0: block}
    flip = lax.axis_size(axis) // 2
    while flip:
        for at, held in list(found.items()):
            found[at ^ flip] = swap(held, axis, flip)
        flip //= 2
    return [found[at] for at in range(lax.axis_size(axis))]


def norm_heads(flat, gain, heads):
    row_count = flat.shape[0]
    head_width = gain.shape[0]
    data = flat.astype(jnp.float32).reshape(row_count, heads, head_width)
    scaled = data * lax.rsqrt(jnp.mean(data * data, axis=-1, keepdims=True) + 1e-06) * gain
    return scaled.astype(jnp.bfloat16)


def attend(queries, keys, values, edge, query_gain, key_gain, sink_logits):
    head_width = query_gain.shape[0]
    row_count = queries.shape[0]
    q_heads = queries.shape[1] // head_width
    k_heads = keys.shape[1] // head_width
    group_size = q_heads // k_heads
    window_len = WINDOW
    block_count = row_count // window_len
    query_norm = norm_heads(queries, query_gain, q_heads)
    key_raw = jnp.concatenate([edge[:, : keys.shape[1]], keys], axis=0)
    key_all = norm_heads(key_raw, key_gain, k_heads).reshape(key_raw.shape)
    value_all = jnp.concatenate([edge[:, keys.shape[1] :], values], axis=0)

    def windows(flat):
        return jnp.concatenate(
            [
                flat[:row_count].reshape(block_count, window_len, k_heads, head_width),
                flat[window_len:].reshape(block_count, window_len, k_heads, head_width),
            ],
            axis=1,
        )

    key_blocks, value_blocks = windows(key_all), windows(value_all)
    query_blocks = query_norm.reshape(block_count, window_len, k_heads, group_size, head_width)
    scores = jnp.einsum(
        "nqhgd,nkhd->nhgqk", query_blocks, key_blocks, preferred_element_type=jnp.float32
    ) * head_width ** (-0.5)
    query_index = jnp.arange(window_len)[:, None]
    key_index = jnp.arange(2 * window_len)[None, :]
    offset_lag = window_len + query_index - key_index
    inband = (offset_lag >= 0) & (offset_lag < window_len)
    leading = (
        (jnp.arange(block_count)[:, None, None] > 0)
        | (key_index[None] >= window_len)
        | (lax.axis_index("sp") > 0)
    )
    valid = inband[None] & leading
    scores = jnp.where(valid[:, None, None], scores, -1e30)
    sink_rows = sink_logits.reshape(k_heads, group_size)[None, :, :, None]
    row_peak = jnp.maximum(jnp.max(scores, axis=-1), sink_rows)
    exp_terms = jnp.exp(scores - row_peak[..., None])
    denom_sum = jnp.sum(exp_terms, axis=-1) + jnp.exp(sink_rows - row_peak)
    weights = (exp_terms / denom_sum[..., None]).astype(jnp.bfloat16)
    attended = jnp.einsum(
        "nhgqk,nkhd->nqhgd", weights, value_blocks, preferred_element_type=jnp.float32
    ).astype(jnp.bfloat16)
    return attended.reshape(row_count, q_heads * head_width)


def permute_device(
    queries,
    keys,
    values,
    query_gain,
    key_gain,
    sink_logits,
    out_weight,
    residual,
    norm_gain,
    gate_weight,
    up_weight,
    down_weight,
):
    n_sp, n_tp = lax.axis_size("sp"), lax.axis_size("tp")
    sp, tp = lax.axis_index("sp"), lax.axis_index("tp")
    half = (sp // PAIR) % 2
    row_count, width = residual.shape
    depth, units = gate_weight.shape
    units //= 2

    def part(array, axis, flip):
        return lax.dynamic_slice_in_dim(array, (half ^ flip) * units, units, axis)

    far = list(range(2 * PAIR, n_sp, 2))

    def send(first, second, flips):
        found = {}
        for flip in flips:
            other = (flip // PAIR) % 2
            if second is None:
                piece = part(first, 0, other)
            else:
                piece = jnp.concatenate([part(first, 1, other), part(second, 1, other)], axis=1)
            found[flip] = swap(piece, "sp", flip) if flip else piece
        return found

    def relay(found, flips):
        for flip in flips:
            found[flip ^ 1] = swap(found[flip], "sp", 1)

    edge = jnp.concatenate([keys, values], axis=1)[row_count - WINDOW :]
    edge = from_behind(edge, "sp", 1)
    gate_weight, up_weight, residual, out_weight, edge = lax.optimization_barrier(
        (gate_weight, up_weight, residual, out_weight, edge)
    )
    near = [0, PAIR]
    first = far[: len(far) // 2]
    residual_pair = swap(residual, "sp", PAIR)
    both = send(gate_weight, up_weight, first)
    both.update(send(gate_weight, up_weight, near))
    attended = attend(queries, keys, values, edge, query_gain, key_gain, sink_logits)
    attended_pair = swap(attended, "sp", PAIR)

    gate_weight, up_weight, down_weight, attended_pair = lax.optimization_barrier(
        (gate_weight, up_weight, down_weight, attended_pair)
    )
    both.update(send(gate_weight, up_weight, far[len(far) // 2 :]))
    early = {flip: both[flip] for flip in first}
    down_weight, early = lax.optimization_barrier((down_weight, early))
    both.update(early)
    down = send(down_weight, None, far)
    down.update(send(down_weight, None, near))
    relay(both, near + far)
    relay(down, near)

    gains = jnp.concatenate(gather_flips(norm_gain, "tp"))
    projections = gather_flips(out_weight, "tp")
    stream = jnp.concatenate([residual, residual_pair], axis=0)
    stream = jnp.concatenate(gather_flips(stream, "tp"), axis=1).astype(jnp.float32)
    heads = gather_flips(jnp.concatenate([attended, attended_pair], axis=0), "tp")

    def own_first(columns):
        pieces = [
            lax.dynamic_slice_in_dim(columns, (tp ^ flip) * width, width, 1)
            for flip in range(n_tp)
        ]
        return jnp.concatenate(pieces, axis=1)

    projection = jnp.concatenate([own_first(piece) for piece in projections], axis=0)
    head = jnp.concatenate(heads, axis=1)
    mixed = jnp.dot(head, projection, preferred_element_type=jnp.float32)
    middle = (stream + mixed).astype(jnp.bfloat16)
    middle = lax.optimization_barrier(middle)
    middle_wide = middle.astype(jnp.float32)
    mean = jnp.mean(middle_wide * middle_wide, axis=1, keepdims=True)
    normed = (middle_wide * lax.rsqrt(mean + 1e-06) * gains).astype(jnp.bfloat16)

    late = {flip: down[flip] for flip in far}
    normed, late = lax.optimization_barrier((normed, late))
    down.update(late)
    relay(down, far)

    per_part = width // depth

    def place(flip):
        block = sp ^ flip
        return (((block // per_part) ^ tp) * per_part + block % per_part) * depth

    flips = range(n_sp)
    normed_in = jnp.concatenate(
        [lax.dynamic_slice_in_dim(normed, place(flip), depth, 1) for flip in flips], axis=1
    )
    gate_full = jnp.concatenate([both[flip][:, :units] for flip in flips], axis=0)
    up_full = jnp.concatenate([both[flip][:, units:] for flip in flips], axis=0)
    gate_acts = jnp.dot(normed_in, gate_full, preferred_element_type=jnp.float32)
    up_acts = jnp.dot(normed_in, up_full, preferred_element_type=jnp.float32)
    hidden = (jax.nn.silu(gate_acts) * up_acts).astype(jnp.bfloat16)

    down_full = jnp.zeros((units, width * n_tp), jnp.bfloat16)
    for flip in flips:
        down_full = lax.dynamic_update_slice_in_dim(down_full, down[flip], place(flip), 1)
    terms = [
        jnp.dot(
            hidden, down_full[:, at * width : (at + 1) * width], preferred_element_type=jnp.float32
        ).astype(jnp.bfloat16)
        for at in range(n_tp)
    ]

    def add(one, other):
        return one.astype(jnp.float32) + other.astype(jnp.float32)

    flip = 1
    held = dict(enumerate(terms))
    while flip < n_tp // 2:
        held = {
            at: add(held[at], swap(held[at ^ flip], "tp", flip)).astype(jnp.bfloat16)
            for at in held
            if not at & flip
        }
        flip *= 2
    own, other = held[0], held[flip]
    cut = width // 2
    across = add(own[:, :cut], swap(other[:, :cut], "tp", flip)).astype(jnp.bfloat16)
    left = add(across[:row_count], swap(across[row_count:], "sp", PAIR))
    pair = jnp.concatenate([own[:, cut:], other[:, cut:]], axis=1)
    pair = add(pair[:row_count], swap(pair[row_count:], "sp", PAIR)).astype(jnp.bfloat16)
    right = add(pair[:, : width - cut], swap(pair[:, width - cut :], "tp", flip))
    feed = jnp.concatenate([left, right], axis=1)
    return (middle_wide[:row_count, :width] + 0.5 * feed).astype(jnp.bfloat16)


def split_units(units):
    tiles = units // LANES
    small = (tiles // 2) * LANES
    return units - small, small


class Link:
    def __init__(self, sems, index):
        self.send, self.recv = sems[0].at[index], sems[1].at[index]

    def copy(self, src, dst, device):
        return pltpu.make_async_remote_copy(
            src_ref=src,
            dst_ref=dst,
            send_sem=self.send,
            recv_sem=self.recv,
            device_id=device,
            device_id_type=MESH,
        )


def layer_kernel(
    n_sp,
    n_tp,
    q_ref,
    k_ref,
    v_ref,
    qg_ref,
    kg_ref,
    sink_ref,
    ow_hbm,
    res_hbm,
    ng_ref,
    gate_hbm,
    up_hbm,
    down_hbm,
    out_ref,
    gt,
    ut,
    dn,
    mid,
    nrm,
    acc_g,
    acc_u,
    hid,
    pb,
    cb,
    xb,
    zs,
    zb,
    att,
    ow,
    gains,
    res,
    kn,
    vn,
    kh,
    send_sems,
    recv_sems,
    local_sems,
):
    s, t = lax.axis_index("sp"), lax.axis_index("tp")
    rows, width = res_hbm.shape
    depth, units = gate_hbm.shape
    big_units, small_units = split_units(units)
    window = WINDOW
    y = s % 2
    half = (s // PAIR) % 2
    is_big = (half + t) % 2 == 0
    core, far_tp = 1, n_tp // 2
    far = list(range(2 * PAIR, n_sp, PAIR))

    def flip_of(index, flip):
        out, bit = index, 1
        while bit <= flip:
            if flip & bit:
                out = out + bit - 2 * bit * ((index // bit) % 2)
            bit *= 2
        return out

    def xor(one, other, size):
        out, bit = 0, 1
        while bit < size:
            a, b = (one // bit) % 2, (other // bit) % 2
            out = out + bit * ((a + b) % 2)
            bit *= 2
        return out

    def sp_dev(flip):
        return {"sp": flip_of(s, flip)}

    def tp_dev(flip):
        return {"tp": flip_of(t, flip)}

    def sized(large, fn):
        if big_units == small_units:
            fn(big_units)
        else:
            pl.when(large)(lambda: fn(big_units))
            pl.when(jnp.logical_not(large))(lambda: fn(small_units))

    counter = [0]

    def new_link():
        counter[0] += 1
        return Link((send_sems, recv_sems), counter[0] - 1)

    ends = []

    locals_used = [0]

    def local(src, dst):
        locals_used[0] += 1
        return pltpu.make_async_copy(src, dst, local_sems.at[locals_used[0] - 1])

    kinds = {"g": (gate_hbm, gt), "u": (up_hbm, ut), "d": (down_hbm, dn)}
    weight_links = {(kind, flip): new_link() for kind in kinds for flip in range(1, n_sp)}

    def slot(kind, flip, size):
        buf = kinds[kind][1]
        if kind == "d":
            return buf.at[flip, pl.ds(0, size), :]
        return buf.at[flip // 2, pl.ds(((y + flip) % 2) * depth, depth), pl.ds(0, size)]

    def origin(kind, side, size):
        ref = kinds[kind][0]
        start = pl.multiple_of(side * (units - size), LANES)
        if kind == "d":
            return ref.at[pl.ds(start, size), :]
        return ref.at[:, pl.ds(start, size)]

    def remote_slot(kind, flip, size, seen_y):
        buf = kinds[kind][1]
        if kind == "d":
            return buf.at[flip, pl.ds(0, size), :]
        return buf.at[flip // 2, pl.ds(((seen_y + flip) % 2) * depth, depth), pl.ds(0, size)]

    def send_own(kind, flip):
        other = (flip // PAIR) % 2
        side = (half + other) % 2
        large = is_big if other == 0 else jnp.logical_not(is_big)
        seen_y = (y + flip) % 2

        def make(size):
            return weight_links[kind, flip].copy(
                origin(kind, side, size), remote_slot(kind, flip, size, seen_y), sp_dev(flip)
            )

        sized(large, lambda size: make(size).start())
        ends.append(lambda: sized(large, lambda size: make(size).wait_send()))

    def wait_weight(kind, flip):
        def wait(size):
            at = slot(kind, flip, size)
            weight_links[kind, flip].copy(at, at, sp_dev(flip)).wait_recv()

        sized(is_big, wait)

    def relay(kind, flip):
        wait_weight(kind, flip)

        def make(size):
            return weight_links[kind, flip ^ 1].copy(
                slot(kind, flip, size), remote_slot(kind, flip ^ 1, size, (y + 1) % 2), sp_dev(1)
            )

        sized(is_big, lambda size: make(size).start())
        ends.append(lambda: sized(is_big, lambda size: make(size).wait_send()))

    def send(link, src, dst, device):
        copy = link.copy(src, dst, device)
        copy.start()
        ends.append(copy.wait_send)

    def wait(link, at):
        link.copy(at, at, tp_dev(core)).wait_recv()

    if big_units != small_units:

        @pl.when(jnp.logical_not(is_big))
        def _():
            pad = big_units - small_units
            zero = jnp.zeros((gt.shape[1], pad), jnp.bfloat16)
            for chunk in range(gt.shape[0]):
                gt[chunk, :, small_units:] = zero
                ut[chunk, :, small_units:] = zero
            for flip in range(n_sp):
                dn[flip, small_units:, :] = jnp.zeros((pad, depth), jnp.bfloat16)

    @pl.when(s == 0)
    def _():
        kh[...] = jnp.zeros_like(kh)

    barrier = pltpu.get_barrier_semaphore()
    sp_flips = [1, PAIR] + far
    tp_flips = list(range(1, n_tp))
    for flip in sp_flips:
        pl.semaphore_signal(barrier, inc=1, device_id=sp_dev(flip), device_id_type=MESH)
    for flip in tp_flips:
        pl.semaphore_signal(barrier, inc=1, device_id=tp_dev(flip), device_id_type=MESH)

    @pl.when(s + 1 < n_sp)
    def _():
        pl.semaphore_signal(barrier, inc=1, device_id={"sp": s + 1}, device_id_type=MESH)

    @pl.when(s > 0)
    def _():
        pl.semaphore_signal(barrier, inc=1, device_id={"sp": s - 1}, device_id_type=MESH)

    greeted = len(sp_flips) + len(tp_flips)
    edges = jnp.where(s > 0, 1, 0) + jnp.where(s + 1 < n_sp, 1, 0)
    pl.semaphore_wait(barrier, greeted + edges)

    halo = [new_link(), new_link()]
    last = pl.ds(rows - window, window)

    def halo_copy(at, ref):
        return halo[at].copy(ref.at[last, :], kh.at[at], {"sp": jnp.minimum(s + 1, n_sp - 1)})

    @pl.when(s + 1 < n_sp)
    def _():
        for at, ref in enumerate((k_ref, v_ref)):
            halo_copy(at, ref).start()

    own_loads = {}
    for kind in kinds:

        def load(kind=kind):
            index = locals_used[0]
            locals_used[0] += 1

            def make(size):
                return pltpu.make_async_copy(
                    origin(kind, half, size), slot(kind, 0, size), local_sems.at[index]
                )

            sized(is_big, lambda size: make(size).start())
            return lambda: sized(is_big, lambda size: make(size).wait())

        own_loads[kind] = load()
    for kind in "gu":
        send_own(kind, 1)
    for flip in [PAIR] + far:
        for kind in "gu":
            send_own(kind, flip)
    res_load = local(res_hbm, res)
    res_load.start()
    ow_links = {flip: new_link() for flip in tp_flips}
    gain_links = {flip: new_link() for flip in tp_flips}
    for flip in tp_flips:
        start = pl.multiple_of(flip_of(t, flip) * width, LANES)
        send(ow_links[flip], ow_hbm.at[:, pl.ds(start, width)], ow.at[flip], tp_dev(flip))
        send(gain_links[flip], ng_ref, gains.at[flip], tp_dev(flip))
    ow_load = local(ow_hbm.at[:, pl.ds(pl.multiple_of(t * width, LANES), width)], ow.at[0])
    ow_load.start()
    gains[0] = ng_ref[...]

    head_width = qg_ref.shape[1]
    heads = q_ref.shape[1] // head_width
    blocks = rows // window
    scale = head_width ** (-0.5)

    def unit_norm(data, gain):
        data = data.astype(jnp.float32)
        mean = jnp.mean(data * data, axis=-1, keepdims=True)
        return (data * lax.rsqrt(mean + EPS) * gain).astype(jnp.bfloat16)

    def norm_keys(at, _):
        here = pl.ds(pl.multiple_of(at * window, window), window)
        there = pl.ds(pl.multiple_of((at + 1) * window, window), window)
        kn[there, :] = unit_norm(k_ref[here, :], kg_ref[...])
        vn[there, :] = v_ref[here, :]
        return 0

    lax.fori_loop(0, blocks, norm_keys, 0)

    def attend_block(at, _):
        here = pl.ds(pl.multiple_of(at * window, window), window)
        both = pl.ds(pl.multiple_of(at * window, window), 2 * window)
        keys, values = kn[both, :], vn[both, :]
        raw = q_ref[here, :]
        query_index = lax.broadcasted_iota(jnp.int32, (window, 2 * window), 0)
        key_index = lax.broadcasted_iota(jnp.int32, (window, 2 * window), 1)
        lag = window + query_index - key_index
        first = jnp.where(s * blocks + at > 0, 0, window)
        valid = (lag >= 0) & (lag < window) & (key_index >= first)
        pieces = []
        for head in range(heads):
            query = unit_norm(raw[:, head * head_width : (head + 1) * head_width], qg_ref[...])
            scores = lax.dot_general(
                query, keys, (((1,), (1,)), ((), ())), preferred_element_type=jnp.float32
            )
            scores = jnp.where(valid, scores * scale, -1e30)
            sink = sink_ref[0, head]
            peak = jnp.maximum(jnp.max(scores, axis=-1, keepdims=True), sink)
            terms = jnp.exp(scores - peak)
            total = jnp.sum(terms, axis=-1, keepdims=True) + jnp.exp(sink - peak)
            weights = (terms / total).astype(jnp.bfloat16)
            piece = jnp.dot(weights, values, preferred_element_type=jnp.float32)
            pieces.append(piece.astype(jnp.bfloat16))
        att[0, here, :] = jnp.concatenate(pieces, axis=1)
        return 0

    lax.fori_loop(1, blocks, attend_block, 0)

    @pl.when(s > 0)
    def _():
        for at in range(2):
            halo[at].copy(kh.at[at], kh.at[at], {"sp": jnp.maximum(s - 1, 0)}).wait_recv()

    kn[0:window, :] = unit_norm(kh[0], kg_ref[...])
    vn[0:window, :] = kh[1]
    lax.fori_loop(0, 1, attend_block, 0)

    att_links = {flip: new_link() for flip in tp_flips}
    send(att_links[far_tp], att.at[0], att.at[far_tp], tp_dev(far_tp))
    send(att_links[core], att.at[0], att.at[core], tp_dev(core))

    for kind in "gu":
        relay(kind, PAIR)

    wait(att_links[far_tp], att.at[far_tp])
    send(att_links[far_tp ^ core], att.at[far_tp], att.at[far_tp ^ core], tp_dev(core))

    for flip in tp_flips:
        wait(ow_links[flip], ow.at[flip])
        wait(gain_links[flip], gains.at[flip])
    ow_load.wait()
    res_load.wait()
    wait(att_links[core], att.at[core])
    wait(att_links[far_tp ^ core], att.at[far_tp ^ core])

    def project(at, _):
        here = pl.ds(pl.multiple_of(at * window, window), window)
        mixed = jnp.zeros((window, width), jnp.float32)
        for flip in range(n_tp):
            product = jnp.dot(att[flip, here, :], ow[flip], preferred_element_type=jnp.float32)
            mixed = mixed + product.astype(jnp.bfloat16).astype(jnp.float32)
        mid[0, 0, here, :] = (res[here, :].astype(jnp.float32) + mixed).astype(jnp.bfloat16)
        return 0

    cuts = 2
    piece = rows // cuts
    mid_links = {
        (side, flip, cut): new_link()
        for side in range(2)
        for flip in range(n_tp)
        for cut in range(cuts)
        if side or flip
    }

    def part(side, flip, cut):
        return mid.at[side, flip, pl.ds(cut * piece, piece), :]

    def pass_mid(side, flip, cut, to_side, to_flip, device):
        send(mid_links[to_side, to_flip, cut], part(side, flip, cut), part(to_side, to_flip, cut), device)

    def wait_mid(side, flip, cut):
        wait(mid_links[side, flip, cut], part(side, flip, cut))

    lax.fori_loop(0, blocks, project, 0)
    for cut in range(cuts):
        pass_mid(0, 0, cut, 1, 0, sp_dev(PAIR))
        pass_mid(0, 0, cut, 0, far_tp, tp_dev(far_tp))
        pass_mid(0, 0, cut, 0, core, tp_dev(core))

    norm_rows = 64

    def normalise(side):
        def step(at, _):
            here = pl.ds(pl.multiple_of(at * norm_rows, norm_rows), norm_rows)
            total = jnp.zeros((norm_rows, 1), jnp.float32)
            for flip in range(n_tp):
                data = mid[side, flip, here, :].astype(jnp.float32)
                total = total + jnp.sum(data * data, axis=1, keepdims=True)
            factor = lax.rsqrt(total / (width * n_tp) + EPS)
            for flip in range(n_tp):
                data = mid[side, flip, here, :].astype(jnp.float32)
                nrm[side, flip, here, :] = (data * factor * gains[flip]).astype(jnp.bfloat16)
            return 0

        lax.fori_loop(0, rows // norm_rows, step, 0)

    tile = 256
    n_chunks = n_sp // 2
    z = s // 2

    def expand(chunk, side):
        at_slot = xor(xor(z, chunk, n_chunks), t, n_chunks)

        def step(at, _):
            here = pl.ds(pl.multiple_of(at * tile, tile), tile)
            there = pl.ds(pl.multiple_of(side * rows + at * tile, tile), tile)
            data = nrm[side, at_slot, here, :]
            gate = jnp.dot(data, gt[chunk], preferred_element_type=jnp.float32)
            up = jnp.dot(data, ut[chunk], preferred_element_type=jnp.float32)
            if chunk:
                gate = gate + acc_g[there, :]
                up = up + acc_u[there, :]
            if chunk < n_chunks - 1:
                acc_g[there, :] = gate
                acc_u[there, :] = up
            else:
                hid[there, :] = (gate / (1.0 + jnp.exp(-gate)) * up).astype(jnp.bfloat16)
            return 0

        lax.fori_loop(0, rows // tile, step, 0)

    first_far = far[: len(far) // 2]
    later_far = far[len(far) // 2 :]
    for flip in first_far:
        relay("g", flip)
    for cut in range(cuts):
        wait_mid(0, far_tp, cut)
        pass_mid(0, far_tp, cut, 0, far_tp ^ core, tp_dev(core))
    for flip in first_far:
        relay("u", flip)
    for cut in range(cuts):
        wait_mid(1, 0, cut)
        pass_mid(1, 0, cut, 1, far_tp, tp_dev(far_tp))
        pass_mid(1, 0, cut, 1, core, tp_dev(core))
    for cut in range(cuts):
        wait_mid(0, core, cut)
        wait_mid(0, far_tp ^ core, cut)
    normalise(0)
    own_loads["g"]()
    own_loads["u"]()
    for kind in "gu":
        wait_weight(kind, 1)
    expand(0, 0)
    for flip in later_far:
        relay("g", flip)
    send_own("d", 1)
    for kind in "gu":
        wait_weight(kind, PAIR ^ 1)
    expand(1, 0)
    for flip in later_far:
        relay("u", flip)
    for flip in [PAIR] + far:
        send_own("d", flip)
    for cut in range(cuts):
        wait_mid(1, far_tp, cut)
        pass_mid(1, far_tp, cut, 1, far_tp ^ core, tp_dev(core))
    for cut in range(cuts):
        wait_mid(1, core, cut)
        wait_mid(1, far_tp ^ core, cut)
    normalise(1)
    expand(0, 1)
    expand(1, 1)
    for flip in first_far:
        for kind in "gu":
            wait_weight(kind, flip ^ 1)
        expand(flip // 2, 0)
        expand(flip // 2, 1)
    relay("d", PAIR)
    for flip in later_far:
        for kind in "gu":
            wait_weight(kind, flip ^ 1)
        expand(flip // 2, 0)
        expand(flip // 2, 1)

    core_links = [new_link() for _ in range(n_sp)]
    x_base = counter[0]
    counter[0] += 2
    z_links = [new_link() for _ in range(2)]

    def x_copy(flip, block):
        link = Link((send_sems, recv_sems), x_base + block)
        return link.copy(pb.at[flip], xb.at[block], tp_dev(far_tp))

    def shrink(flip):
        role = xor(xor(z, flip // 2, n_chunks), t, n_chunks)

        def step(at, _):
            here = pl.ds(pl.multiple_of(at * tile, tile), tile)
            product = jnp.dot(hid[here, :], dn[flip], preferred_element_type=jnp.float32)
            pb[flip, here, :] = product.astype(jnp.bfloat16)
            return 0

        lax.fori_loop(0, 2 * rows // tile, step, 0)
        copy = core_links[flip].copy(pb.at[flip], cb.at[flip], tp_dev(core))
        pl.when(role % 2 == 1)(copy.start)
        ends.append(lambda: pl.when(role % 2 == 1)(copy.wait_send))
        pl.when(role % 2 == 0)(copy.wait_recv)
        block = (y + flip) % 2

        @pl.when(role == far_tp)
        def _():
            def add(at, _):
                here = pl.ds(pl.multiple_of(at * tile, tile), tile)
                both = pb[flip, here, :].astype(jnp.float32) + cb[flip, here, :].astype(jnp.float32)
                pb[flip, here, :] = both.astype(jnp.bfloat16)
                return 0

            lax.fori_loop(0, 2 * rows // tile, add, 0)
            x_copy(flip, block).start()

        ends.append(lambda: pl.when(role == far_tp)(lambda: x_copy(flip, block).wait_send()))

    own_loads["d"]()
    shrink(0)
    wait_weight("d", 1)
    shrink(1)
    shrink(PAIR)
    for flip in first_far:
        relay("d", flip)
    wait_weight("d", PAIR ^ 1)
    shrink(PAIR ^ 1)
    for flip in first_far:
        shrink(flip)
    for flip in later_far:
        relay("d", flip)
    for flip in first_far:
        wait_weight("d", flip ^ 1)
        shrink(flip ^ 1)
    for flip in later_far:
        shrink(flip)
    for flip in later_far:
        wait_weight("d", flip ^ 1)
        shrink(flip ^ 1)

    mine = xor(z, t, n_chunks)
    for block in range(2):
        flip = 2 * mine + (y + block) % 2
        Link((send_sems, recv_sems), x_base + block).copy(
            xb.at[block], xb.at[block], tp_dev(far_tp)
        ).wait_recv()

        def total(at, base, flip=flip, block=block):
            here = pl.ds(pl.multiple_of(base + at * tile, tile), tile)
            held = pb[flip, here, :].astype(jnp.float32) + cb[flip, here, :].astype(jnp.float32)
            return held + xb[block, here, :].astype(jnp.float32)

        def give(at, _, block=block, total=total):
            here = pl.ds(pl.multiple_of(at * tile, tile), tile)
            zs[block, here, :] = total(at, rows).astype(jnp.bfloat16)
            return 0

        lax.fori_loop(0, rows // tile, give, 0)
        send(z_links[block], zs.at[block], zb.at[block], sp_dev(PAIR))
    for block in range(2):
        flip = 2 * mine + (y + block) % 2
        wait(z_links[block], zb.at[block])
        columns = slice(block * depth, (block + 1) * depth)

        def finish(at, _, flip=flip, block=block, columns=columns):
            here = pl.ds(pl.multiple_of(at * tile, tile), tile)
            held = pb[flip, here, :].astype(jnp.float32) + cb[flip, here, :].astype(jnp.float32)
            held = held + xb[block, here, :].astype(jnp.float32)
            feed = held + zb[block, here, :].astype(jnp.float32)
            base = mid[0, 0, here, columns].astype(jnp.float32)
            out_ref[here, columns] = (base + 0.5 * feed).astype(jnp.bfloat16)
            return 0

        lax.fori_loop(0, rows // tile, finish, 0)

    for end in ends:
        end()

    @pl.when(s + 1 < n_sp)
    def _():
        for at, ref in enumerate((k_ref, v_ref)):
            halo_copy(at, ref).wait_send()


def kernel_device(
    queries,
    keys,
    values,
    query_gain,
    key_gain,
    sink_logits,
    out_weight,
    residual,
    norm_gain,
    gate_weight,
    up_weight,
    down_weight,
):
    n_sp, n_tp = lax.axis_size("sp"), lax.axis_size("tp")
    rows, width = residual.shape
    depth, units = gate_weight.shape
    big, _ = split_units(units)
    heads_width = queries.shape[1]
    head_width = query_gain.shape[0]
    bf16, f32 = jnp.bfloat16, jnp.float32
    vmem = pl.BlockSpec(memory_space=pltpu.VMEM)
    smem = pl.BlockSpec(memory_space=pltpu.SMEM)
    hbm = pl.BlockSpec(memory_space=pl.ANY)
    n_links = 128
    scratch = [
        pltpu.VMEM((n_sp // 2, 2 * depth, big), bf16),
        pltpu.VMEM((n_sp // 2, 2 * depth, big), bf16),
        pltpu.VMEM((n_sp, big, depth), bf16),
        pltpu.VMEM((2, n_tp, rows, width), bf16),
        pltpu.VMEM((2, n_tp, rows, width), bf16),
        pltpu.VMEM((2 * rows, big), f32),
        pltpu.VMEM((2 * rows, big), f32),
        pltpu.VMEM((2 * rows, big), bf16),
        pltpu.VMEM((n_sp, 2 * rows, depth), bf16),
        pltpu.VMEM((n_sp, 2 * rows, depth), bf16),
        pltpu.VMEM((2, 2 * rows, depth), bf16),
        pltpu.VMEM((2, rows, depth), bf16),
        pltpu.VMEM((2, rows, depth), bf16),
        pltpu.VMEM((n_tp, rows, heads_width), bf16),
        pltpu.VMEM((n_tp, heads_width, width), bf16),
        pltpu.VMEM((n_tp, 1, width), f32),
        pltpu.VMEM((rows, width), bf16),
        pltpu.VMEM((rows + WINDOW, head_width), bf16),
        pltpu.VMEM((rows + WINDOW, head_width), bf16),
        pltpu.VMEM((2, WINDOW, head_width), bf16),
        pltpu.SemaphoreType.DMA((n_links,)),
        pltpu.SemaphoreType.DMA((n_links,)),
        pltpu.SemaphoreType.DMA((8,)),
    ]
    return pl.pallas_call(
        functools.partial(layer_kernel, n_sp, n_tp),
        out_shape=jax.ShapeDtypeStruct((rows, width), bf16),
        in_specs=[vmem, vmem, vmem, vmem, vmem, smem, hbm, hbm, vmem, hbm, hbm, hbm],
        out_specs=vmem,
        scratch_shapes=scratch,
        compiler_params=pltpu.CompilerParams(
            collective_id=0, has_side_effects=True, vmem_limit_bytes=66 * 1000 * 1000
        ),
    )(
        queries,
        keys,
        values,
        query_gain[None],
        key_gain[None],
        sink_logits[None],
        out_weight,
        residual,
        norm_gain[None],
        gate_weight,
        up_weight,
        down_weight,
    )


def per_device(*args):
    queries, keys, query_gain, residual, gate_weight = args[0], args[1], args[3], args[7], args[9]
    n_sp, n_tp = lax.axis_size("sp"), lax.axis_size("tp")
    depth, units = gate_weight.shape
    rows, width = residual.shape
    fits = (
        depth % LANES == 0
        and units % LANES == 0
        and rows % (2 * LANES) == 0
        and width == 2 * depth
        and n_sp == 2 * n_tp
        and n_tp // 2 == PAIR
        and n_sp % (2 * PAIR) == 0
        and keys.shape[1] == query_gain.shape[0]
    )
    return kernel_device(*args) if fits else permute_device(*args)


def solution(mesh):
    in_specs = (
        P("sp", "tp"),
        P("sp", "tp"),
        P("sp", "tp"),
        P(),
        P(),
        P("tp"),
        P("tp", None),
        P("sp", "tp"),
        P("tp"),
        P("sp", "tp"),
        P("sp", "tp"),
        P("tp", "sp"),
    )
    out_specs = P("sp", "tp")
    return jax.shard_map(
        per_device, mesh=mesh, in_specs=in_specs, out_specs=out_specs, check_vma=False
    )
```

```python
import functools

import jax
import jax.numpy as jnp
from jax import lax
from jax.experimental import pallas as pl
from jax.experimental.pallas import tpu as pltpu
from jax.sharding import PartitionSpec as P

WINDOW = 128
PAIR = 2
LANES = 128
PARTS = 2
EPS = 1e-06
MESH = pl.DeviceIdType.MESH


def swap(block, axis, flip):
    return lax.ppermute(block, axis, [(i, i ^ flip) for i in range(lax.axis_size(axis))])


def from_behind(block, axis, distance):
    devices = range(lax.axis_size(axis))
    route = [(i - distance, i) for i in devices if i - distance in devices]
    return lax.ppermute(block, axis, route)


def gather_flips(block, axis):
    found = {0: block}
    flip = lax.axis_size(axis) // 2
    while flip:
        for at, held in list(found.items()):
            found[at ^ flip] = swap(held, axis, flip)
        flip //= 2
    return [found[at] for at in range(lax.axis_size(axis))]


def norm_heads(flat, gain, heads):
    row_count = flat.shape[0]
    head_width = gain.shape[0]
    data = flat.astype(jnp.float32).reshape(row_count, heads, head_width)
    scaled = data * lax.rsqrt(jnp.mean(data * data, axis=-1, keepdims=True) + 1e-06) * gain
    return scaled.astype(jnp.bfloat16)


def attend(queries, keys, values, edge, query_gain, key_gain, sink_logits):
    head_width = query_gain.shape[0]
    row_count = queries.shape[0]
    q_heads = queries.shape[1] // head_width
    k_heads = keys.shape[1] // head_width
    group_size = q_heads // k_heads
    window_len = WINDOW
    block_count = row_count // window_len
    query_norm = norm_heads(queries, query_gain, q_heads)
    key_raw = jnp.concatenate([edge[:, : keys.shape[1]], keys], axis=0)
    key_all = norm_heads(key_raw, key_gain, k_heads).reshape(key_raw.shape)
    value_all = jnp.concatenate([edge[:, keys.shape[1] :], values], axis=0)

    def windows(flat):
        return jnp.concatenate(
            [
                flat[:row_count].reshape(block_count, window_len, k_heads, head_width),
                flat[window_len:].reshape(block_count, window_len, k_heads, head_width),
            ],
            axis=1,
        )

    key_blocks, value_blocks = windows(key_all), windows(value_all)
    query_blocks = query_norm.reshape(block_count, window_len, k_heads, group_size, head_width)
    scores = jnp.einsum(
        "nqhgd,nkhd->nhgqk", query_blocks, key_blocks, preferred_element_type=jnp.float32
    ) * head_width ** (-0.5)
    query_index = jnp.arange(window_len)[:, None]
    key_index = jnp.arange(2 * window_len)[None, :]
    offset_lag = window_len + query_index - key_index
    inband = (offset_lag >= 0) & (offset_lag < window_len)
    leading = (
        (jnp.arange(block_count)[:, None, None] > 0)
        | (key_index[None] >= window_len)
        | (lax.axis_index("sp") > 0)
    )
    valid = inband[None] & leading
    scores = jnp.where(valid[:, None, None], scores, -1e30)
    sink_rows = sink_logits.reshape(k_heads, group_size)[None, :, :, None]
    row_peak = jnp.maximum(jnp.max(scores, axis=-1), sink_rows)
    exp_terms = jnp.exp(scores - row_peak[..., None])
    denom_sum = jnp.sum(exp_terms, axis=-1) + jnp.exp(sink_rows - row_peak)
    weights = (exp_terms / denom_sum[..., None]).astype(jnp.bfloat16)
    attended = jnp.einsum(
        "nhgqk,nkhd->nqhgd", weights, value_blocks, preferred_element_type=jnp.float32
    ).astype(jnp.bfloat16)
    return attended.reshape(row_count, q_heads * head_width)


def permute_device(
    queries,
    keys,
    values,
    query_gain,
    key_gain,
    sink_logits,
    out_weight,
    residual,
    norm_gain,
    gate_weight,
    up_weight,
    down_weight,
):
    n_sp, n_tp = lax.axis_size("sp"), lax.axis_size("tp")
    sp, tp = lax.axis_index("sp"), lax.axis_index("tp")
    half = (sp // PAIR) % 2
    row_count, width = residual.shape
    depth, units = gate_weight.shape
    units //= 2

    def part(array, axis, flip):
        return lax.dynamic_slice_in_dim(array, (half ^ flip) * units, units, axis)

    far = list(range(2 * PAIR, n_sp, 2))

    def send(first, second, flips):
        found = {}
        for flip in flips:
            other = (flip // PAIR) % 2
            if second is None:
                piece = part(first, 0, other)
            else:
                piece = jnp.concatenate([part(first, 1, other), part(second, 1, other)], axis=1)
            found[flip] = swap(piece, "sp", flip) if flip else piece
        return found

    def relay(found, flips):
        for flip in flips:
            found[flip ^ 1] = swap(found[flip], "sp", 1)

    edge = jnp.concatenate([keys, values], axis=1)[row_count - WINDOW :]
    edge = from_behind(edge, "sp", 1)
    gate_weight, up_weight, residual, out_weight, edge = lax.optimization_barrier(
        (gate_weight, up_weight, residual, out_weight, edge)
    )
    near = [0, PAIR]
    first = far[: len(far) // 2]
    residual_pair = swap(residual, "sp", PAIR)
    both = send(gate_weight, up_weight, first)
    both.update(send(gate_weight, up_weight, near))
    attended = attend(queries, keys, values, edge, query_gain, key_gain, sink_logits)
    attended_pair = swap(attended, "sp", PAIR)

    gate_weight, up_weight, down_weight, attended_pair = lax.optimization_barrier(
        (gate_weight, up_weight, down_weight, attended_pair)
    )
    both.update(send(gate_weight, up_weight, far[len(far) // 2 :]))
    early = {flip: both[flip] for flip in first}
    down_weight, early = lax.optimization_barrier((down_weight, early))
    both.update(early)
    down = send(down_weight, None, far)
    down.update(send(down_weight, None, near))
    relay(both, near + far)
    relay(down, near)

    gains = jnp.concatenate(gather_flips(norm_gain, "tp"))
    projections = gather_flips(out_weight, "tp")
    stream = jnp.concatenate([residual, residual_pair], axis=0)
    stream = jnp.concatenate(gather_flips(stream, "tp"), axis=1).astype(jnp.float32)
    heads = gather_flips(jnp.concatenate([attended, attended_pair], axis=0), "tp")

    def own_first(columns):
        pieces = [
            lax.dynamic_slice_in_dim(columns, (tp ^ flip) * width, width, 1)
            for flip in range(n_tp)
        ]
        return jnp.concatenate(pieces, axis=1)

    projection = jnp.concatenate([own_first(piece) for piece in projections], axis=0)
    head = jnp.concatenate(heads, axis=1)
    mixed = jnp.dot(head, projection, preferred_element_type=jnp.float32)
    middle = (stream + mixed).astype(jnp.bfloat16)
    middle = lax.optimization_barrier(middle)
    middle_wide = middle.astype(jnp.float32)
    mean = jnp.mean(middle_wide * middle_wide, axis=1, keepdims=True)
    normed = (middle_wide * lax.rsqrt(mean + 1e-06) * gains).astype(jnp.bfloat16)

    late = {flip: down[flip] for flip in far}
    normed, late = lax.optimization_barrier((normed, late))
    down.update(late)
    relay(down, far)

    per_part = width // depth

    def place(flip):
        block = sp ^ flip
        return (((block // per_part) ^ tp) * per_part + block % per_part) * depth

    flips = range(n_sp)
    normed_in = jnp.concatenate(
        [lax.dynamic_slice_in_dim(normed, place(flip), depth, 1) for flip in flips], axis=1
    )
    gate_full = jnp.concatenate([both[flip][:, :units] for flip in flips], axis=0)
    up_full = jnp.concatenate([both[flip][:, units:] for flip in flips], axis=0)
    gate_acts = jnp.dot(normed_in, gate_full, preferred_element_type=jnp.float32)
    up_acts = jnp.dot(normed_in, up_full, preferred_element_type=jnp.float32)
    hidden = (jax.nn.silu(gate_acts) * up_acts).astype(jnp.bfloat16)

    down_full = jnp.zeros((units, width * n_tp), jnp.bfloat16)
    for flip in flips:
        down_full = lax.dynamic_update_slice_in_dim(down_full, down[flip], place(flip), 1)
    terms = [
        jnp.dot(
            hidden, down_full[:, at * width : (at + 1) * width], preferred_element_type=jnp.float32
        ).astype(jnp.bfloat16)
        for at in range(n_tp)
    ]

    def add(one, other):
        return one.astype(jnp.float32) + other.astype(jnp.float32)

    flip = 1
    held = dict(enumerate(terms))
    while flip < n_tp // 2:
        held = {
            at: add(held[at], swap(held[at ^ flip], "tp", flip)).astype(jnp.bfloat16)
            for at in held
            if not at & flip
        }
        flip *= 2
    own, other = held[0], held[flip]
    cut = width // 2
    across = add(own[:, :cut], swap(other[:, :cut], "tp", flip)).astype(jnp.bfloat16)
    left = add(across[:row_count], swap(across[row_count:], "sp", PAIR))
    pair = jnp.concatenate([own[:, cut:], other[:, cut:]], axis=1)
    pair = add(pair[:row_count], swap(pair[row_count:], "sp", PAIR)).astype(jnp.bfloat16)
    right = add(pair[:, : width - cut], swap(pair[:, width - cut :], "tp", flip))
    feed = jnp.concatenate([left, right], axis=1)
    return (middle_wide[:row_count, :width] + 0.5 * feed).astype(jnp.bfloat16)


def split_units(units):
    tiles = units // LANES
    small = (tiles // 2) * LANES
    return units - small, small


def scoped(name):
    def wrap(fn):
        def run(*args):
            tags = [str(arg) for arg in args if isinstance(arg, (int, str))]
            with jax.named_scope("_".join([name, *tags])):
                return fn(*args)

        return run

    return wrap


class Link:
    def __init__(self, sems, index):
        self.send, self.recv = sems[0].at[index], sems[1].at[index]

    def copy(self, src, dst, device):
        return pltpu.make_async_remote_copy(
            src_ref=src,
            dst_ref=dst,
            send_sem=self.send,
            recv_sem=self.recv,
            device_id=device,
            device_id_type=MESH,
        )


def layer_kernel(
    n_sp,
    n_tp,
    q_hbm,
    k_hbm,
    v_hbm,
    qg_ref,
    kg_ref,
    sink_ref,
    ow_hbm,
    res_hbm,
    ng_ref,
    gate_hbm,
    up_hbm,
    down_hbm,
    out_ref,
    gt,
    ut,
    dn,
    mid,
    nrm,
    acc_g,
    acc_u,
    hid,
    pb,
    cb,
    xb,
    zs,
    zb,
    att,
    ow,
    gains,
    res,
    kn,
    vn,
    kh,
    q_ref,
    k_ref,
    v_ref,
    send_sems,
    recv_sems,
    local_sems,
):
    s, t = lax.axis_index("sp"), lax.axis_index("tp")
    rows, width = res_hbm.shape
    depth, units = gate_hbm.shape
    big_units, small_units = split_units(units)
    window = WINDOW
    y = s % 2
    half = (s // PAIR) % 2
    is_big = (half + t) % 2 == 0
    core, far_tp = 1, n_tp // 2
    far = list(range(2 * PAIR, n_sp, PAIR))
    inner = (half + s // far[0]) % 2 == 1
    outer = jnp.logical_not(inner)
    soon = jnp.where(inner, far[1], far[0])
    late = jnp.where(inner, far[0], far[1])

    def flip_of(index, flip):
        out, bit = index, 1
        while bit <= flip:
            if flip & bit:
                out = out + bit - 2 * bit * ((index // bit) % 2)
            bit *= 2
        return out

    def xor(one, other, size):
        out, bit = 0, 1
        while bit < size:
            a, b = (one // bit) % 2, (other // bit) % 2
            out = out + bit * ((a + b) % 2)
            bit *= 2
        return out

    def sp_dev(flip):
        return {"sp": flip_of(s, flip)}

    def tp_dev(flip):
        return {"tp": flip_of(t, flip)}

    def sized(large, fn):
        if big_units == small_units:
            fn(big_units)
        else:
            pl.when(large)(lambda: fn(big_units))
            pl.when(jnp.logical_not(large))(lambda: fn(small_units))

    counter = [0]

    def new_link():
        counter[0] += 1
        return Link((send_sems, recv_sems), counter[0] - 1)

    ends = []

    locals_used = [0]

    def local(src, dst):
        locals_used[0] += 1
        return pltpu.make_async_copy(src, dst, local_sems.at[locals_used[0] - 1])

    kinds = {"g": (gate_hbm, gt), "u": (up_hbm, ut), "d": (down_hbm, dn)}
    counter[0] = len(kinds) * n_sp * PARTS
    step_depth = depth // PARTS

    def weight_link(kind, flip, cut):
        index = ("gud".index(kind) * n_sp + flip) * PARTS + cut
        return Link((send_sems, recv_sems), index)

    def slot(kind, flip, size, cut=None, seen_y=y):
        buf = kinds[kind][1]
        first, count = (0, depth) if cut is None else (cut * step_depth, step_depth)
        if kind == "d":
            return buf.at[flip, pl.ds(0, size), pl.ds(first, count)]
        start = ((seen_y + flip) % 2) * depth + first
        return buf.at[flip // 2, pl.ds(start, count), pl.ds(0, size)]

    def origin(kind, side, size, cut=None):
        ref = kinds[kind][0]
        first, count = (0, depth) if cut is None else (cut * step_depth, step_depth)
        start = pl.multiple_of(side * (units - size), LANES)
        if kind == "d":
            return ref.at[pl.ds(start, size), pl.ds(first, count)]
        return ref.at[pl.ds(first, count), pl.ds(start, size)]

    def own_copies(kind, flip):
        other = (flip // PAIR) % 2
        side = (half + other) % 2
        large = is_big if other == 0 else jnp.logical_not(is_big)

        def make(size, cut):
            return weight_link(kind, flip, cut).copy(
                origin(kind, side, size, cut),
                slot(kind, flip, size, cut, (y + flip) % 2),
                sp_dev(flip),
            )

        return large, make

    def send_own(kind, flip):
        large, make = own_copies(kind, flip)
        for cut in range(PARTS):
            sized(large, lambda size: make(size, cut).start())

    def drain_own(kind, flip):
        large, make = own_copies(kind, flip)
        for cut in range(PARTS):
            sized(large, lambda size: make(size, cut).wait_send())

    def wait_part(kind, flip, cut):
        def wait(size):
            at = slot(kind, flip, size, cut)
            weight_link(kind, flip, cut).copy(at, at, sp_dev(1)).wait_recv()

        sized(is_big, wait)

    @scoped("wait_weight")
    def wait_weight(kind, flip):
        for cut in range(PARTS):
            wait_part(kind, flip, cut)

    def relay_copy(kind, flip, size, cut):
        return weight_link(kind, flip + 1, cut).copy(
            slot(kind, flip, size, cut), slot(kind, flip + 1, size, cut, (y + 1) % 2), sp_dev(1)
        )

    @scoped("relay")
    def relay(kind, flip):
        for cut in range(PARTS):
            wait_part(kind, flip, cut)
            sized(is_big, lambda size: relay_copy(kind, flip, size, cut).start())

    def drain_relay(kind, flip):
        for cut in range(PARTS):
            sized(is_big, lambda size: relay_copy(kind, flip, size, cut).wait_send())

    def send(link, src, dst, device):
        copy = link.copy(src, dst, device)
        copy.start()
        ends.append(copy.wait_send)

    def wait(link, at):
        link.copy(at, at, tp_dev(core)).wait_recv()

    if big_units != small_units:

        @pl.when(jnp.logical_not(is_big))
        def _():
            pad = big_units - small_units
            zero = jnp.zeros((gt.shape[1], pad), jnp.bfloat16)
            for chunk in range(gt.shape[0]):
                gt[chunk, :, small_units:] = zero
                ut[chunk, :, small_units:] = zero
            for flip in range(n_sp):
                dn[flip, small_units:, :] = jnp.zeros((pad, depth), jnp.bfloat16)

    @pl.when(s == 0)
    def _():
        kh[...] = jnp.zeros_like(kh)

    qkv_loads = [local(q_hbm, q_ref), local(k_hbm, k_ref), local(v_hbm, v_ref)]
    for load in qkv_loads:
        load.start()

    barrier = pltpu.get_barrier_semaphore()
    sp_flips = [1, PAIR] + far
    tp_flips = list(range(1, n_tp))
    for flip in sp_flips:
        pl.semaphore_signal(barrier, inc=1, device_id=sp_dev(flip), device_id_type=MESH)
    for flip in tp_flips:
        pl.semaphore_signal(barrier, inc=1, device_id=tp_dev(flip), device_id_type=MESH)

    @pl.when(s + 1 < n_sp)
    def _():
        pl.semaphore_signal(barrier, inc=1, device_id={"sp": s + 1}, device_id_type=MESH)

    @pl.when(s > 0)
    def _():
        pl.semaphore_signal(barrier, inc=1, device_id={"sp": s - 1}, device_id_type=MESH)

    greeted = len(sp_flips) + len(tp_flips)
    edges = jnp.where(s > 0, 1, 0) + jnp.where(s + 1 < n_sp, 1, 0)
    with jax.named_scope("barrier"):
        pl.semaphore_wait(barrier, greeted + edges)

    halo = [new_link(), new_link()]
    last = pl.ds(rows - window, window)

    def halo_copy(at, ref):
        return halo[at].copy(ref.at[:, last], kh.at[at], {"sp": jnp.minimum(s + 1, n_sp - 1)})

    @pl.when(s + 1 < n_sp)
    def _():
        for at, ref in enumerate((k_hbm, v_hbm)):
            halo_copy(at, ref).start()

    own_loads = {}
    for kind in kinds:

        def load(kind=kind):
            index = locals_used[0]
            locals_used[0] += 1

            def make(size):
                return pltpu.make_async_copy(
                    origin(kind, half, size), slot(kind, 0, size), local_sems.at[index]
                )

            sized(is_big, lambda size: make(size).start())
            return lambda: sized(is_big, lambda size: make(size).wait())

        own_loads[kind] = load()
    for kind in kinds:
        send_own(kind, 1)
    for kind in "gu":
        send_own(kind, PAIR)
    pl.when(outer)(lambda: send_own("d", PAIR))

    @pl.when(inner)
    def _():
        for flip in reversed(far):
            for kind in "gu":
                send_own(kind, flip)
        send_own("d", far[1])

    res_load = local(res_hbm, res)
    res_load.start()
    ow_links = {flip: new_link() for flip in tp_flips}
    gain_links = {flip: new_link() for flip in tp_flips}
    for flip in tp_flips:
        start = pl.multiple_of(flip_of(t, flip) * width, LANES)
        send(ow_links[flip], ow_hbm.at[:, pl.ds(start, width)], ow.at[flip], tp_dev(flip))
        send(gain_links[flip], ng_ref, gains.at[flip], tp_dev(flip))
    ow_load = local(ow_hbm.at[:, pl.ds(pl.multiple_of(t * width, LANES), width)], ow.at[0])
    ow_load.start()
    gains[0] = ng_ref[...]

    head_width = qg_ref.shape[1]
    heads = q_ref.shape[1] // head_width
    blocks = rows // window
    scale = head_width ** (-0.5)

    def unit_norm(data, gain):
        data = data.astype(jnp.float32)
        mean = jnp.mean(data * data, axis=-1, keepdims=True)
        return (data * lax.rsqrt(mean + EPS) * gain).astype(jnp.bfloat16)

    def turn(block):
        return block.astype(jnp.float32).T

    for load in qkv_loads:
        load.wait()

    def norm_keys(at, _):
        here = pl.ds(pl.multiple_of(at * window, window), window)
        there = pl.ds(pl.multiple_of((at + 1) * window, window), window)
        kn[there, :] = unit_norm(turn(k_ref[:, here]), kg_ref[...])
        vn[there, :] = turn(v_ref[:, here]).astype(jnp.bfloat16)
        return 0

    lax.fori_loop(0, blocks, norm_keys, 0)

    def attend_block(at, _):
        here = pl.ds(pl.multiple_of(at * window, window), window)
        both = pl.ds(pl.multiple_of(at * window, window), 2 * window)
        keys, values = kn[both, :], vn[both, :]
        raw = q_ref[here, :]
        query_index = lax.broadcasted_iota(jnp.int32, (window, 2 * window), 0)
        key_index = lax.broadcasted_iota(jnp.int32, (window, 2 * window), 1)
        lag = window + query_index - key_index
        first = jnp.where(s * blocks + at > 0, 0, window)
        valid = (lag >= 0) & (lag < window) & (key_index >= first)
        pieces = []
        for head in range(heads):
            query = unit_norm(raw[:, head * head_width : (head + 1) * head_width], qg_ref[...])
            scores = lax.dot_general(
                query, keys, (((1,), (1,)), ((), ())), preferred_element_type=jnp.float32
            )
            scores = jnp.where(valid, scores * scale, -1e30)
            sink = sink_ref[0, head]
            peak = jnp.maximum(jnp.max(scores, axis=-1, keepdims=True), sink)
            terms = jnp.exp(scores - peak)
            total = jnp.sum(terms, axis=-1, keepdims=True) + jnp.exp(sink - peak)
            weights = (terms / total).astype(jnp.bfloat16)
            piece = jnp.dot(weights, values, preferred_element_type=jnp.float32)
            pieces.append(piece.astype(jnp.bfloat16))
        att[0, here, :] = jnp.concatenate(pieces, axis=1)
        return 0

    with jax.named_scope("attend"):
        lax.fori_loop(1, blocks, attend_block, 0)

    @pl.when(s > 0)
    def _():
        for at in range(2):
            halo[at].copy(kh.at[at], kh.at[at], {"sp": jnp.maximum(s - 1, 0)}).wait_recv()

    kn[0:window, :] = unit_norm(turn(kh[0]), kg_ref[...])
    vn[0:window, :] = turn(kh[1]).astype(jnp.bfloat16)
    with jax.named_scope("attend_first"):
        lax.fori_loop(0, 1, attend_block, 0)

    att_links = {flip: new_link() for flip in tp_flips}
    send(att_links[far_tp], att.at[0], att.at[far_tp], tp_dev(far_tp))
    send(att_links[core], att.at[0], att.at[core], tp_dev(core))

    with jax.named_scope("wait_att"):
        wait(att_links[far_tp], att.at[far_tp])
    send(att_links[far_tp ^ core], att.at[far_tp], att.at[far_tp ^ core], tp_dev(core))

    for flip in tp_flips:
        with jax.named_scope("wait_ow"):
            wait(ow_links[flip], ow.at[flip])
        wait(gain_links[flip], gains.at[flip])
    ow_load.wait()
    res_load.wait()
    wait(att_links[core], att.at[core])
    wait(att_links[far_tp ^ core], att.at[far_tp ^ core])

    def project(at, _):
        here = pl.ds(pl.multiple_of(at * window, window), window)
        mixed = jnp.zeros((window, width), jnp.float32)
        for flip in range(n_tp):
            product = jnp.dot(att[flip, here, :], ow[flip], preferred_element_type=jnp.float32)
            mixed = mixed + product.astype(jnp.bfloat16).astype(jnp.float32)
        mid[0, 0, here, :] = (res[here, :].astype(jnp.float32) + mixed).astype(jnp.bfloat16)
        return 0

    cuts = 2
    piece = rows // cuts
    mid_links = {
        (side, flip, cut): new_link()
        for side in range(2)
        for flip in range(n_tp)
        for cut in range(cuts)
        if side or flip
    }

    def part(side, flip, cut):
        return mid.at[side, flip, pl.ds(cut * piece, piece), :]

    def pass_mid(side, flip, cut, to_side, to_flip, device):
        send(mid_links[to_side, to_flip, cut], part(side, flip, cut), part(to_side, to_flip, cut), device)

    @scoped("wait_mid")
    def wait_mid(side, flip, cut):
        wait(mid_links[side, flip, cut], part(side, flip, cut))

    with jax.named_scope("project"):
        lax.fori_loop(0, blocks, project, 0)
    for cut in range(cuts):
        pass_mid(0, 0, cut, 1, 0, sp_dev(PAIR))
        pass_mid(0, 0, cut, 0, far_tp, tp_dev(far_tp))
        pass_mid(0, 0, cut, 0, core, tp_dev(core))

    norm_rows = 64

    @scoped("normalise")
    def normalise(side):
        def step(at, _):
            here = pl.ds(pl.multiple_of(at * norm_rows, norm_rows), norm_rows)
            total = jnp.zeros((norm_rows, 1), jnp.float32)
            for flip in range(n_tp):
                data = mid[side, flip, here, :].astype(jnp.float32)
                total = total + jnp.sum(data * data, axis=1, keepdims=True)
            factor = lax.rsqrt(total / (width * n_tp) + EPS)
            for flip in range(n_tp):
                data = mid[side, flip, here, :].astype(jnp.float32)
                nrm[side, flip, here, :] = (data * factor * gains[flip]).astype(jnp.bfloat16)
            return 0

        lax.fori_loop(0, rows // norm_rows, step, 0)

    pl.when(inner)(lambda: send_own("d", PAIR))

    @pl.when(outer)
    def _():
        for kind in "gu":
            for flip in reversed(far):
                send_own(kind, flip)
        for flip in reversed(far):
            send_own("d", flip)

    tile = 256
    n_chunks = n_sp // 2
    z = s // 2

    @scoped("expand")
    def expand(chunk, side, first=False, last=False):
        at_slot = xor(xor(z, chunk, n_chunks), t, n_chunks)

        def step(at, _):
            here = pl.ds(pl.multiple_of(at * tile, tile), tile)
            there = pl.ds(pl.multiple_of(side * rows + at * tile, tile), tile)
            data = nrm[side, at_slot, here, :]
            gate = jnp.dot(data, gt[chunk], preferred_element_type=jnp.float32)
            up = jnp.dot(data, ut[chunk], preferred_element_type=jnp.float32)
            if not first:
                gate = gate + acc_g[there, :]
                up = up + acc_u[there, :]
            if not last:
                acc_g[there, :] = gate
                acc_u[there, :] = up
            else:
                hid[there, :] = (gate / (1.0 + jnp.exp(-gate)) * up).astype(jnp.bfloat16)
            return 0

        lax.fori_loop(0, rows // tile, step, 0)

    def wait_beside(flip):
        for kind in "gu":
            wait_weight(kind, flip + 1)

    def spread(cut):
        wait_mid(1, 0, cut)
        pass_mid(1, 0, cut, 1, far_tp, tp_dev(far_tp))
        pass_mid(1, 0, cut, 1, core, tp_dev(core))

    for kind in "gu":
        relay(kind, PAIR)
    for kind in "gu":
        relay(kind, soon)
    for cut in range(cuts):
        wait_mid(0, far_tp, cut)
        pass_mid(0, far_tp, cut, 0, far_tp ^ core, tp_dev(core))
    spread(0)
    pl.when(inner)(lambda: relay("d", PAIR))
    for cut in range(cuts):
        wait_mid(0, core, cut)
        wait_mid(0, far_tp ^ core, cut)
    normalise(0)
    own_loads["g"]()
    own_loads["u"]()
    wait_beside(0)
    expand(0, 0, True)
    spread(1)
    wait_beside(PAIR)
    expand(1, 0)
    relay("g", late)
    wait_beside(soon)
    expand(soon // 2, 0)
    pl.when(inner)(lambda: send_own("d", far[0]))
    for cut in range(cuts):
        wait_mid(1, far_tp, cut)
        pass_mid(1, far_tp, cut, 1, far_tp ^ core, tp_dev(core))
    for cut in range(cuts):
        wait_mid(1, core, cut)
        wait_mid(1, far_tp ^ core, cut)
    normalise(1)
    expand(0, 1, True)
    relay("u", late)

    @pl.when(inner)
    def _():
        relay("d", soon)

    pl.when(outer)(lambda: relay("d", PAIR))
    expand(1, 1)
    expand(soon // 2, 1)
    wait_beside(late)
    expand(late // 2, 0, False, True)
    expand(late // 2, 1, False, True)

    core_links = counter[0]
    x_links = core_links + 2 * n_sp
    z_links = x_links + 4
    counter[0] += 2 * n_sp + 8
    my_end = (t // far_tp + t) % 2 == 0
    not_end = jnp.logical_not(my_end)

    def link(index):
        return Link((send_sems, recv_sems), index)

    def role_of(flip):
        return xor(xor(z, flip // 2, n_chunks), t, n_chunks)

    def side_rows(side):
        return pl.ds(side * rows, rows)

    def core_copy(flip, side):
        some = side_rows(side)
        return link(core_links + 2 * flip + side).copy(
            pb.at[flip, some, :], cb.at[flip, some, :], tp_dev(core)
        )

    def x_copy(flip, block, side):
        some = side_rows(side)
        return link(x_links + 2 * block + side).copy(
            pb.at[flip, some, :], xb.at[block, some, :], tp_dev(far_tp)
        )

    def z_copy(place, block):
        return link(z_links + 2 * place + block).copy(
            zs.at[place, block], zb.at[place, block], sp_dev(PAIR)
        )

    def over_rows(fn):
        def step(at, _):
            fn(pl.multiple_of(at * tile, tile))
            return 0

        lax.fori_loop(0, rows // tile, step, 0)

    def wide(ref, *index):
        return ref[index].astype(jnp.float32)

    def at_side(side, base):
        return pl.ds(pl.multiple_of(side * rows + base, tile), tile)

    @scoped("shrink")
    def shrink(flip):
        for side in (1, 0):

            def step(base, side=side):
                here = at_side(side, base)
                product = jnp.dot(hid[here, :], dn[flip], preferred_element_type=jnp.float32)
                pb[flip, here, :] = product.astype(jnp.bfloat16)

            over_rows(step)
            pl.when(role_of(flip) % 2 == 1)(lambda: core_copy(flip, side).start())

    def give_pair(place, flip, block, with_x):
        core_copy(flip, 1).wait_recv()
        if with_x:
            x_copy(flip, block, 1).wait_recv()

        def step(base):
            there = at_side(1, base)
            held = wide(pb, flip, there) + wide(cb, flip, there)
            if with_x:
                held = held + wide(xb, block, there)
            zs[place, block, pl.ds(base, tile), :] = held.astype(jnp.bfloat16)

        over_rows(step)
        z_copy(place, block).start()

    @scoped("collect")
    def collect(flip):
        role = role_of(flip)
        block = (y + flip) % 2

        @pl.when(jnp.logical_and(role == far_tp, my_end))
        def _():
            for side in (1, 0):
                core_copy(flip, side).wait_recv()

                def step(base, side=side):
                    here = at_side(side, base)
                    held = wide(pb, flip, here) + wide(cb, flip, here)
                    pb[flip, here, :] = held.astype(jnp.bfloat16)

                over_rows(step)
                x_copy(flip, block, side).start()

        pl.when(jnp.logical_and(role == far_tp, not_end))(lambda: give_pair(1, flip, block, False))
        pl.when(jnp.logical_and(role == 0, my_end))(lambda: give_pair(0, flip, block, False))

    mine = xor(z, t, n_chunks)
    theirs = xor(mine, far_tp, n_chunks)

    def flip_at(chunk, block):
        return 2 * chunk + (y + block) % 2

    def second_theirs(block):
        flip = flip_at(theirs, block)
        z_copy(1, block).wait_recv()
        core_copy(flip, 0).wait_recv()

        def step(base):
            here = pl.ds(base, tile)
            held = wide(pb, flip, here) + wide(cb, flip, here) + wide(zb, 1, block, here)
            pb[flip, here, :] = held.astype(jnp.bfloat16)

        over_rows(step)
        x_copy(flip, block, 0).start()

    own_loads["d"]()
    shrink(0)
    wait_weight("d", 1)
    shrink(1)
    collect(0)
    collect(1)
    pl.when(outer)(lambda: relay("d", soon))
    shrink(PAIR)
    wait_weight("d", PAIR + 1)
    shrink(PAIR + 1)
    collect(PAIR)
    collect(PAIR + 1)
    shrink(soon)
    wait_weight("d", soon + 1)
    shrink(soon + 1)
    collect(soon)
    collect(soon + 1)
    relay("d", late)
    shrink(late)

    @pl.when(jnp.logical_and(not_end, theirs < n_chunks // 2))
    def _():
        with jax.named_scope("theirs_near"):
            for block in range(2):
                second_theirs(block)

    collect(late)
    wait_weight("d", late + 1)
    shrink(late + 1)
    collect(late + 1)

    @pl.when(jnp.logical_and(not_end, theirs < n_chunks // 2))
    def _():
        with jax.named_scope("mine_far"):
            for block in range(2):
                give_pair(0, flip_at(mine, block), block, True)

    @pl.when(jnp.logical_and(not_end, theirs >= n_chunks // 2))
    def _():
        with jax.named_scope("mine_near"):
            for block in range(2):
                give_pair(0, flip_at(mine, block), block, True)
        with jax.named_scope("theirs_far"):
            for block in range(2):
                second_theirs(block)

    for block in range(2):
        flip = flip_at(mine, block)
        with jax.named_scope("wait_z"):
            core_copy(flip, 0).wait_recv()
            z_copy(0, block).wait_recv()
        with jax.named_scope("wait_x"):
            x_copy(flip, block, 0).wait_recv()
        columns = slice(block * depth, (block + 1) * depth)

        def finish(base, flip=flip, block=block, columns=columns):
            here = pl.ds(base, tile)
            feed = wide(pb, flip, here) + wide(cb, flip, here) + wide(zb, 0, block, here)
            feed = feed + wide(xb, block, here)
            out_ref[here, columns] = (wide(mid, 0, 0, here, columns) + 0.5 * feed).astype(jnp.bfloat16)

        over_rows(finish)

    with jax.named_scope("ends"):
        for end in ends:
            end()
        for kind in kinds:
            for flip in [1, PAIR] + far:
                drain_own(kind, flip)
            for flip in [PAIR] + far:
                drain_relay(kind, flip)
        for flip in range(n_sp):
            for side in range(2):
                pl.when(role_of(flip) % 2 == 1)(lambda: core_copy(flip, side).wait_send())
        for block in range(2):
            flip = flip_at(theirs, block)
            x_copy(flip, block, 0).wait_send()
            pl.when(my_end)(lambda: x_copy(flip, block, 1).wait_send())
            z_copy(0, block).wait_send()
            pl.when(not_end)(lambda: z_copy(1, block).wait_send())

    @pl.when(s + 1 < n_sp)
    def _():
        for at, ref in enumerate((k_hbm, v_hbm)):
            halo_copy(at, ref).wait_send()


def kernel_device(
    queries,
    keys,
    values,
    query_gain,
    key_gain,
    sink_logits,
    out_weight,
    residual,
    norm_gain,
    gate_weight,
    up_weight,
    down_weight,
):
    n_sp, n_tp = lax.axis_size("sp"), lax.axis_size("tp")
    rows, width = residual.shape
    depth, units = gate_weight.shape
    big, _ = split_units(units)
    heads_width = queries.shape[1]
    head_width = query_gain.shape[0]
    bf16, f32 = jnp.bfloat16, jnp.float32
    vmem = pl.BlockSpec(memory_space=pltpu.VMEM)
    smem = pl.BlockSpec(memory_space=pltpu.SMEM)
    hbm = pl.BlockSpec(memory_space=pl.ANY)
    n_links = 128
    scratch = [
        pltpu.VMEM((n_sp // 2, 2 * depth, big), bf16),
        pltpu.VMEM((n_sp // 2, 2 * depth, big), bf16),
        pltpu.VMEM((n_sp, big, depth), bf16),
        pltpu.VMEM((2, n_tp, rows, width), bf16),
        pltpu.VMEM((2, n_tp, rows, width), bf16),
        pltpu.VMEM((2 * rows, big), f32),
        pltpu.VMEM((2 * rows, big), f32),
        pltpu.VMEM((2 * rows, big), bf16),
        pltpu.VMEM((n_sp, 2 * rows, depth), bf16),
        pltpu.VMEM((n_sp, 2 * rows, depth), bf16),
        pltpu.VMEM((2, 2 * rows, depth), bf16),
        pltpu.VMEM((2, 2, rows, depth), bf16),
        pltpu.VMEM((2, 2, rows, depth), bf16),
        pltpu.VMEM((n_tp, rows, heads_width), bf16),
        pltpu.VMEM((n_tp, heads_width, width), bf16),
        pltpu.VMEM((n_tp, 1, width), f32),
        pltpu.VMEM((rows, width), bf16),
        pltpu.VMEM((rows + WINDOW, head_width), bf16),
        pltpu.VMEM((rows + WINDOW, head_width), bf16),
        pltpu.VMEM((2, head_width, WINDOW), bf16),
        pltpu.VMEM((rows, heads_width), bf16),
        pltpu.VMEM((head_width, rows), bf16),
        pltpu.VMEM((head_width, rows), bf16),
        pltpu.SemaphoreType.DMA((n_links,)),
        pltpu.SemaphoreType.DMA((n_links,)),
        pltpu.SemaphoreType.DMA((8,)),
    ]
    return pl.pallas_call(
        functools.partial(layer_kernel, n_sp, n_tp),
        out_shape=jax.ShapeDtypeStruct((rows, width), bf16),
        in_specs=[hbm, hbm, hbm, vmem, vmem, smem, hbm, hbm, vmem, hbm, hbm, hbm],
        out_specs=vmem,
        scratch_shapes=scratch,
        compiler_params=pltpu.CompilerParams(
            collective_id=0, has_side_effects=True, vmem_limit_bytes=66 * 1000 * 1000
        ),
    )(
        queries,
        keys.T,
        values.T,
        query_gain[None],
        key_gain[None],
        sink_logits[None],
        out_weight,
        residual,
        norm_gain[None],
        gate_weight,
        up_weight,
        down_weight,
    )


def per_device(*args):
    queries, keys, query_gain, residual, gate_weight = args[0], args[1], args[3], args[7], args[9]
    n_sp, n_tp = lax.axis_size("sp"), lax.axis_size("tp")
    depth, units = gate_weight.shape
    rows, width = residual.shape
    fits = (
        depth % LANES == 0
        and units % LANES == 0
        and rows % (2 * LANES) == 0
        and width == 2 * depth
        and n_sp == 2 * n_tp
        and n_tp // 2 == PAIR
        and n_sp % (2 * PAIR) == 0
        and keys.shape[1] == query_gain.shape[0]
    )
    return kernel_device(*args) if fits else permute_device(*args)


def solution(mesh):
    in_specs = (
        P("sp", "tp"),
        P("sp", "tp"),
        P("sp", "tp"),
        P(),
        P(),
        P("tp"),
        P("tp", None),
        P("sp", "tp"),
        P("tp"),
        P("sp", "tp"),
        P("sp", "tp"),
        P("tp", "sp"),
    )
    out_specs = P("sp", "tp")
    return jax.shard_map(
        per_device, mesh=mesh, in_specs=in_specs, out_specs=out_specs, check_vma=False
    )
```

```python
import functools

import jax
import jax.numpy as jnp
from jax import lax
from jax.experimental import pallas as pl
from jax.experimental.pallas import tpu as pltpu
from jax.sharding import PartitionSpec as P

WINDOW = 128
PAIR = 2
LANES = 128
PARTS = 2
EPS = 1e-06
MESH = pl.DeviceIdType.MESH


def swap(block, axis, flip):
    return lax.ppermute(block, axis, [(i, i ^ flip) for i in range(lax.axis_size(axis))])


def from_behind(block, axis, distance):
    devices = range(lax.axis_size(axis))
    route = [(i - distance, i) for i in devices if i - distance in devices]
    return lax.ppermute(block, axis, route)


def gather_flips(block, axis):
    found = {0: block}
    flip = lax.axis_size(axis) // 2
    while flip:
        for at, held in list(found.items()):
            found[at ^ flip] = swap(held, axis, flip)
        flip //= 2
    return [found[at] for at in range(lax.axis_size(axis))]


def norm_heads(flat, gain, heads):
    row_count = flat.shape[0]
    head_width = gain.shape[0]
    data = flat.astype(jnp.float32).reshape(row_count, heads, head_width)
    scaled = data * lax.rsqrt(jnp.mean(data * data, axis=-1, keepdims=True) + 1e-06) * gain
    return scaled.astype(jnp.bfloat16)


def attend(queries, keys, values, edge, query_gain, key_gain, sink_logits):
    head_width = query_gain.shape[0]
    row_count = queries.shape[0]
    q_heads = queries.shape[1] // head_width
    k_heads = keys.shape[1] // head_width
    group_size = q_heads // k_heads
    window_len = WINDOW
    block_count = row_count // window_len
    query_norm = norm_heads(queries, query_gain, q_heads)
    key_raw = jnp.concatenate([edge[:, : keys.shape[1]], keys], axis=0)
    key_all = norm_heads(key_raw, key_gain, k_heads).reshape(key_raw.shape)
    value_all = jnp.concatenate([edge[:, keys.shape[1] :], values], axis=0)

    def windows(flat):
        return jnp.concatenate(
            [
                flat[:row_count].reshape(block_count, window_len, k_heads, head_width),
                flat[window_len:].reshape(block_count, window_len, k_heads, head_width),
            ],
            axis=1,
        )

    key_blocks, value_blocks = windows(key_all), windows(value_all)
    query_blocks = query_norm.reshape(block_count, window_len, k_heads, group_size, head_width)
    scores = jnp.einsum(
        "nqhgd,nkhd->nhgqk", query_blocks, key_blocks, preferred_element_type=jnp.float32
    ) * head_width ** (-0.5)
    query_index = jnp.arange(window_len)[:, None]
    key_index = jnp.arange(2 * window_len)[None, :]
    offset_lag = window_len + query_index - key_index
    inband = (offset_lag >= 0) & (offset_lag < window_len)
    leading = (
        (jnp.arange(block_count)[:, None, None] > 0)
        | (key_index[None] >= window_len)
        | (lax.axis_index("sp") > 0)
    )
    valid = inband[None] & leading
    scores = jnp.where(valid[:, None, None], scores, -1e30)
    sink_rows = sink_logits.reshape(k_heads, group_size)[None, :, :, None]
    row_peak = jnp.maximum(jnp.max(scores, axis=-1), sink_rows)
    exp_terms = jnp.exp(scores - row_peak[..., None])
    denom_sum = jnp.sum(exp_terms, axis=-1) + jnp.exp(sink_rows - row_peak)
    weights = (exp_terms / denom_sum[..., None]).astype(jnp.bfloat16)
    attended = jnp.einsum(
        "nhgqk,nkhd->nqhgd", weights, value_blocks, preferred_element_type=jnp.float32
    ).astype(jnp.bfloat16)
    return attended.reshape(row_count, q_heads * head_width)


def permute_device(
    queries,
    keys,
    values,
    query_gain,
    key_gain,
    sink_logits,
    out_weight,
    residual,
    norm_gain,
    gate_weight,
    up_weight,
    down_weight,
):
    n_sp, n_tp = lax.axis_size("sp"), lax.axis_size("tp")
    sp, tp = lax.axis_index("sp"), lax.axis_index("tp")
    half = (sp // PAIR) % 2
    row_count, width = residual.shape
    depth, units = gate_weight.shape
    units //= 2

    def part(array, axis, flip):
        return lax.dynamic_slice_in_dim(array, (half ^ flip) * units, units, axis)

    far = list(range(2 * PAIR, n_sp, 2))

    def send(first, second, flips):
        found = {}
        for flip in flips:
            other = (flip // PAIR) % 2
            if second is None:
                piece = part(first, 0, other)
            else:
                piece = jnp.concatenate([part(first, 1, other), part(second, 1, other)], axis=1)
            found[flip] = swap(piece, "sp", flip) if flip else piece
        return found

    def relay(found, flips):
        for flip in flips:
            found[flip ^ 1] = swap(found[flip], "sp", 1)

    edge = jnp.concatenate([keys, values], axis=1)[row_count - WINDOW :]
    edge = from_behind(edge, "sp", 1)
    gate_weight, up_weight, residual, out_weight, edge = lax.optimization_barrier(
        (gate_weight, up_weight, residual, out_weight, edge)
    )
    near = [0, PAIR]
    first = far[: len(far) // 2]
    residual_pair = swap(residual, "sp", PAIR)
    both = send(gate_weight, up_weight, first)
    both.update(send(gate_weight, up_weight, near))
    attended = attend(queries, keys, values, edge, query_gain, key_gain, sink_logits)
    attended_pair = swap(attended, "sp", PAIR)

    gate_weight, up_weight, down_weight, attended_pair = lax.optimization_barrier(
        (gate_weight, up_weight, down_weight, attended_pair)
    )
    both.update(send(gate_weight, up_weight, far[len(far) // 2 :]))
    early = {flip: both[flip] for flip in first}
    down_weight, early = lax.optimization_barrier((down_weight, early))
    both.update(early)
    down = send(down_weight, None, far)
    down.update(send(down_weight, None, near))
    relay(both, near + far)
    relay(down, near)

    gains = jnp.concatenate(gather_flips(norm_gain, "tp"))
    projections = gather_flips(out_weight, "tp")
    stream = jnp.concatenate([residual, residual_pair], axis=0)
    stream = jnp.concatenate(gather_flips(stream, "tp"), axis=1).astype(jnp.float32)
    heads = gather_flips(jnp.concatenate([attended, attended_pair], axis=0), "tp")

    def own_first(columns):
        pieces = [
            lax.dynamic_slice_in_dim(columns, (tp ^ flip) * width, width, 1)
            for flip in range(n_tp)
        ]
        return jnp.concatenate(pieces, axis=1)

    projection = jnp.concatenate([own_first(piece) for piece in projections], axis=0)
    head = jnp.concatenate(heads, axis=1)
    mixed = jnp.dot(head, projection, preferred_element_type=jnp.float32)
    middle = (stream + mixed).astype(jnp.bfloat16)
    middle = lax.optimization_barrier(middle)
    middle_wide = middle.astype(jnp.float32)
    mean = jnp.mean(middle_wide * middle_wide, axis=1, keepdims=True)
    normed = (middle_wide * lax.rsqrt(mean + 1e-06) * gains).astype(jnp.bfloat16)

    late = {flip: down[flip] for flip in far}
    normed, late = lax.optimization_barrier((normed, late))
    down.update(late)
    relay(down, far)

    per_part = width // depth

    def place(flip):
        block = sp ^ flip
        return (((block // per_part) ^ tp) * per_part + block % per_part) * depth

    flips = range(n_sp)
    normed_in = jnp.concatenate(
        [lax.dynamic_slice_in_dim(normed, place(flip), depth, 1) for flip in flips], axis=1
    )
    gate_full = jnp.concatenate([both[flip][:, :units] for flip in flips], axis=0)
    up_full = jnp.concatenate([both[flip][:, units:] for flip in flips], axis=0)
    gate_acts = jnp.dot(normed_in, gate_full, preferred_element_type=jnp.float32)
    up_acts = jnp.dot(normed_in, up_full, preferred_element_type=jnp.float32)
    hidden = (jax.nn.silu(gate_acts) * up_acts).astype(jnp.bfloat16)

    down_full = jnp.zeros((units, width * n_tp), jnp.bfloat16)
    for flip in flips:
        down_full = lax.dynamic_update_slice_in_dim(down_full, down[flip], place(flip), 1)
    terms = [
        jnp.dot(
            hidden, down_full[:, at * width : (at + 1) * width], preferred_element_type=jnp.float32
        ).astype(jnp.bfloat16)
        for at in range(n_tp)
    ]

    def add(one, other):
        return one.astype(jnp.float32) + other.astype(jnp.float32)

    flip = 1
    held = dict(enumerate(terms))
    while flip < n_tp // 2:
        held = {
            at: add(held[at], swap(held[at ^ flip], "tp", flip)).astype(jnp.bfloat16)
            for at in held
            if not at & flip
        }
        flip *= 2
    own, other = held[0], held[flip]
    cut = width // 2
    across = add(own[:, :cut], swap(other[:, :cut], "tp", flip)).astype(jnp.bfloat16)
    left = add(across[:row_count], swap(across[row_count:], "sp", PAIR))
    pair = jnp.concatenate([own[:, cut:], other[:, cut:]], axis=1)
    pair = add(pair[:row_count], swap(pair[row_count:], "sp", PAIR)).astype(jnp.bfloat16)
    right = add(pair[:, : width - cut], swap(pair[:, width - cut :], "tp", flip))
    feed = jnp.concatenate([left, right], axis=1)
    return (middle_wide[:row_count, :width] + 0.5 * feed).astype(jnp.bfloat16)


def split_units(units):
    tiles = units // LANES
    small = (tiles // 2) * LANES
    return units - small, small


def scoped(name):
    def wrap(fn):
        def run(*args, **options):
            tags = [str(arg) for arg in args if isinstance(arg, (int, str))]
            with jax.named_scope("_".join([name, *tags])):
                return fn(*args, **options)

        return run

    return wrap


class Link:
    def __init__(self, sems, index):
        self.send, self.recv = sems[0].at[index], sems[1].at[index]

    def copy(self, src, dst, device):
        return pltpu.make_async_remote_copy(
            src_ref=src,
            dst_ref=dst,
            send_sem=self.send,
            recv_sem=self.recv,
            device_id=device,
            device_id_type=MESH,
        )


def layer_kernel(
    n_sp,
    n_tp,
    q_hbm,
    k_hbm,
    v_hbm,
    qg_ref,
    kg_ref,
    sink_ref,
    ow_hbm,
    res_hbm,
    ng_ref,
    gate_hbm,
    up_hbm,
    down_hbm,
    out_hbm,
    gt,
    ut,
    dn,
    mid,
    nrm,
    acc_g,
    acc_u,
    hid,
    pb,
    cb,
    xb,
    zs,
    zb,
    att,
    ow,
    gains,
    res,
    kn,
    vn,
    kh,
    q_ref,
    k_ref,
    v_ref,
    out_ref,
    send_sems,
    recv_sems,
    local_sems,
):
    s, t = lax.axis_index("sp"), lax.axis_index("tp")
    rows, width = res_hbm.shape
    depth, units = gate_hbm.shape
    big_units, small_units = split_units(units)
    window = WINDOW
    y = s % 2
    half = (s // PAIR) % 2
    is_big = (half + t) % 2 == 0
    core, far_tp = 1, n_tp // 2
    far = list(range(2 * PAIR, n_sp, PAIR))
    inner = (half + s // far[0]) % 2 == 1
    outer = jnp.logical_not(inner)
    soon = jnp.where(inner, far[1], far[0])
    late = jnp.where(inner, far[0], far[1])

    def flip_of(index, flip):
        out, bit = index, 1
        while bit <= flip:
            if flip & bit:
                out = out + bit - 2 * bit * ((index // bit) % 2)
            bit *= 2
        return out

    def xor(one, other, size):
        out, bit = 0, 1
        while bit < size:
            a, b = (one // bit) % 2, (other // bit) % 2
            out = out + bit * ((a + b) % 2)
            bit *= 2
        return out

    def sp_dev(flip):
        return {"sp": flip_of(s, flip)}

    def tp_dev(flip):
        return {"tp": flip_of(t, flip)}

    def sized(large, fn):
        if big_units == small_units:
            fn(big_units)
        else:
            pl.when(large)(lambda: fn(big_units))
            pl.when(jnp.logical_not(large))(lambda: fn(small_units))

    counter = [0]

    def new_link():
        counter[0] += 1
        return Link((send_sems, recv_sems), counter[0] - 1)

    ends = []

    locals_used = [0]

    def local(src, dst):
        locals_used[0] += 1
        return pltpu.make_async_copy(src, dst, local_sems.at[locals_used[0] - 1])

    kinds = {"g": (gate_hbm, gt), "u": (up_hbm, ut), "d": (down_hbm, dn)}
    counter[0] = len(kinds) * n_sp * PARTS
    step_depth = depth // PARTS

    def weight_link(kind, flip, cut):
        index = ("gud".index(kind) * n_sp + flip) * PARTS + cut
        return Link((send_sems, recv_sems), index)

    def slot(kind, flip, size, cut=None, seen_y=y):
        buf = kinds[kind][1]
        first, count = (0, depth) if cut is None else (cut * step_depth, step_depth)
        if kind == "d":
            return buf.at[flip, pl.ds(0, size), pl.ds(first, count)]
        start = ((seen_y + flip) % 2) * depth + first
        return buf.at[flip // 2, pl.ds(start, count), pl.ds(0, size)]

    def origin(kind, side, size, cut=None):
        ref = kinds[kind][0]
        first, count = (0, depth) if cut is None else (cut * step_depth, step_depth)
        start = pl.multiple_of(side * (units - size), LANES)
        if kind == "d":
            return ref.at[pl.ds(start, size), pl.ds(first, count)]
        return ref.at[pl.ds(first, count), pl.ds(start, size)]

    def own_copies(kind, flip):
        other = (flip // PAIR) % 2
        side = (half + other) % 2
        large = is_big if other == 0 else jnp.logical_not(is_big)

        def make(size, cut):
            return weight_link(kind, flip, cut).copy(
                origin(kind, side, size, cut),
                slot(kind, flip, size, cut, (y + flip) % 2),
                sp_dev(flip),
            )

        return large, make

    def send_own(kind, flip):
        large, make = own_copies(kind, flip)
        for cut in range(PARTS):
            sized(large, lambda size: make(size, cut).start())

    def drain_own(kind, flip):
        large, make = own_copies(kind, flip)
        for cut in range(PARTS):
            sized(large, lambda size: make(size, cut).wait_send())

    def wait_part(kind, flip, cut):
        def wait(size):
            at = slot(kind, flip, size, cut)
            weight_link(kind, flip, cut).copy(at, at, sp_dev(1)).wait_recv()

        sized(is_big, wait)

    @scoped("wait_weight")
    def wait_weight(kind, flip):
        for cut in range(PARTS):
            wait_part(kind, flip, cut)

    def relay_copy(kind, flip, size, cut):
        return weight_link(kind, flip + 1, cut).copy(
            slot(kind, flip, size, cut), slot(kind, flip + 1, size, cut, (y + 1) % 2), sp_dev(1)
        )

    @scoped("relay")
    def relay(kind, flip):
        for cut in range(PARTS):
            wait_part(kind, flip, cut)
            sized(is_big, lambda size: relay_copy(kind, flip, size, cut).start())

    def drain_relay(kind, flip):
        for cut in range(PARTS):
            sized(is_big, lambda size: relay_copy(kind, flip, size, cut).wait_send())

    def send(link, src, dst, device):
        copy = link.copy(src, dst, device)
        copy.start()
        ends.append(copy.wait_send)

    def wait(link, at):
        link.copy(at, at, tp_dev(core)).wait_recv()

    if big_units != small_units:

        @pl.when(jnp.logical_not(is_big))
        def _():
            pad = big_units - small_units
            zero = jnp.zeros((gt.shape[1], pad), jnp.bfloat16)
            for chunk in range(gt.shape[0]):
                gt[chunk, :, small_units:] = zero
                ut[chunk, :, small_units:] = zero
            for flip in range(n_sp):
                dn[flip, small_units:, :] = jnp.zeros((pad, depth), jnp.bfloat16)

    @pl.when(s == 0)
    def _():
        kh[...] = jnp.zeros_like(kh)

    qkv_loads = [local(q_hbm, q_ref), local(k_hbm, k_ref), local(v_hbm, v_ref)]
    for load in qkv_loads:
        load.start()

    barrier = pltpu.get_barrier_semaphore()
    sp_flips = [1, PAIR] + far
    tp_flips = list(range(1, n_tp))
    for flip in sp_flips:
        pl.semaphore_signal(barrier, inc=1, device_id=sp_dev(flip), device_id_type=MESH)
    for flip in tp_flips:
        pl.semaphore_signal(barrier, inc=1, device_id=tp_dev(flip), device_id_type=MESH)

    @pl.when(s + 1 < n_sp)
    def _():
        pl.semaphore_signal(barrier, inc=1, device_id={"sp": s + 1}, device_id_type=MESH)

    @pl.when(s > 0)
    def _():
        pl.semaphore_signal(barrier, inc=1, device_id={"sp": s - 1}, device_id_type=MESH)

    greeted = len(sp_flips) + len(tp_flips)
    edges = jnp.where(s > 0, 1, 0) + jnp.where(s + 1 < n_sp, 1, 0)
    with jax.named_scope("barrier"):
        pl.semaphore_wait(barrier, greeted + edges)

    halo = [new_link(), new_link()]
    last = pl.ds(rows - window, window)

    def halo_copy(at, ref):
        return halo[at].copy(ref.at[:, last], kh.at[at], {"sp": jnp.minimum(s + 1, n_sp - 1)})

    @pl.when(s + 1 < n_sp)
    def _():
        for at, ref in enumerate((k_hbm, v_hbm)):
            halo_copy(at, ref).start()

    own_loads = {}
    for kind in kinds:

        def load(kind=kind):
            index = locals_used[0]
            locals_used[0] += 1

            def make(size):
                return pltpu.make_async_copy(
                    origin(kind, half, size), slot(kind, 0, size), local_sems.at[index]
                )

            sized(is_big, lambda size: make(size).start())
            return lambda: sized(is_big, lambda size: make(size).wait())

        own_loads[kind] = load()
    for kind in kinds:
        send_own(kind, 1)
    for kind in "gu":
        send_own(kind, PAIR)
    pl.when(outer)(lambda: send_own("d", PAIR))

    @pl.when(inner)
    def _():
        for flip in reversed(far):
            for kind in "gu":
                send_own(kind, flip)
        for flip in far:
            send_own("d", flip)

    res_load = local(res_hbm, res)
    res_load.start()
    ow_links = {flip: new_link() for flip in tp_flips}
    gain_links = {flip: new_link() for flip in tp_flips}
    for flip in tp_flips:
        start = pl.multiple_of(flip_of(t, flip) * width, LANES)
        send(ow_links[flip], ow_hbm.at[:, pl.ds(start, width)], ow.at[flip], tp_dev(flip))
        send(gain_links[flip], ng_ref, gains.at[flip], tp_dev(flip))
    ow_load = local(ow_hbm.at[:, pl.ds(pl.multiple_of(t * width, LANES), width)], ow.at[0])
    ow_load.start()
    gains[0] = ng_ref[...]

    head_width = qg_ref.shape[1]
    heads = q_ref.shape[1] // head_width
    blocks = rows // window
    scale = head_width ** (-0.5)

    def unit_norm(data, gain):
        data = data.astype(jnp.float32)
        mean = jnp.mean(data * data, axis=-1, keepdims=True)
        return (data * lax.rsqrt(mean + EPS) * gain).astype(jnp.bfloat16)

    def turn(block):
        return block.astype(jnp.float32).T

    for load in qkv_loads:
        load.wait()

    def norm_keys(at, _):
        here = pl.ds(pl.multiple_of(at * window, window), window)
        there = pl.ds(pl.multiple_of((at + 1) * window, window), window)
        kn[there, :] = unit_norm(turn(k_ref[:, here]), kg_ref[...])
        vn[there, :] = turn(v_ref[:, here]).astype(jnp.bfloat16)
        return 0

    lax.fori_loop(0, blocks, norm_keys, 0)

    def attend_block(at, _):
        here = pl.ds(pl.multiple_of(at * window, window), window)
        both = pl.ds(pl.multiple_of(at * window, window), 2 * window)
        keys, values = kn[both, :], vn[both, :]
        raw = q_ref[here, :]
        query_index = lax.broadcasted_iota(jnp.int32, (window, 2 * window), 0)
        key_index = lax.broadcasted_iota(jnp.int32, (window, 2 * window), 1)
        lag = window + query_index - key_index
        first = jnp.where(s * blocks + at > 0, 0, window)
        valid = (lag >= 0) & (lag < window) & (key_index >= first)
        pieces = []
        for head in range(heads):
            query = unit_norm(raw[:, head * head_width : (head + 1) * head_width], qg_ref[...])
            scores = lax.dot_general(
                query, keys, (((1,), (1,)), ((), ())), preferred_element_type=jnp.float32
            )
            scores = jnp.where(valid, scores * scale, -1e30)
            sink = sink_ref[0, head]
            peak = jnp.maximum(jnp.max(scores, axis=-1, keepdims=True), sink)
            terms = jnp.exp(scores - peak)
            total = jnp.sum(terms, axis=-1, keepdims=True) + jnp.exp(sink - peak)
            weights = (terms / total).astype(jnp.bfloat16)
            piece = jnp.dot(weights, values, preferred_element_type=jnp.float32)
            pieces.append(piece.astype(jnp.bfloat16))
        att[0, here, :] = jnp.concatenate(pieces, axis=1)
        return 0

    with jax.named_scope("attend"):
        lax.fori_loop(1, blocks, attend_block, 0)

    @pl.when(s > 0)
    def _():
        for at in range(2):
            halo[at].copy(kh.at[at], kh.at[at], {"sp": jnp.maximum(s - 1, 0)}).wait_recv()

    kn[0:window, :] = unit_norm(turn(kh[0]), kg_ref[...])
    vn[0:window, :] = turn(kh[1]).astype(jnp.bfloat16)
    with jax.named_scope("attend_first"):
        lax.fori_loop(0, 1, attend_block, 0)

    att_links = {flip: new_link() for flip in tp_flips}
    send(att_links[far_tp], att.at[0], att.at[far_tp], tp_dev(far_tp))
    send(att_links[core], att.at[0], att.at[core], tp_dev(core))

    with jax.named_scope("wait_att"):
        wait(att_links[far_tp], att.at[far_tp])
    send(att_links[far_tp ^ core], att.at[far_tp], att.at[far_tp ^ core], tp_dev(core))

    for flip in tp_flips:
        with jax.named_scope("wait_ow"):
            wait(ow_links[flip], ow.at[flip])
        wait(gain_links[flip], gains.at[flip])
    ow_load.wait()
    res_load.wait()
    wait(att_links[core], att.at[core])
    wait(att_links[far_tp ^ core], att.at[far_tp ^ core])

    def project(at, _):
        here = pl.ds(pl.multiple_of(at * window, window), window)
        mixed = jnp.zeros((window, width), jnp.float32)
        for flip in range(n_tp):
            product = jnp.dot(att[flip, here, :], ow[flip], preferred_element_type=jnp.float32)
            mixed = mixed + product.astype(jnp.bfloat16).astype(jnp.float32)
        mid[0, 0, here, :] = (res[here, :].astype(jnp.float32) + mixed).astype(jnp.bfloat16)
        return 0

    cuts = 2
    piece = rows // cuts
    mid_links = {
        (side, flip, cut): new_link()
        for side in range(2)
        for flip in range(n_tp)
        for cut in range(cuts)
        if side or flip
    }

    def part(side, flip, cut):
        return mid.at[side, flip, pl.ds(cut * piece, piece), :]

    mid_ends = {}

    def pass_mid(side, flip, cut, to_side, to_flip, device_of, hop):
        def make():
            return mid_links[to_side, to_flip, cut].copy(
                part(side, flip, cut), part(to_side, to_flip, cut), device_of(hop)
            )

        make().start()
        mid_ends[to_side, to_flip, cut] = lambda: make().wait_send()

    @scoped("wait_mid")
    def wait_mid(side, flip, cut):
        wait(mid_links[side, flip, cut], part(side, flip, cut))

    with jax.named_scope("project"):
        lax.fori_loop(0, blocks, project, 0)
    for cut in range(cuts):
        pass_mid(0, 0, cut, 1, 0, sp_dev, PAIR)
        pass_mid(0, 0, cut, 0, far_tp, tp_dev, far_tp)
        pass_mid(0, 0, cut, 0, core, tp_dev, core)

    norm_rows = 64

    @scoped("normalise")
    def normalise(side):
        def step(at, _):
            here = pl.ds(pl.multiple_of(at * norm_rows, norm_rows), norm_rows)
            total = jnp.zeros((norm_rows, 1), jnp.float32)
            for flip in range(n_tp):
                data = mid[side, flip, here, :].astype(jnp.float32)
                total = total + jnp.sum(data * data, axis=1, keepdims=True)
            factor = lax.rsqrt(total / (width * n_tp) + EPS)
            for flip in range(n_tp):
                data = mid[side, flip, here, :].astype(jnp.float32)
                nrm[side, flip, here, :] = (data * factor * gains[flip]).astype(jnp.bfloat16)
            return 0

        lax.fori_loop(0, rows // norm_rows, step, 0)

    pl.when(inner)(lambda: send_own("d", PAIR))

    @pl.when(outer)
    def _():
        for flip in far:
            for kind in "gu":
                send_own(kind, flip)
        for flip in far:
            send_own("d", flip)

    tile = 256
    n_chunks = n_sp // 2
    z = s // 2

    @scoped("expand")
    def expand(chunk, side, first=False, last=False, flip=None):
        at_slot = xor(xor(z, chunk, n_chunks), t, n_chunks)
        if flip is None:
            part = pl.ds(0, 2 * depth)
        else:
            part = pl.ds(pl.multiple_of(((y + flip) % 2) * depth, depth), depth)

        def step(at, _):
            here = pl.ds(pl.multiple_of(at * tile, tile), tile)
            there = pl.ds(pl.multiple_of(side * rows + at * tile, tile), tile)
            data = nrm[side, at_slot, here, part]
            gate = jnp.dot(data, gt[chunk, part, :], preferred_element_type=jnp.float32)
            up = jnp.dot(data, ut[chunk, part, :], preferred_element_type=jnp.float32)
            if not first:
                gate = gate + acc_g[there, :]
                up = up + acc_u[there, :]
            if not last:
                acc_g[there, :] = gate
                acc_u[there, :] = up
            else:
                hid[there, :] = (gate / (1.0 + jnp.exp(-gate)) * up).astype(jnp.bfloat16)
            return 0

        lax.fori_loop(0, rows // tile, step, 0)

    def wait_beside(flip):
        for kind in "gu":
            wait_weight(kind, flip + 1)

    def spread(cut):
        wait_mid(1, 0, cut)
        pass_mid(1, 0, cut, 1, far_tp, tp_dev, far_tp)
        pass_mid(1, 0, cut, 1, core, tp_dev, core)

    for kind in "gu":
        relay(kind, PAIR)
    for kind in "gu":
        relay(kind, soon)
    for cut in range(cuts):
        wait_mid(0, far_tp, cut)
        pass_mid(0, far_tp, cut, 0, far_tp ^ core, tp_dev, core)
    @pl.when(inner)
    def _():
        for cut in range(cuts):
            spread(cut)
        relay("d", PAIR)

    pl.when(outer)(lambda: relay("d", far[0]))
    for cut in range(cuts):
        wait_mid(0, core, cut)
        wait_mid(0, far_tp ^ core, cut)
    normalise(0)
    own_loads["g"]()
    own_loads["u"]()
    wait_beside(0)
    expand(0, 0, True)
    pl.when(outer)(lambda: spread(0))
    wait_beside(PAIR)
    expand(1, 0)
    pl.when(inner)(lambda: relay("g", late))
    pl.when(outer)(lambda: spread(1))
    wait_beside(soon)
    expand(soon // 2, 0)
    pl.when(inner)(lambda: relay("u", late))
    for cut in range(cuts):
        wait_mid(1, far_tp, cut)
        pass_mid(1, far_tp, cut, 1, far_tp ^ core, tp_dev, core)
        if cut == 0:
            pl.when(outer)(lambda: relay("g", late))
    for cut in range(cuts):
        wait_mid(1, core, cut)
        wait_mid(1, far_tp ^ core, cut)
    normalise(1)
    expand(0, 1, True)
    pl.when(outer)(lambda: relay("u", late))
    expand(1, 1)
    expand(soon // 2, 1)
    for side in range(2):
        expand(late // 2, side, flip=late)
    pl.when(outer)(lambda: relay("d", PAIR))
    wait_beside(late)
    for side in range(2):
        expand(late // 2, side, last=True, flip=late + 1)

    core_links = counter[0]
    x_links = core_links + 2 * n_sp
    z_links = x_links + 4
    counter[0] += 2 * n_sp + 8
    my_end = (t // far_tp + t) % 2 == 0
    not_end = jnp.logical_not(my_end)

    def link(index):
        return Link((send_sems, recv_sems), index)

    def role_of(flip):
        return xor(xor(z, flip // 2, n_chunks), t, n_chunks)

    def side_rows(side):
        return pl.ds(side * rows, rows)

    def core_copy(flip, side):
        some = side_rows(side)
        return link(core_links + 2 * flip + side).copy(
            pb.at[flip, some, :], cb.at[flip, some, :], tp_dev(core)
        )

    def x_copy(flip, block, side):
        some = side_rows(side)
        return link(x_links + 2 * block + side).copy(
            pb.at[flip, some, :], xb.at[block, some, :], tp_dev(far_tp)
        )

    def z_copy(place, block):
        return link(z_links + 2 * place + block).copy(
            zs.at[place, block], zb.at[place, block], sp_dev(PAIR)
        )

    def over_rows(fn):
        def step(at, _):
            fn(pl.multiple_of(at * tile, tile))
            return 0

        lax.fori_loop(0, rows // tile, step, 0)

    def wide(ref, *index):
        return ref[index].astype(jnp.float32)

    def at_side(side, base):
        return pl.ds(pl.multiple_of(side * rows + base, tile), tile)

    @scoped("shrink")
    def shrink(flip):
        for side in (1, 0):

            def step(base, side=side):
                here = at_side(side, base)
                product = jnp.dot(hid[here, :], dn[flip], preferred_element_type=jnp.float32)
                pb[flip, here, :] = product.astype(jnp.bfloat16)

            over_rows(step)
            pl.when(role_of(flip) % 2 == 1)(lambda: core_copy(flip, side).start())

    def give_pair(place, flip, block, with_x):
        core_copy(flip, 1).wait_recv()
        if with_x:
            x_copy(flip, block, 1).wait_recv()

        def step(base):
            there = at_side(1, base)
            held = wide(pb, flip, there) + wide(cb, flip, there)
            if with_x:
                held = held + wide(xb, block, there)
            zs[place, block, pl.ds(base, tile), :] = held.astype(jnp.bfloat16)

        over_rows(step)
        z_copy(place, block).start()

    @scoped("collect")
    def collect(flip):
        role = role_of(flip)
        block = (y + flip) % 2

        @pl.when(jnp.logical_and(role == far_tp, my_end))
        def _():
            for side in (1, 0):
                core_copy(flip, side).wait_recv()

                def step(base, side=side):
                    here = at_side(side, base)
                    held = wide(pb, flip, here) + wide(cb, flip, here)
                    pb[flip, here, :] = held.astype(jnp.bfloat16)

                over_rows(step)
                x_copy(flip, block, side).start()

        pl.when(jnp.logical_and(role == far_tp, not_end))(lambda: give_pair(1, flip, block, False))
        pl.when(jnp.logical_and(role == 0, my_end))(lambda: give_pair(0, flip, block, False))

    mine = xor(z, t, n_chunks)
    theirs = xor(mine, far_tp, n_chunks)

    def second_theirs(beside):
        flip, block = 2 * theirs + beside, (y + beside) % 2
        z_copy(1, block).wait_recv()
        core_copy(flip, 0).wait_recv()

        def step(base):
            here = pl.ds(base, tile)
            held = wide(pb, flip, here) + wide(cb, flip, here) + wide(zb, 1, block, here)
            pb[flip, here, :] = held.astype(jnp.bfloat16)

        over_rows(step)
        x_copy(flip, block, 0).start()

    def down(flip):
        if not (isinstance(flip, int) and flip in (0, PAIR)):
            wait_weight("d", flip)
        shrink(flip)

    def first_relay():
        pl.when(inner)(lambda: relay("d", far[0]))
        pl.when(outer)(lambda: relay("d", far[1]))

    def second_relay():
        pl.when(inner)(lambda: relay("d", far[1]))

    own_loads["d"]()
    far_foreign = t // far_tp == z // far_tp

    @pl.when(jnp.logical_not(far_foreign))
    def _():
        down(0)
        first_relay()
        down(1)
        collect(0)
        down(PAIR)
        collect(1)
        down(PAIR + 1)
        collect(PAIR)
        shrink(far[0])
        collect(PAIR + 1)
        down(far[0] + 1)
        collect(far[0])
        second_relay()
        shrink(far[1])
        collect(far[0] + 1)

        @pl.when(not_end)
        def _():
            with jax.named_scope("theirs_near"):
                for beside in range(2):
                    second_theirs(beside)

        collect(far[1])
        down(far[1] + 1)
        collect(far[1] + 1)

        @pl.when(not_end)
        def _():
            with jax.named_scope("mine_far"):
                for beside in range(2):
                    give_pair(0, 2 * mine + beside, (y + beside) % 2, True)

    @pl.when(far_foreign)
    def _():
        down(0)
        first_relay()
        shrink(far[0])
        collect(0)
        down(1)
        collect(far[0])
        down(PAIR)
        collect(1)
        down(PAIR + 1)
        collect(PAIR)
        down(far[0] + 1)
        collect(PAIR + 1)
        second_relay()
        shrink(far[1])
        collect(far[0] + 1)
        collect(far[1])
        down(far[1] + 1)
        collect(far[1] + 1)

        @pl.when(not_end)
        def _():
            with jax.named_scope("mine_near"):
                for beside in range(2):
                    give_pair(0, 2 * mine + beside, (y + beside) % 2, True)
            with jax.named_scope("theirs_far"):
                for beside in range(2):
                    second_theirs(beside)

    out_copies = []
    for beside in range(2):
        flip, block = 2 * mine + beside, (y + beside) % 2
        with jax.named_scope("wait_z"):
            core_copy(flip, 0).wait_recv()
            z_copy(0, block).wait_recv()
        with jax.named_scope("wait_x"):
            x_copy(flip, block, 0).wait_recv()
        columns = pl.ds(pl.multiple_of(block * depth, depth), depth)

        def finish(base, flip=flip, block=block, columns=columns):
            here = pl.ds(base, tile)
            feed = wide(pb, flip, here) + wide(cb, flip, here) + wide(zb, 0, block, here)
            feed = feed + wide(xb, block, here)
            out_ref[here, columns] = (wide(mid, 0, 0, here, columns) + 0.5 * feed).astype(jnp.bfloat16)

        over_rows(finish)
        out_copies.append(local(out_ref.at[:, columns], out_hbm.at[:, columns]))
        out_copies[-1].start()

    with jax.named_scope("ends"):
        for copy in out_copies:
            copy.wait()
        for end in [*ends, *mid_ends.values()]:
            end()
        for kind in kinds:
            for flip in [1, PAIR] + far:
                drain_own(kind, flip)
            for flip in [PAIR] + far:
                drain_relay(kind, flip)
        for flip in range(n_sp):
            for side in range(2):
                pl.when(role_of(flip) % 2 == 1)(lambda: core_copy(flip, side).wait_send())
        for beside in range(2):
            flip, block = 2 * theirs + beside, (y + beside) % 2
            x_copy(flip, block, 0).wait_send()
            pl.when(my_end)(lambda: x_copy(flip, block, 1).wait_send())
            z_copy(0, block).wait_send()
            pl.when(not_end)(lambda: z_copy(1, block).wait_send())

    @pl.when(s + 1 < n_sp)
    def _():
        for at, ref in enumerate((k_hbm, v_hbm)):
            halo_copy(at, ref).wait_send()


def kernel_device(
    queries,
    keys,
    values,
    query_gain,
    key_gain,
    sink_logits,
    out_weight,
    residual,
    norm_gain,
    gate_weight,
    up_weight,
    down_weight,
):
    n_sp, n_tp = lax.axis_size("sp"), lax.axis_size("tp")
    rows, width = residual.shape
    depth, units = gate_weight.shape
    big, _ = split_units(units)
    heads_width = queries.shape[1]
    head_width = query_gain.shape[0]
    bf16, f32 = jnp.bfloat16, jnp.float32
    vmem = pl.BlockSpec(memory_space=pltpu.VMEM)
    smem = pl.BlockSpec(memory_space=pltpu.SMEM)
    hbm = pl.BlockSpec(memory_space=pl.ANY)
    n_links = 97
    scratch = [
        pltpu.VMEM((n_sp // 2, 2 * depth, big), bf16),
        pltpu.VMEM((n_sp // 2, 2 * depth, big), bf16),
        pltpu.VMEM((n_sp, big, depth), bf16),
        pltpu.VMEM((2, n_tp, rows, width), bf16),
        pltpu.VMEM((2, n_tp, rows, width), bf16),
        pltpu.VMEM((2 * rows, big), f32),
        pltpu.VMEM((2 * rows, big), f32),
        pltpu.VMEM((2 * rows, big), bf16),
        pltpu.VMEM((n_sp, 2 * rows, depth), bf16),
        pltpu.VMEM((n_sp, 2 * rows, depth), bf16),
        pltpu.VMEM((2, 2 * rows, depth), bf16),
        pltpu.VMEM((2, 2, rows, depth), bf16),
        pltpu.VMEM((2, 2, rows, depth), bf16),
        pltpu.VMEM((n_tp, rows, heads_width), bf16),
        pltpu.VMEM((n_tp, heads_width, width), bf16),
        pltpu.VMEM((n_tp, 1, width), f32),
        pltpu.VMEM((rows, width), bf16),
        pltpu.VMEM((rows + WINDOW, head_width), bf16),
        pltpu.VMEM((rows + WINDOW, head_width), bf16),
        pltpu.VMEM((2, head_width, WINDOW), bf16),
        pltpu.VMEM((rows, heads_width), bf16),
        pltpu.VMEM((head_width, rows), bf16),
        pltpu.VMEM((head_width, rows), bf16),
        pltpu.VMEM((rows, width), bf16),
        pltpu.SemaphoreType.DMA((n_links,)),
        pltpu.SemaphoreType.DMA((n_links,)),
        pltpu.SemaphoreType.DMA((16,)),
    ]
    return pl.pallas_call(
        functools.partial(layer_kernel, n_sp, n_tp),
        out_shape=jax.ShapeDtypeStruct((rows, width), bf16),
        in_specs=[hbm, hbm, hbm, vmem, vmem, smem, hbm, hbm, vmem, hbm, hbm, hbm],
        out_specs=hbm,
        scratch_shapes=scratch,
        compiler_params=pltpu.CompilerParams(
            collective_id=0, has_side_effects=True, vmem_limit_bytes=66 * 1000 * 1000
        ),
    )(
        queries,
        keys.T,
        values.T,
        query_gain[None],
        key_gain[None],
        sink_logits[None],
        out_weight,
        residual,
        norm_gain[None],
        gate_weight,
        up_weight,
        down_weight,
    )


def per_device(*args):
    queries, keys, query_gain, residual, gate_weight = args[0], args[1], args[3], args[7], args[9]
    n_sp, n_tp = lax.axis_size("sp"), lax.axis_size("tp")
    depth, units = gate_weight.shape
    rows, width = residual.shape
    fits = (
        depth % LANES == 0
        and units % LANES == 0
        and rows % (2 * LANES) == 0
        and width == 2 * depth
        and n_sp == 2 * n_tp
        and n_tp // 2 == PAIR
        and n_sp % (2 * PAIR) == 0
        and keys.shape[1] == query_gain.shape[0]
    )
    return kernel_device(*args) if fits else permute_device(*args)


def solution(mesh):
    in_specs = (
        P("sp", "tp"),
        P("sp", "tp"),
        P("sp", "tp"),
        P(),
        P(),
        P("tp"),
        P("tp", None),
        P("sp", "tp"),
        P("tp"),
        P("sp", "tp"),
        P("sp", "tp"),
        P("tp", "sp"),
    )
    out_specs = P("sp", "tp")
    return jax.shard_map(
        per_device, mesh=mesh, in_specs=in_specs, out_specs=out_specs, check_vma=False
    )
```

```python
import functools

import jax
import jax.numpy as jnp
from jax import lax
from jax.experimental import pallas as pl
from jax.experimental.pallas import tpu as pltpu
from jax.sharding import PartitionSpec as P

WINDOW = 128
PAIR = 2
LANES = 128
PARTS = 2
EPS = 1e-06
MESH = pl.DeviceIdType.MESH


def swap(block, axis, flip):
    return lax.ppermute(block, axis, [(i, i ^ flip) for i in range(lax.axis_size(axis))])


def from_behind(block, axis, distance):
    devices = range(lax.axis_size(axis))
    route = [(i - distance, i) for i in devices if i - distance in devices]
    return lax.ppermute(block, axis, route)


def gather_flips(block, axis):
    found = {0: block}
    flip = lax.axis_size(axis) // 2
    while flip:
        for at, held in list(found.items()):
            found[at ^ flip] = swap(held, axis, flip)
        flip //= 2
    return [found[at] for at in range(lax.axis_size(axis))]


def norm_heads(flat, gain, heads):
    row_count = flat.shape[0]
    head_width = gain.shape[0]
    data = flat.astype(jnp.float32).reshape(row_count, heads, head_width)
    scaled = data * lax.rsqrt(jnp.mean(data * data, axis=-1, keepdims=True) + 1e-06) * gain
    return scaled.astype(jnp.bfloat16)


def attend(queries, keys, values, edge, query_gain, key_gain, sink_logits):
    head_width = query_gain.shape[0]
    row_count = queries.shape[0]
    q_heads = queries.shape[1] // head_width
    k_heads = keys.shape[1] // head_width
    group_size = q_heads // k_heads
    window_len = WINDOW
    block_count = row_count // window_len
    query_norm = norm_heads(queries, query_gain, q_heads)
    key_raw = jnp.concatenate([edge[:, : keys.shape[1]], keys], axis=0)
    key_all = norm_heads(key_raw, key_gain, k_heads).reshape(key_raw.shape)
    value_all = jnp.concatenate([edge[:, keys.shape[1] :], values], axis=0)

    def windows(flat):
        return jnp.concatenate(
            [
                flat[:row_count].reshape(block_count, window_len, k_heads, head_width),
                flat[window_len:].reshape(block_count, window_len, k_heads, head_width),
            ],
            axis=1,
        )

    key_blocks, value_blocks = windows(key_all), windows(value_all)
    query_blocks = query_norm.reshape(block_count, window_len, k_heads, group_size, head_width)
    scores = jnp.einsum(
        "nqhgd,nkhd->nhgqk", query_blocks, key_blocks, preferred_element_type=jnp.float32
    ) * head_width ** (-0.5)
    query_index = jnp.arange(window_len)[:, None]
    key_index = jnp.arange(2 * window_len)[None, :]
    offset_lag = window_len + query_index - key_index
    inband = (offset_lag >= 0) & (offset_lag < window_len)
    leading = (
        (jnp.arange(block_count)[:, None, None] > 0)
        | (key_index[None] >= window_len)
        | (lax.axis_index("sp") > 0)
    )
    valid = inband[None] & leading
    scores = jnp.where(valid[:, None, None], scores, -1e30)
    sink_rows = sink_logits.reshape(k_heads, group_size)[None, :, :, None]
    row_peak = jnp.maximum(jnp.max(scores, axis=-1), sink_rows)
    exp_terms = jnp.exp(scores - row_peak[..., None])
    denom_sum = jnp.sum(exp_terms, axis=-1) + jnp.exp(sink_rows - row_peak)
    weights = (exp_terms / denom_sum[..., None]).astype(jnp.bfloat16)
    attended = jnp.einsum(
        "nhgqk,nkhd->nqhgd", weights, value_blocks, preferred_element_type=jnp.float32
    ).astype(jnp.bfloat16)
    return attended.reshape(row_count, q_heads * head_width)


def permute_device(
    queries,
    keys,
    values,
    query_gain,
    key_gain,
    sink_logits,
    out_weight,
    residual,
    norm_gain,
    gate_weight,
    up_weight,
    down_weight,
):
    n_sp, n_tp = lax.axis_size("sp"), lax.axis_size("tp")
    sp, tp = lax.axis_index("sp"), lax.axis_index("tp")
    half = (sp // PAIR) % 2
    row_count, width = residual.shape
    depth, units = gate_weight.shape
    units //= 2

    def part(array, axis, flip):
        return lax.dynamic_slice_in_dim(array, (half ^ flip) * units, units, axis)

    far = list(range(2 * PAIR, n_sp, 2))

    def send(first, second, flips):
        found = {}
        for flip in flips:
            other = (flip // PAIR) % 2
            if second is None:
                piece = part(first, 0, other)
            else:
                piece = jnp.concatenate([part(first, 1, other), part(second, 1, other)], axis=1)
            found[flip] = swap(piece, "sp", flip) if flip else piece
        return found

    def relay(found, flips):
        for flip in flips:
            found[flip ^ 1] = swap(found[flip], "sp", 1)

    edge = jnp.concatenate([keys, values], axis=1)[row_count - WINDOW :]
    edge = from_behind(edge, "sp", 1)
    gate_weight, up_weight, residual, out_weight, edge = lax.optimization_barrier(
        (gate_weight, up_weight, residual, out_weight, edge)
    )
    near = [0, PAIR]
    first = far[: len(far) // 2]
    residual_pair = swap(residual, "sp", PAIR)
    both = send(gate_weight, up_weight, first)
    both.update(send(gate_weight, up_weight, near))
    attended = attend(queries, keys, values, edge, query_gain, key_gain, sink_logits)
    attended_pair = swap(attended, "sp", PAIR)

    gate_weight, up_weight, down_weight, attended_pair = lax.optimization_barrier(
        (gate_weight, up_weight, down_weight, attended_pair)
    )
    both.update(send(gate_weight, up_weight, far[len(far) // 2 :]))
    early = {flip: both[flip] for flip in first}
    down_weight, early = lax.optimization_barrier((down_weight, early))
    both.update(early)
    down = send(down_weight, None, far)
    down.update(send(down_weight, None, near))
    relay(both, near + far)
    relay(down, near)

    gains = jnp.concatenate(gather_flips(norm_gain, "tp"))
    projections = gather_flips(out_weight, "tp")
    stream = jnp.concatenate([residual, residual_pair], axis=0)
    stream = jnp.concatenate(gather_flips(stream, "tp"), axis=1).astype(jnp.float32)
    heads = gather_flips(jnp.concatenate([attended, attended_pair], axis=0), "tp")

    def own_first(columns):
        pieces = [
            lax.dynamic_slice_in_dim(columns, (tp ^ flip) * width, width, 1)
            for flip in range(n_tp)
        ]
        return jnp.concatenate(pieces, axis=1)

    projection = jnp.concatenate([own_first(piece) for piece in projections], axis=0)
    head = jnp.concatenate(heads, axis=1)
    mixed = jnp.dot(head, projection, preferred_element_type=jnp.float32)
    middle = (stream + mixed).astype(jnp.bfloat16)
    middle = lax.optimization_barrier(middle)
    middle_wide = middle.astype(jnp.float32)
    mean = jnp.mean(middle_wide * middle_wide, axis=1, keepdims=True)
    normed = (middle_wide * lax.rsqrt(mean + 1e-06) * gains).astype(jnp.bfloat16)

    late = {flip: down[flip] for flip in far}
    normed, late = lax.optimization_barrier((normed, late))
    down.update(late)
    relay(down, far)

    per_part = width // depth

    def place(flip):
        block = sp ^ flip
        return (((block // per_part) ^ tp) * per_part + block % per_part) * depth

    flips = range(n_sp)
    normed_in = jnp.concatenate(
        [lax.dynamic_slice_in_dim(normed, place(flip), depth, 1) for flip in flips], axis=1
    )
    gate_full = jnp.concatenate([both[flip][:, :units] for flip in flips], axis=0)
    up_full = jnp.concatenate([both[flip][:, units:] for flip in flips], axis=0)
    gate_acts = jnp.dot(normed_in, gate_full, preferred_element_type=jnp.float32)
    up_acts = jnp.dot(normed_in, up_full, preferred_element_type=jnp.float32)
    hidden = (jax.nn.silu(gate_acts) * up_acts).astype(jnp.bfloat16)

    down_full = jnp.zeros((units, width * n_tp), jnp.bfloat16)
    for flip in flips:
        down_full = lax.dynamic_update_slice_in_dim(down_full, down[flip], place(flip), 1)
    terms = [
        jnp.dot(
            hidden, down_full[:, at * width : (at + 1) * width], preferred_element_type=jnp.float32
        ).astype(jnp.bfloat16)
        for at in range(n_tp)
    ]

    def add(one, other):
        return one.astype(jnp.float32) + other.astype(jnp.float32)

    flip = 1
    held = dict(enumerate(terms))
    while flip < n_tp // 2:
        held = {
            at: add(held[at], swap(held[at ^ flip], "tp", flip)).astype(jnp.bfloat16)
            for at in held
            if not at & flip
        }
        flip *= 2
    own, other = held[0], held[flip]
    cut = width // 2
    across = add(own[:, :cut], swap(other[:, :cut], "tp", flip)).astype(jnp.bfloat16)
    left = add(across[:row_count], swap(across[row_count:], "sp", PAIR))
    pair = jnp.concatenate([own[:, cut:], other[:, cut:]], axis=1)
    pair = add(pair[:row_count], swap(pair[row_count:], "sp", PAIR)).astype(jnp.bfloat16)
    right = add(pair[:, : width - cut], swap(pair[:, width - cut :], "tp", flip))
    feed = jnp.concatenate([left, right], axis=1)
    return (middle_wide[:row_count, :width] + 0.5 * feed).astype(jnp.bfloat16)


def split_units(units):
    tiles = units // LANES
    small = (tiles // 2) * LANES
    return units - small, small


def scoped(name):
    def wrap(fn):
        def run(*args, **options):
            tags = [str(arg) for arg in args if isinstance(arg, (int, str))]
            with jax.named_scope("_".join([name, *tags])):
                return fn(*args, **options)

        return run

    return wrap


class Link:
    def __init__(self, sems, index):
        self.send, self.recv = sems[0].at[index], sems[1].at[index]

    def copy(self, src, dst, device):
        return pltpu.make_async_remote_copy(
            src_ref=src,
            dst_ref=dst,
            send_sem=self.send,
            recv_sem=self.recv,
            device_id=device,
            device_id_type=MESH,
        )


def layer_kernel(
    n_sp,
    n_tp,
    q_hbm,
    k_hbm,
    v_hbm,
    qg_ref,
    kg_ref,
    sink_ref,
    ow_hbm,
    res_hbm,
    ng_ref,
    gate_hbm,
    up_hbm,
    down_hbm,
    out_hbm,
    gt,
    ut,
    dn,
    mid,
    nrm,
    acc_g,
    acc_u,
    hid,
    pb,
    cb,
    xb,
    zs,
    zb,
    att,
    ow,
    gains,
    res,
    kn,
    vn,
    kh,
    q_ref,
    k_ref,
    v_ref,
    out_ref,
    send_sems,
    recv_sems,
    local_sems,
):
    s, t = lax.axis_index("sp"), lax.axis_index("tp")
    rows, width = res_hbm.shape
    depth, units = gate_hbm.shape
    big_units, small_units = split_units(units)
    window = WINDOW
    y = s % 2
    half = (s // PAIR) % 2
    is_big = (half + t) % 2 == 0
    core, far_tp = 1, n_tp // 2
    far = list(range(2 * PAIR, n_sp, PAIR))
    inner = (half + s // far[0]) % 2 == 1
    outer = jnp.logical_not(inner)
    soon = jnp.where(inner, far[1], far[0])
    late = jnp.where(inner, far[0], far[1])

    def flip_of(index, flip):
        out, bit = index, 1
        while bit <= flip:
            if flip & bit:
                out = out + bit - 2 * bit * ((index // bit) % 2)
            bit *= 2
        return out

    def xor(one, other, size):
        out, bit = 0, 1
        while bit < size:
            a, b = (one // bit) % 2, (other // bit) % 2
            out = out + bit * ((a + b) % 2)
            bit *= 2
        return out

    def sp_dev(flip):
        return {"sp": flip_of(s, flip)}

    def tp_dev(flip):
        return {"tp": flip_of(t, flip)}

    def sized(large, fn):
        if big_units == small_units:
            fn(big_units)
        else:
            pl.when(large)(lambda: fn(big_units))
            pl.when(jnp.logical_not(large))(lambda: fn(small_units))

    counter = [0]

    def new_link():
        counter[0] += 1
        return Link((send_sems, recv_sems), counter[0] - 1)

    ends = []

    locals_used = [0]

    def local(src, dst):
        locals_used[0] += 1
        return pltpu.make_async_copy(src, dst, local_sems.at[locals_used[0] - 1])

    kinds = {"g": (gate_hbm, gt), "u": (up_hbm, ut), "d": (down_hbm, dn)}
    counter[0] = len(kinds) * n_sp * PARTS
    step_depth = depth // PARTS

    def weight_link(kind, flip, cut):
        index = ("gud".index(kind) * n_sp + flip) * PARTS + cut
        return Link((send_sems, recv_sems), index)

    def slot(kind, flip, size, cut=None, seen_y=y):
        buf = kinds[kind][1]
        first, count = (0, depth) if cut is None else (cut * step_depth, step_depth)
        if kind == "d":
            return buf.at[flip, pl.ds(0, size), pl.ds(first, count)]
        start = ((seen_y + flip) % 2) * depth + first
        return buf.at[flip // 2, pl.ds(start, count), pl.ds(0, size)]

    def origin(kind, side, size, cut=None):
        ref = kinds[kind][0]
        first, count = (0, depth) if cut is None else (cut * step_depth, step_depth)
        start = pl.multiple_of(side * (units - size), LANES)
        if kind == "d":
            return ref.at[pl.ds(start, size), pl.ds(first, count)]
        return ref.at[pl.ds(first, count), pl.ds(start, size)]

    def own_copies(kind, flip):
        other = (flip // PAIR) % 2
        side = (half + other) % 2
        large = is_big if other == 0 else jnp.logical_not(is_big)

        def make(size, cut):
            return weight_link(kind, flip, cut).copy(
                origin(kind, side, size, cut),
                slot(kind, flip, size, cut, (y + flip) % 2),
                sp_dev(flip),
            )

        return large, make

    def send_own(kind, flip):
        large, make = own_copies(kind, flip)
        for cut in range(PARTS):
            sized(large, lambda size: make(size, cut).start())

    def drain_own(kind, flip):
        large, make = own_copies(kind, flip)
        for cut in range(PARTS):
            sized(large, lambda size: make(size, cut).wait_send())

    def wait_part(kind, flip, cut):
        def wait(size):
            at = slot(kind, flip, size, cut)
            weight_link(kind, flip, cut).copy(at, at, sp_dev(1)).wait_recv()

        sized(is_big, wait)

    @scoped("wait_weight")
    def wait_weight(kind, flip):
        for cut in range(PARTS):
            wait_part(kind, flip, cut)

    def relay_copy(kind, flip, size, cut):
        return weight_link(kind, flip + 1, cut).copy(
            slot(kind, flip, size, cut), slot(kind, flip + 1, size, cut, (y + 1) % 2), sp_dev(1)
        )

    @scoped("relay")
    def relay(kind, flip):
        for cut in range(PARTS):
            wait_part(kind, flip, cut)
            sized(is_big, lambda size: relay_copy(kind, flip, size, cut).start())

    def drain_relay(kind, flip):
        for cut in range(PARTS):
            sized(is_big, lambda size: relay_copy(kind, flip, size, cut).wait_send())

    def send(link, src, dst, device):
        copy = link.copy(src, dst, device)
        copy.start()
        ends.append(copy.wait_send)

    def wait(link, at):
        link.copy(at, at, tp_dev(core)).wait_recv()

    if big_units != small_units:

        @pl.when(jnp.logical_not(is_big))
        def _():
            pad = big_units - small_units
            zero = jnp.zeros((gt.shape[1], pad), jnp.bfloat16)
            for chunk in range(gt.shape[0]):
                gt[chunk, :, small_units:] = zero
                ut[chunk, :, small_units:] = zero
            for flip in range(n_sp):
                dn[flip, small_units:, :] = jnp.zeros((pad, depth), jnp.bfloat16)

    @pl.when(s == 0)
    def _():
        kh[...] = jnp.zeros_like(kh)

    qkv_loads = [local(q_hbm, q_ref), local(k_hbm, k_ref), local(v_hbm, v_ref)]
    for load in qkv_loads:
        load.start()

    barrier = pltpu.get_barrier_semaphore()
    sp_flips = [1, PAIR] + far
    tp_flips = list(range(1, n_tp))
    for flip in sp_flips:
        pl.semaphore_signal(barrier, inc=1, device_id=sp_dev(flip), device_id_type=MESH)
    for flip in tp_flips:
        pl.semaphore_signal(barrier, inc=1, device_id=tp_dev(flip), device_id_type=MESH)

    @pl.when(s + 1 < n_sp)
    def _():
        pl.semaphore_signal(barrier, inc=1, device_id={"sp": s + 1}, device_id_type=MESH)

    @pl.when(s > 0)
    def _():
        pl.semaphore_signal(barrier, inc=1, device_id={"sp": s - 1}, device_id_type=MESH)

    greeted = len(sp_flips) + len(tp_flips)
    edges = jnp.where(s > 0, 1, 0) + jnp.where(s + 1 < n_sp, 1, 0)
    with jax.named_scope("barrier"):
        pl.semaphore_wait(barrier, greeted + edges)

    halo = [new_link(), new_link()]
    last = pl.ds(rows - window, window)

    def halo_copy(at, ref):
        return halo[at].copy(ref.at[:, last], kh.at[at], {"sp": jnp.minimum(s + 1, n_sp - 1)})

    @pl.when(s + 1 < n_sp)
    def _():
        for at, ref in enumerate((k_hbm, v_hbm)):
            halo_copy(at, ref).start()

    own_loads = {}
    for kind in kinds:

        def load(kind=kind):
            index = locals_used[0]
            locals_used[0] += 1

            def make(size):
                return pltpu.make_async_copy(
                    origin(kind, half, size), slot(kind, 0, size), local_sems.at[index]
                )

            sized(is_big, lambda size: make(size).start())
            return lambda: sized(is_big, lambda size: make(size).wait())

        own_loads[kind] = load()
    for kind in kinds:
        send_own(kind, 1)
    for kind in "gu":
        send_own(kind, PAIR)
    pl.when(outer)(lambda: send_own("d", PAIR))

    @pl.when(inner)
    def _():
        for flip in reversed(far):
            for kind in "gu":
                send_own(kind, flip)
        for flip in far:
            send_own("d", flip)

    res_load = local(res_hbm, res)
    res_load.start()
    ow_links = {flip: new_link() for flip in tp_flips}
    gain_links = {flip: new_link() for flip in tp_flips}
    for flip in tp_flips:
        start = pl.multiple_of(flip_of(t, flip) * width, LANES)
        send(ow_links[flip], ow_hbm.at[:, pl.ds(start, width)], ow.at[flip], tp_dev(flip))
        send(gain_links[flip], ng_ref, gains.at[flip], tp_dev(flip))
    ow_load = local(ow_hbm.at[:, pl.ds(pl.multiple_of(t * width, LANES), width)], ow.at[0])
    ow_load.start()
    gains[0] = ng_ref[...]

    head_width = qg_ref.shape[1]
    heads = q_ref.shape[1] // head_width
    blocks = rows // window
    scale = head_width ** (-0.5)

    def unit_norm(data, gain):
        data = data.astype(jnp.float32)
        mean = jnp.mean(data * data, axis=-1, keepdims=True)
        return (data * lax.rsqrt(mean + EPS) * gain).astype(jnp.bfloat16)

    def turn(block):
        return block.astype(jnp.float32).T

    for load in qkv_loads:
        load.wait()

    def norm_keys(at, _):
        here = pl.ds(pl.multiple_of(at * window, window), window)
        there = pl.ds(pl.multiple_of((at + 1) * window, window), window)
        kn[there, :] = unit_norm(turn(k_ref[:, here]), kg_ref[...])
        vn[there, :] = turn(v_ref[:, here]).astype(jnp.bfloat16)
        return 0

    lax.fori_loop(0, blocks, norm_keys, 0)

    def attend_block(at, _):
        here = pl.ds(pl.multiple_of(at * window, window), window)
        both = pl.ds(pl.multiple_of(at * window, window), 2 * window)
        keys, values = kn[both, :], vn[both, :]
        raw = q_ref[here, :]
        query_index = lax.broadcasted_iota(jnp.int32, (window, 2 * window), 0)
        key_index = lax.broadcasted_iota(jnp.int32, (window, 2 * window), 1)
        lag = window + query_index - key_index
        first = jnp.where(s * blocks + at > 0, 0, window)
        valid = (lag >= 0) & (lag < window) & (key_index >= first)
        pieces = []
        for head in range(heads):
            query = unit_norm(raw[:, head * head_width : (head + 1) * head_width], qg_ref[...])
            scores = lax.dot_general(
                query, keys, (((1,), (1,)), ((), ())), preferred_element_type=jnp.float32
            )
            scores = jnp.where(valid, scores * scale, -1e30)
            sink = sink_ref[0, head]
            peak = jnp.maximum(jnp.max(scores, axis=-1, keepdims=True), sink)
            terms = jnp.exp(scores - peak)
            total = jnp.sum(terms, axis=-1, keepdims=True) + jnp.exp(sink - peak)
            weights = (terms / total).astype(jnp.bfloat16)
            piece = jnp.dot(weights, values, preferred_element_type=jnp.float32)
            pieces.append(piece.astype(jnp.bfloat16))
        att[0, here, :] = jnp.concatenate(pieces, axis=1)
        return 0

    with jax.named_scope("attend"):
        lax.fori_loop(1, blocks, attend_block, 0)

    @pl.when(s > 0)
    def _():
        for at in range(2):
            halo[at].copy(kh.at[at], kh.at[at], {"sp": jnp.maximum(s - 1, 0)}).wait_recv()

    kn[0:window, :] = unit_norm(turn(kh[0]), kg_ref[...])
    vn[0:window, :] = turn(kh[1]).astype(jnp.bfloat16)
    with jax.named_scope("attend_first"):
        lax.fori_loop(0, 1, attend_block, 0)

    att_links = {flip: new_link() for flip in tp_flips}
    send(att_links[far_tp], att.at[0], att.at[far_tp], tp_dev(far_tp))
    send(att_links[core], att.at[0], att.at[core], tp_dev(core))

    with jax.named_scope("wait_att"):
        wait(att_links[far_tp], att.at[far_tp])
    send(att_links[far_tp ^ core], att.at[far_tp], att.at[far_tp ^ core], tp_dev(core))

    for flip in tp_flips:
        with jax.named_scope("wait_ow"):
            wait(ow_links[flip], ow.at[flip])
        wait(gain_links[flip], gains.at[flip])
    ow_load.wait()
    res_load.wait()
    wait(att_links[core], att.at[core])
    wait(att_links[far_tp ^ core], att.at[far_tp ^ core])

    def project(at, _):
        here = pl.ds(pl.multiple_of(at * window, window), window)
        mixed = jnp.zeros((window, width), jnp.float32)
        for flip in range(n_tp):
            product = jnp.dot(att[flip, here, :], ow[flip], preferred_element_type=jnp.float32)
            mixed = mixed + product.astype(jnp.bfloat16).astype(jnp.float32)
        mid[0, 0, here, :] = (res[here, :].astype(jnp.float32) + mixed).astype(jnp.bfloat16)
        return 0

    cuts = 2
    piece = rows // cuts
    mid_links = {
        (side, flip, cut): new_link()
        for side in range(2)
        for flip in range(n_tp)
        for cut in range(cuts)
        if side or flip
    }

    def part(side, flip, cut):
        return mid.at[side, flip, pl.ds(cut * piece, piece), :]

    mid_ends = {}

    def pass_mid(side, flip, cut, to_side, to_flip, device_of, hop):
        def make():
            return mid_links[to_side, to_flip, cut].copy(
                part(side, flip, cut), part(to_side, to_flip, cut), device_of(hop)
            )

        make().start()
        mid_ends[to_side, to_flip, cut] = lambda: make().wait_send()

    @scoped("wait_mid")
    def wait_mid(side, flip, cut):
        wait(mid_links[side, flip, cut], part(side, flip, cut))

    with jax.named_scope("project"):
        lax.fori_loop(0, blocks, project, 0)
    for cut in range(cuts):
        pass_mid(0, 0, cut, 1, 0, sp_dev, PAIR)
        pass_mid(0, 0, cut, 0, far_tp, tp_dev, far_tp)
        pass_mid(0, 0, cut, 0, core, tp_dev, core)

    norm_rows = 64

    @scoped("normalise")
    def normalise(side):
        def step(at, _):
            here = pl.ds(pl.multiple_of(at * norm_rows, norm_rows), norm_rows)
            total = jnp.zeros((norm_rows, 1), jnp.float32)
            for flip in range(n_tp):
                data = mid[side, flip, here, :].astype(jnp.float32)
                total = total + jnp.sum(data * data, axis=1, keepdims=True)
            factor = lax.rsqrt(total / (width * n_tp) + EPS)
            for flip in range(n_tp):
                data = mid[side, flip, here, :].astype(jnp.float32)
                nrm[side, flip, here, :] = (data * factor * gains[flip]).astype(jnp.bfloat16)
            return 0

        lax.fori_loop(0, rows // norm_rows, step, 0)

    pl.when(inner)(lambda: send_own("d", PAIR))

    @pl.when(outer)
    def _():
        for flip in far:
            for kind in "gu":
                send_own(kind, flip)
        for flip in far:
            send_own("d", flip)

    tile = 256
    tall = rows // 2
    wide_tile = rows // 2
    n_chunks = n_sp // 2
    z = s // 2

    @scoped("expand")
    def expand(chunk, side, first=False, last=False, flip=None):
        at_slot = xor(xor(z, chunk, n_chunks), t, n_chunks)
        if flip is None:
            part = pl.ds(0, 2 * depth)
        else:
            part = pl.ds(pl.multiple_of(((y + flip) % 2) * depth, depth), depth)

        def step(at, _):
            here = pl.ds(pl.multiple_of(at * wide_tile, wide_tile), wide_tile)
            there = pl.ds(pl.multiple_of(side * rows + at * wide_tile, wide_tile), wide_tile)
            data = nrm[side, at_slot, here, part]
            gate = jnp.dot(data, gt[chunk, part, :], preferred_element_type=jnp.float32)
            up = jnp.dot(data, ut[chunk, part, :], preferred_element_type=jnp.float32)
            if not first:
                gate = gate + acc_g[there, :]
                up = up + acc_u[there, :]
            if not last:
                acc_g[there, :] = gate
                acc_u[there, :] = up
            else:
                hid[there, :] = (gate / (1.0 + jnp.exp(-gate)) * up).astype(jnp.bfloat16)
            return 0

        lax.fori_loop(0, rows // wide_tile, step, 0)

    def wait_beside(flip):
        for kind in "gu":
            wait_weight(kind, flip + 1)

    def spread(cut):
        wait_mid(1, 0, cut)
        pass_mid(1, 0, cut, 1, far_tp, tp_dev, far_tp)
        pass_mid(1, 0, cut, 1, core, tp_dev, core)

    for kind in "gu":
        relay(kind, PAIR)
    for kind in "gu":
        relay(kind, soon)
    for cut in range(cuts):
        wait_mid(0, far_tp, cut)
        pass_mid(0, far_tp, cut, 0, far_tp ^ core, tp_dev, core)
    @pl.when(inner)
    def _():
        for cut in range(cuts):
            spread(cut)
        relay("d", PAIR)

    pl.when(outer)(lambda: relay("d", far[0]))
    for cut in range(cuts):
        wait_mid(0, core, cut)
        wait_mid(0, far_tp ^ core, cut)
    normalise(0)
    own_loads["g"]()
    own_loads["u"]()
    wait_beside(0)
    expand(0, 0, True)
    pl.when(outer)(lambda: spread(0))
    wait_beside(PAIR)
    expand(1, 0)
    pl.when(inner)(lambda: relay("g", late))
    pl.when(outer)(lambda: spread(1))
    wait_beside(soon)
    expand(soon // 2, 0)
    pl.when(inner)(lambda: relay("u", late))
    for cut in range(cuts):
        wait_mid(1, far_tp, cut)
        pass_mid(1, far_tp, cut, 1, far_tp ^ core, tp_dev, core)
        if cut == 0:
            pl.when(outer)(lambda: relay("g", late))
    for cut in range(cuts):
        wait_mid(1, core, cut)
        wait_mid(1, far_tp ^ core, cut)
    normalise(1)
    expand(0, 1, True)
    pl.when(outer)(lambda: relay("u", late))
    expand(1, 1)
    expand(soon // 2, 1)
    for side in range(2):
        expand(late // 2, side, flip=late)
    pl.when(outer)(lambda: relay("d", PAIR))
    wait_beside(late)
    for side in range(2):
        expand(late // 2, side, last=True, flip=late + 1)

    core_links = counter[0]
    x_links = core_links + 2 * n_sp
    z_links = x_links + 4
    counter[0] += 2 * n_sp + 8
    by_tp = (z + t) % 2 == 0
    by_pair = jnp.logical_not(by_tp)

    def link(index):
        return Link((send_sems, recv_sems), index)

    def role_of(flip):
        return xor(xor(z, flip // 2, n_chunks), t, n_chunks)

    def side_rows(side):
        return pl.ds(side * rows, rows)

    def core_copy(flip, side):
        some = side_rows(side)
        return link(core_links + 2 * flip + side).copy(
            pb.at[flip, some, :], cb.at[flip, some, :], tp_dev(core)
        )

    def x_copy(flip, block, side):
        some = side_rows(side)
        return link(x_links + 2 * block + side).copy(
            pb.at[flip, some, :], xb.at[block, some, :], tp_dev(far_tp)
        )

    def z_copy(place, block):
        return link(z_links + 2 * place + block).copy(
            zs.at[place, block], zb.at[place, block], sp_dev(PAIR)
        )

    def over_rows(fn, size=tile):
        def step(at, _):
            fn(pl.multiple_of(at * size, size))
            return 0

        lax.fori_loop(0, rows // size, step, 0)

    def wide(ref, *index):
        return ref[index].astype(jnp.float32)

    def at_side(side, base, size=tile):
        return pl.ds(pl.multiple_of(side * rows + base, size), size)

    @scoped("shrink")
    def shrink(flip):
        for side in (1, 0):

            def step(base, side=side):
                here = at_side(side, base, tall)
                product = jnp.dot(hid[here, :], dn[flip], preferred_element_type=jnp.float32)
                pb[flip, here, :] = product.astype(jnp.bfloat16)

            step(0)
            step(tall)
            pl.when(role_of(flip) % 2 == 1)(lambda: core_copy(flip, side).start())

    def give_pair(place, flip, block, with_x):
        core_copy(flip, 1).wait_recv()
        if with_x:
            x_copy(flip, block, 1).wait_recv()

        def step(base):
            there = at_side(1, base)
            held = wide(pb, flip, there) + wide(cb, flip, there)
            if with_x:
                held = held + wide(xb, block, there)
            zs[place, block, pl.ds(base, tile), :] = held.astype(jnp.bfloat16)

        over_rows(step)
        z_copy(place, block).start()

    def give_tp(flip, block, side, with_z):
        if with_z:
            z_copy(1, block).wait_recv()
        core_copy(flip, side).wait_recv()

        def step(base):
            here = at_side(side, base)
            held = wide(pb, flip, here) + wide(cb, flip, here)
            if with_z:
                held = held + wide(zb, 1, block, pl.ds(base, tile))
            pb[flip, here, :] = held.astype(jnp.bfloat16)

        over_rows(step)
        x_copy(flip, block, side).start()

    @scoped("collect")
    def collect(flip):
        role = role_of(flip)
        block = (y + flip) % 2
        pl.when(jnp.logical_and(role == far_tp, by_tp))(lambda: give_tp(flip, block, 1, False))

        @pl.when(jnp.logical_and(role == far_tp, by_pair))
        def _():
            give_pair(1, flip, block, False)
            give_tp(flip, block, 0, False)

        pl.when(jnp.logical_and(role == 0, by_pair))(lambda: give_pair(0, flip, block, False))

    mine = xor(z, t, n_chunks)
    theirs = xor(mine, far_tp, n_chunks)

    def second_theirs(*places):
        with jax.named_scope("theirs"):
            for beside in places:
                give_tp(2 * theirs + beside, (y + beside) % 2, 0, True)

    def second_mine():
        with jax.named_scope("mine"):
            for beside in range(2):
                give_pair(0, 2 * mine + beside, (y + beside) % 2, True)

    def down(flip):
        if not (isinstance(flip, int) and flip in (0, PAIR)):
            wait_weight("d", flip)
        shrink(flip)

    def first_relay():
        pl.when(inner)(lambda: relay("d", far[0]))
        pl.when(outer)(lambda: relay("d", far[1]))

    def second_relay():
        pl.when(inner)(lambda: relay("d", far[1]))

    def both(one, other):
        return jnp.logical_and(one, other)

    own_loads["d"]()
    far_foreign = t // far_tp == z // far_tp
    here_first, there_first = far

    @pl.when(jnp.logical_not(far_foreign))
    def _():
        down(0)
        first_relay()
        down(1)
        collect(0)
        down(PAIR)
        collect(1)
        down(PAIR + 1)
        collect(PAIR)
        shrink(here_first)
        collect(PAIR + 1)
        down(here_first + 1)
        collect(here_first)
        second_relay()
        shrink(there_first)
        collect(here_first + 1)
        collect(there_first)

        pl.when(both(inner, by_tp))(second_mine)
        down(there_first + 1)
        collect(there_first + 1)
        pl.when(both(outer, by_tp))(second_mine)
        pl.when(by_tp)(lambda: second_theirs(0, 1))

    @pl.when(both(far_foreign, inner))
    def _():
        down(0)
        first_relay()
        shrink(here_first)
        collect(0)
        down(1)
        collect(here_first)
        down(PAIR)
        collect(1)
        down(PAIR + 1)
        collect(PAIR)
        down(here_first + 1)
        collect(PAIR + 1)
        collect(here_first + 1)
        second_relay()
        shrink(there_first)
        pl.when(by_tp)(second_mine)
        collect(there_first)
        down(there_first + 1)
        collect(there_first + 1)
        pl.when(by_tp)(lambda: second_theirs(0, 1))

    @pl.when(both(far_foreign, outer))
    def _():
        shrink(here_first)
        first_relay()
        down(PAIR)
        collect(here_first)
        down(here_first + 1)
        collect(PAIR)
        down(PAIR + 1)
        collect(here_first + 1)
        shrink(there_first)
        down(0)
        collect(there_first)
        down(1)
        collect(0)
        collect(1)
        down(there_first + 1)
        collect(there_first + 1)
        collect(PAIR + 1)
        pl.when(by_tp)(second_mine)
        pl.when(by_tp)(lambda: second_theirs(0, 1))

    out_copies = []
    for beside in range(2):
        flip, block = 2 * mine + beside, (y + beside) % 2
        with jax.named_scope("wait_z"):
            core_copy(flip, 0).wait_recv()
            z_copy(0, block).wait_recv()
        with jax.named_scope("wait_x"):
            x_copy(flip, block, 0).wait_recv()
        columns = pl.ds(pl.multiple_of(block * depth, depth), depth)

        def finish(base, flip=flip, block=block, columns=columns):
            here = pl.ds(base, tile)
            feed = wide(pb, flip, here) + wide(cb, flip, here) + wide(zb, 0, block, here)
            feed = feed + wide(xb, block, here)
            out_ref[here, columns] = (wide(mid, 0, 0, here, columns) + 0.5 * feed).astype(jnp.bfloat16)

        over_rows(finish)
        out_copies.append(local(out_ref.at[:, columns], out_hbm.at[:, columns]))
        out_copies[-1].start()

    with jax.named_scope("ends"):
        for copy in out_copies:
            copy.wait()
        for end in [*ends, *mid_ends.values()]:
            end()
        for kind in kinds:
            for flip in [1, PAIR] + far:
                drain_own(kind, flip)
            for flip in [PAIR] + far:
                drain_relay(kind, flip)
        for flip in range(n_sp):
            for side in range(2):
                pl.when(role_of(flip) % 2 == 1)(lambda: core_copy(flip, side).wait_send())
        for beside in range(2):
            flip, block = 2 * theirs + beside, (y + beside) % 2
            x_copy(flip, block, 0).wait_send()
            pl.when(by_tp)(lambda: x_copy(flip, block, 1).wait_send())
            z_copy(0, block).wait_send()
            pl.when(by_pair)(lambda: z_copy(1, block).wait_send())

    @pl.when(s + 1 < n_sp)
    def _():
        for at, ref in enumerate((k_hbm, v_hbm)):
            halo_copy(at, ref).wait_send()


def kernel_device(
    queries,
    keys,
    values,
    query_gain,
    key_gain,
    sink_logits,
    out_weight,
    residual,
    norm_gain,
    gate_weight,
    up_weight,
    down_weight,
):
    n_sp, n_tp = lax.axis_size("sp"), lax.axis_size("tp")
    rows, width = residual.shape
    depth, units = gate_weight.shape
    big, _ = split_units(units)
    heads_width = queries.shape[1]
    head_width = query_gain.shape[0]
    bf16, f32 = jnp.bfloat16, jnp.float32
    vmem = pl.BlockSpec(memory_space=pltpu.VMEM)
    smem = pl.BlockSpec(memory_space=pltpu.SMEM)
    hbm = pl.BlockSpec(memory_space=pl.ANY)
    n_links = 97
    scratch = [
        pltpu.VMEM((n_sp // 2, 2 * depth, big), bf16),
        pltpu.VMEM((n_sp // 2, 2 * depth, big), bf16),
        pltpu.VMEM((n_sp, big, depth), bf16),
        pltpu.VMEM((2, n_tp, rows, width), bf16),
        pltpu.VMEM((2, n_tp, rows, width), bf16),
        pltpu.VMEM((2 * rows, big), f32),
        pltpu.VMEM((2 * rows, big), f32),
        pltpu.VMEM((2 * rows, big), bf16),
        pltpu.VMEM((n_sp, 2 * rows, depth), bf16),
        pltpu.VMEM((n_sp, 2 * rows, depth), bf16),
        pltpu.VMEM((2, 2 * rows, depth), bf16),
        pltpu.VMEM((2, 2, rows, depth), bf16),
        pltpu.VMEM((2, 2, rows, depth), bf16),
        pltpu.VMEM((n_tp, rows, heads_width), bf16),
        pltpu.VMEM((n_tp, heads_width, width), bf16),
        pltpu.VMEM((n_tp, 1, width), f32),
        pltpu.VMEM((rows, width), bf16),
        pltpu.VMEM((rows + WINDOW, head_width), bf16),
        pltpu.VMEM((rows + WINDOW, head_width), bf16),
        pltpu.VMEM((2, head_width, WINDOW), bf16),
        pltpu.VMEM((rows, heads_width), bf16),
        pltpu.VMEM((head_width, rows), bf16),
        pltpu.VMEM((head_width, rows), bf16),
        pltpu.VMEM((rows, width), bf16),
        pltpu.SemaphoreType.DMA((n_links,)),
        pltpu.SemaphoreType.DMA((n_links,)),
        pltpu.SemaphoreType.DMA((16,)),
    ]
    return pl.pallas_call(
        functools.partial(layer_kernel, n_sp, n_tp),
        out_shape=jax.ShapeDtypeStruct((rows, width), bf16),
        in_specs=[hbm, hbm, hbm, vmem, vmem, smem, hbm, hbm, vmem, hbm, hbm, hbm],
        out_specs=hbm,
        scratch_shapes=scratch,
        compiler_params=pltpu.CompilerParams(
            collective_id=0, has_side_effects=True, vmem_limit_bytes=66 * 1000 * 1000
        ),
    )(
        queries,
        keys.T,
        values.T,
        query_gain[None],
        key_gain[None],
        sink_logits[None],
        out_weight,
        residual,
        norm_gain[None],
        gate_weight,
        up_weight,
        down_weight,
    )


def per_device(*args):
    queries, keys, query_gain, residual, gate_weight = args[0], args[1], args[3], args[7], args[9]
    n_sp, n_tp = lax.axis_size("sp"), lax.axis_size("tp")
    depth, units = gate_weight.shape
    rows, width = residual.shape
    fits = (
        depth % LANES == 0
        and units % LANES == 0
        and rows % (2 * LANES) == 0
        and width == 2 * depth
        and n_sp == 2 * n_tp
        and n_tp // 2 == PAIR
        and n_sp % (2 * PAIR) == 0
        and keys.shape[1] == query_gain.shape[0]
    )
    return kernel_device(*args) if fits else permute_device(*args)


def solution(mesh):
    in_specs = (
        P("sp", "tp"),
        P("sp", "tp"),
        P("sp", "tp"),
        P(),
        P(),
        P("tp"),
        P("tp", None),
        P("sp", "tp"),
        P("tp"),
        P("sp", "tp"),
        P("sp", "tp"),
        P("tp", "sp"),
    )
    out_specs = P("sp", "tp")
    return jax.shard_map(
        per_device, mesh=mesh, in_specs=in_specs, out_specs=out_specs, check_vma=False
    )
```

```python
import functools

import jax
import jax.numpy as jnp
from jax import lax
from jax.experimental import pallas as pl
from jax.experimental.pallas import tpu as pltpu
from jax.sharding import PartitionSpec as P

WINDOW = 128
PAIR = 2
LANES = 128
PARTS = 2
EPS = 1e-06
MESH = pl.DeviceIdType.MESH


def swap(block, axis, flip):
    return lax.ppermute(block, axis, [(i, i ^ flip) for i in range(lax.axis_size(axis))])


def from_behind(block, axis, distance):
    devices = range(lax.axis_size(axis))
    route = [(i - distance, i) for i in devices if i - distance in devices]
    return lax.ppermute(block, axis, route)


def gather_flips(block, axis):
    found = {0: block}
    flip = lax.axis_size(axis) // 2
    while flip:
        for at, held in list(found.items()):
            found[at ^ flip] = swap(held, axis, flip)
        flip //= 2
    return [found[at] for at in range(lax.axis_size(axis))]


def norm_heads(flat, gain, heads):
    row_count = flat.shape[0]
    head_width = gain.shape[0]
    data = flat.astype(jnp.float32).reshape(row_count, heads, head_width)
    scaled = data * lax.rsqrt(jnp.mean(data * data, axis=-1, keepdims=True) + 1e-06) * gain
    return scaled.astype(jnp.bfloat16)


def attend(queries, keys, values, edge, query_gain, key_gain, sink_logits):
    head_width = query_gain.shape[0]
    row_count = queries.shape[0]
    q_heads = queries.shape[1] // head_width
    k_heads = keys.shape[1] // head_width
    group_size = q_heads // k_heads
    window_len = WINDOW
    block_count = row_count // window_len
    query_norm = norm_heads(queries, query_gain, q_heads)
    key_raw = jnp.concatenate([edge[:, : keys.shape[1]], keys], axis=0)
    key_all = norm_heads(key_raw, key_gain, k_heads).reshape(key_raw.shape)
    value_all = jnp.concatenate([edge[:, keys.shape[1] :], values], axis=0)

    def windows(flat):
        return jnp.concatenate(
            [
                flat[:row_count].reshape(block_count, window_len, k_heads, head_width),
                flat[window_len:].reshape(block_count, window_len, k_heads, head_width),
            ],
            axis=1,
        )

    key_blocks, value_blocks = windows(key_all), windows(value_all)
    query_blocks = query_norm.reshape(block_count, window_len, k_heads, group_size, head_width)
    scores = jnp.einsum(
        "nqhgd,nkhd->nhgqk", query_blocks, key_blocks, preferred_element_type=jnp.float32
    ) * head_width ** (-0.5)
    query_index = jnp.arange(window_len)[:, None]
    key_index = jnp.arange(2 * window_len)[None, :]
    offset_lag = window_len + query_index - key_index
    inband = (offset_lag >= 0) & (offset_lag < window_len)
    leading = (
        (jnp.arange(block_count)[:, None, None] > 0)
        | (key_index[None] >= window_len)
        | (lax.axis_index("sp") > 0)
    )
    valid = inband[None] & leading
    scores = jnp.where(valid[:, None, None], scores, -1e30)
    sink_rows = sink_logits.reshape(k_heads, group_size)[None, :, :, None]
    row_peak = jnp.maximum(jnp.max(scores, axis=-1), sink_rows)
    exp_terms = jnp.exp(scores - row_peak[..., None])
    denom_sum = jnp.sum(exp_terms, axis=-1) + jnp.exp(sink_rows - row_peak)
    weights = (exp_terms / denom_sum[..., None]).astype(jnp.bfloat16)
    attended = jnp.einsum(
        "nhgqk,nkhd->nqhgd", weights, value_blocks, preferred_element_type=jnp.float32
    ).astype(jnp.bfloat16)
    return attended.reshape(row_count, q_heads * head_width)


def permute_device(
    queries,
    keys,
    values,
    query_gain,
    key_gain,
    sink_logits,
    out_weight,
    residual,
    norm_gain,
    gate_weight,
    up_weight,
    down_weight,
):
    n_sp, n_tp = lax.axis_size("sp"), lax.axis_size("tp")
    sp, tp = lax.axis_index("sp"), lax.axis_index("tp")
    half = (sp // PAIR) % 2
    row_count, width = residual.shape
    depth, units = gate_weight.shape
    units //= 2

    def part(array, axis, flip):
        return lax.dynamic_slice_in_dim(array, (half ^ flip) * units, units, axis)

    far = list(range(2 * PAIR, n_sp, 2))

    def send(first, second, flips):
        found = {}
        for flip in flips:
            other = (flip // PAIR) % 2
            if second is None:
                piece = part(first, 0, other)
            else:
                piece = jnp.concatenate([part(first, 1, other), part(second, 1, other)], axis=1)
            found[flip] = swap(piece, "sp", flip) if flip else piece
        return found

    def relay(found, flips):
        for flip in flips:
            found[flip ^ 1] = swap(found[flip], "sp", 1)

    edge = jnp.concatenate([keys, values], axis=1)[row_count - WINDOW :]
    edge = from_behind(edge, "sp", 1)
    gate_weight, up_weight, residual, out_weight, edge = lax.optimization_barrier(
        (gate_weight, up_weight, residual, out_weight, edge)
    )
    near = [0, PAIR]
    first = far[: len(far) // 2]
    residual_pair = swap(residual, "sp", PAIR)
    both = send(gate_weight, up_weight, first)
    both.update(send(gate_weight, up_weight, near))
    attended = attend(queries, keys, values, edge, query_gain, key_gain, sink_logits)
    attended_pair = swap(attended, "sp", PAIR)

    gate_weight, up_weight, down_weight, attended_pair = lax.optimization_barrier(
        (gate_weight, up_weight, down_weight, attended_pair)
    )
    both.update(send(gate_weight, up_weight, far[len(far) // 2 :]))
    early = {flip: both[flip] for flip in first}
    down_weight, early = lax.optimization_barrier((down_weight, early))
    both.update(early)
    down = send(down_weight, None, far)
    down.update(send(down_weight, None, near))
    relay(both, near + far)
    relay(down, near)

    gains = jnp.concatenate(gather_flips(norm_gain, "tp"))
    projections = gather_flips(out_weight, "tp")
    stream = jnp.concatenate([residual, residual_pair], axis=0)
    stream = jnp.concatenate(gather_flips(stream, "tp"), axis=1).astype(jnp.float32)
    heads = gather_flips(jnp.concatenate([attended, attended_pair], axis=0), "tp")

    def own_first(columns):
        pieces = [
            lax.dynamic_slice_in_dim(columns, (tp ^ flip) * width, width, 1)
            for flip in range(n_tp)
        ]
        return jnp.concatenate(pieces, axis=1)

    projection = jnp.concatenate([own_first(piece) for piece in projections], axis=0)
    head = jnp.concatenate(heads, axis=1)
    mixed = jnp.dot(head, projection, preferred_element_type=jnp.float32)
    middle = (stream + mixed).astype(jnp.bfloat16)
    middle = lax.optimization_barrier(middle)
    middle_wide = middle.astype(jnp.float32)
    mean = jnp.mean(middle_wide * middle_wide, axis=1, keepdims=True)
    normed = (middle_wide * lax.rsqrt(mean + 1e-06) * gains).astype(jnp.bfloat16)

    late = {flip: down[flip] for flip in far}
    normed, late = lax.optimization_barrier((normed, late))
    down.update(late)
    relay(down, far)

    per_part = width // depth

    def place(flip):
        block = sp ^ flip
        return (((block // per_part) ^ tp) * per_part + block % per_part) * depth

    flips = range(n_sp)
    normed_in = jnp.concatenate(
        [lax.dynamic_slice_in_dim(normed, place(flip), depth, 1) for flip in flips], axis=1
    )
    gate_full = jnp.concatenate([both[flip][:, :units] for flip in flips], axis=0)
    up_full = jnp.concatenate([both[flip][:, units:] for flip in flips], axis=0)
    gate_acts = jnp.dot(normed_in, gate_full, preferred_element_type=jnp.float32)
    up_acts = jnp.dot(normed_in, up_full, preferred_element_type=jnp.float32)
    hidden = (jax.nn.silu(gate_acts) * up_acts).astype(jnp.bfloat16)

    down_full = jnp.zeros((units, width * n_tp), jnp.bfloat16)
    for flip in flips:
        down_full = lax.dynamic_update_slice_in_dim(down_full, down[flip], place(flip), 1)
    terms = [
        jnp.dot(
            hidden, down_full[:, at * width : (at + 1) * width], preferred_element_type=jnp.float32
        ).astype(jnp.bfloat16)
        for at in range(n_tp)
    ]

    def add(one, other):
        return one.astype(jnp.float32) + other.astype(jnp.float32)

    flip = 1
    held = dict(enumerate(terms))
    while flip < n_tp // 2:
        held = {
            at: add(held[at], swap(held[at ^ flip], "tp", flip)).astype(jnp.bfloat16)
            for at in held
            if not at & flip
        }
        flip *= 2
    own, other = held[0], held[flip]
    cut = width // 2
    across = add(own[:, :cut], swap(other[:, :cut], "tp", flip)).astype(jnp.bfloat16)
    left = add(across[:row_count], swap(across[row_count:], "sp", PAIR))
    pair = jnp.concatenate([own[:, cut:], other[:, cut:]], axis=1)
    pair = add(pair[:row_count], swap(pair[row_count:], "sp", PAIR)).astype(jnp.bfloat16)
    right = add(pair[:, : width - cut], swap(pair[:, width - cut :], "tp", flip))
    feed = jnp.concatenate([left, right], axis=1)
    return (middle_wide[:row_count, :width] + 0.5 * feed).astype(jnp.bfloat16)


def split_units(units):
    tiles = units // LANES
    small = (tiles // 2) * LANES
    return units - small, small


def scoped(name):
    def wrap(fn):
        def run(*args, **options):
            tags = [str(arg) for arg in args if isinstance(arg, (int, str))]
            with jax.named_scope("_".join([name, *tags])):
                return fn(*args, **options)

        return run

    return wrap


class Link:
    def __init__(self, sems, index):
        self.send, self.recv = sems[0].at[index], sems[1].at[index]

    def copy(self, src, dst, device):
        return pltpu.make_async_remote_copy(
            src_ref=src,
            dst_ref=dst,
            send_sem=self.send,
            recv_sem=self.recv,
            device_id=device,
            device_id_type=MESH,
        )


def layer_kernel(
    n_sp,
    n_tp,
    q_hbm,
    k_hbm,
    v_hbm,
    qg_ref,
    kg_ref,
    sink_ref,
    ow_hbm,
    res_hbm,
    ng_ref,
    gate_hbm,
    up_hbm,
    down_hbm,
    out_hbm,
    gt,
    ut,
    dn,
    mid,
    nrm,
    acc_g,
    acc_u,
    hid,
    pb,
    cb,
    xb,
    zs,
    zb,
    att,
    ow,
    gains,
    res,
    kn,
    vn,
    kh,
    q_ref,
    k_ref,
    v_ref,
    out_ref,
    send_sems,
    recv_sems,
    local_sems,
):
    s, t = lax.axis_index("sp"), lax.axis_index("tp")
    rows, width = res_hbm.shape
    depth, units = gate_hbm.shape
    big_units, small_units = split_units(units)
    window = WINDOW
    y = s % 2
    half = (s // PAIR) % 2
    is_big = (half + t) % 2 == 0
    core, far_tp = 1, n_tp // 2
    far = list(range(2 * PAIR, n_sp, PAIR))
    inner = (half + s // far[0]) % 2 == 1
    outer = jnp.logical_not(inner)
    soon = jnp.where(inner, far[1], far[0])
    late = jnp.where(inner, far[0], far[1])

    def flip_of(index, flip):
        out, bit = index, 1
        while bit <= flip:
            if flip & bit:
                out = out + bit - 2 * bit * ((index // bit) % 2)
            bit *= 2
        return out

    def xor(one, other, size):
        out, bit = 0, 1
        while bit < size:
            a, b = (one // bit) % 2, (other // bit) % 2
            out = out + bit * ((a + b) % 2)
            bit *= 2
        return out

    def sp_dev(flip):
        return {"sp": flip_of(s, flip)}

    def tp_dev(flip):
        return {"tp": flip_of(t, flip)}

    def sized(large, fn):
        if big_units == small_units:
            fn(big_units)
        else:
            pl.when(large)(lambda: fn(big_units))
            pl.when(jnp.logical_not(large))(lambda: fn(small_units))

    counter = [0]

    def new_link():
        counter[0] += 1
        return Link((send_sems, recv_sems), counter[0] - 1)

    ends = []

    locals_used = [0]

    def local(src, dst):
        locals_used[0] += 1
        return pltpu.make_async_copy(src, dst, local_sems.at[locals_used[0] - 1])

    kinds = {"g": (gate_hbm, gt), "u": (up_hbm, ut), "d": (down_hbm, dn)}
    counter[0] = len(kinds) * n_sp * PARTS
    step_depth = depth // PARTS

    def weight_link(kind, flip, cut):
        index = ("gud".index(kind) * n_sp + flip) * PARTS + cut
        return Link((send_sems, recv_sems), index)

    def slot(kind, flip, size, cut=None, seen_y=y):
        buf = kinds[kind][1]
        first, count = (0, depth) if cut is None else (cut * step_depth, step_depth)
        if kind == "d":
            return buf.at[flip, pl.ds(0, size), pl.ds(first, count)]
        start = ((seen_y + flip) % 2) * depth + first
        return buf.at[flip // 2, pl.ds(start, count), pl.ds(0, size)]

    def origin(kind, side, size, cut=None):
        ref = kinds[kind][0]
        first, count = (0, depth) if cut is None else (cut * step_depth, step_depth)
        start = pl.multiple_of(side * (units - size), LANES)
        if kind == "d":
            return ref.at[pl.ds(start, size), pl.ds(first, count)]
        return ref.at[pl.ds(first, count), pl.ds(start, size)]

    def own_copies(kind, flip):
        other = (flip // PAIR) % 2
        side = (half + other) % 2
        large = is_big if other == 0 else jnp.logical_not(is_big)

        def make(size, cut):
            return weight_link(kind, flip, cut).copy(
                origin(kind, side, size, cut),
                slot(kind, flip, size, cut, (y + flip) % 2),
                sp_dev(flip),
            )

        return large, make

    def send_own(kind, flip):
        large, make = own_copies(kind, flip)
        for cut in range(PARTS):
            sized(large, lambda size: make(size, cut).start())

    def drain_own(kind, flip):
        large, make = own_copies(kind, flip)
        for cut in range(PARTS):
            sized(large, lambda size: make(size, cut).wait_send())

    def wait_part(kind, flip, cut):
        def wait(size):
            at = slot(kind, flip, size, cut)
            weight_link(kind, flip, cut).copy(at, at, sp_dev(1)).wait_recv()

        sized(is_big, wait)

    @scoped("wait_weight")
    def wait_weight(kind, flip):
        for cut in range(PARTS):
            wait_part(kind, flip, cut)

    def relay_copy(kind, flip, size, cut):
        return weight_link(kind, flip + 1, cut).copy(
            slot(kind, flip, size, cut), slot(kind, flip + 1, size, cut, (y + 1) % 2), sp_dev(1)
        )

    @scoped("relay")
    def relay(kind, flip):
        for cut in range(PARTS):
            wait_part(kind, flip, cut)
            sized(is_big, lambda size: relay_copy(kind, flip, size, cut).start())

    def drain_relay(kind, flip):
        for cut in range(PARTS):
            sized(is_big, lambda size: relay_copy(kind, flip, size, cut).wait_send())

    def send(link, src, dst, device):
        copy = link.copy(src, dst, device)
        copy.start()
        ends.append(copy.wait_send)

    def wait(link, at):
        link.copy(at, at, tp_dev(core)).wait_recv()

    if big_units != small_units:

        @pl.when(jnp.logical_not(is_big))
        def _():
            pad = big_units - small_units
            zero = jnp.zeros((gt.shape[1], pad), jnp.bfloat16)
            for chunk in range(gt.shape[0]):
                gt[chunk, :, small_units:] = zero
                ut[chunk, :, small_units:] = zero
            for flip in range(n_sp):
                dn[flip, small_units:, :] = jnp.zeros((pad, depth), jnp.bfloat16)

    @pl.when(s == 0)
    def _():
        kh[...] = jnp.zeros_like(kh)

    qkv_loads = [local(q_hbm, q_ref), local(k_hbm, k_ref), local(v_hbm, v_ref)]
    for load in qkv_loads:
        load.start()

    barrier = pltpu.get_barrier_semaphore()
    sp_flips = [1, PAIR] + far
    tp_flips = list(range(1, n_tp))
    for flip in sp_flips:
        pl.semaphore_signal(barrier, inc=1, device_id=sp_dev(flip), device_id_type=MESH)
    for flip in tp_flips:
        pl.semaphore_signal(barrier, inc=1, device_id=tp_dev(flip), device_id_type=MESH)

    @pl.when(s + 1 < n_sp)
    def _():
        pl.semaphore_signal(barrier, inc=1, device_id={"sp": s + 1}, device_id_type=MESH)

    @pl.when(s > 0)
    def _():
        pl.semaphore_signal(barrier, inc=1, device_id={"sp": s - 1}, device_id_type=MESH)

    greeted = len(sp_flips) + len(tp_flips)
    edges = jnp.where(s > 0, 1, 0) + jnp.where(s + 1 < n_sp, 1, 0)
    with jax.named_scope("barrier"):
        pl.semaphore_wait(barrier, greeted + edges)

    halo = [new_link(), new_link()]
    last = pl.ds(rows - window, window)

    def halo_copy(at, ref):
        return halo[at].copy(ref.at[:, last], kh.at[at], {"sp": jnp.minimum(s + 1, n_sp - 1)})

    @pl.when(s + 1 < n_sp)
    def _():
        for at, ref in enumerate((k_hbm, v_hbm)):
            halo_copy(at, ref).start()

    own_loads = {}
    for kind in kinds:

        def load(kind=kind):
            index = locals_used[0]
            locals_used[0] += 1

            def make(size):
                return pltpu.make_async_copy(
                    origin(kind, half, size), slot(kind, 0, size), local_sems.at[index]
                )

            sized(is_big, lambda size: make(size).start())
            return lambda: sized(is_big, lambda size: make(size).wait())

        own_loads[kind] = load()
    for kind in kinds:
        send_own(kind, 1)
    for kind in "gu":
        send_own(kind, PAIR)
    pl.when(outer)(lambda: send_own("d", PAIR))

    @pl.when(inner)
    def _():
        for flip in reversed(far):
            for kind in "gu":
                send_own(kind, flip)
        for flip in far:
            send_own("d", flip)

    res_load = local(res_hbm, res)
    res_load.start()
    ow_links = {flip: new_link() for flip in tp_flips}
    gain_links = {flip: new_link() for flip in tp_flips}
    for flip in tp_flips:
        start = pl.multiple_of(flip_of(t, flip) * width, LANES)
        send(ow_links[flip], ow_hbm.at[:, pl.ds(start, width)], ow.at[flip], tp_dev(flip))
        send(gain_links[flip], ng_ref, gains.at[flip], tp_dev(flip))
    ow_load = local(ow_hbm.at[:, pl.ds(pl.multiple_of(t * width, LANES), width)], ow.at[0])
    ow_load.start()
    gains[0] = ng_ref[...]

    head_width = qg_ref.shape[1]
    heads = q_ref.shape[1] // head_width
    blocks = rows // window
    scale = head_width ** (-0.5)

    def unit_norm(data, gain):
        data = data.astype(jnp.float32)
        mean = jnp.mean(data * data, axis=-1, keepdims=True)
        return (data * lax.rsqrt(mean + EPS) * gain).astype(jnp.bfloat16)

    def turn(block):
        return block.astype(jnp.float32).T

    for load in qkv_loads:
        load.wait()

    def norm_keys(at, _):
        here = pl.ds(pl.multiple_of(at * window, window), window)
        there = pl.ds(pl.multiple_of((at + 1) * window, window), window)
        kn[there, :] = unit_norm(turn(k_ref[:, here]), kg_ref[...])
        vn[there, :] = turn(v_ref[:, here]).astype(jnp.bfloat16)
        return 0

    lax.fori_loop(0, blocks, norm_keys, 0)

    def attend_block(at, _):
        here = pl.ds(pl.multiple_of(at * window, window), window)
        both = pl.ds(pl.multiple_of(at * window, window), 2 * window)
        keys, values = kn[both, :], vn[both, :]
        raw = q_ref[here, :]
        query_index = lax.broadcasted_iota(jnp.int32, (window, 2 * window), 0)
        key_index = lax.broadcasted_iota(jnp.int32, (window, 2 * window), 1)
        lag = window + query_index - key_index
        first = jnp.where(s * blocks + at > 0, 0, window)
        valid = (lag >= 0) & (lag < window) & (key_index >= first)
        pieces = []
        for head in range(heads):
            query = unit_norm(raw[:, head * head_width : (head + 1) * head_width], qg_ref[...])
            scores = lax.dot_general(
                query, keys, (((1,), (1,)), ((), ())), preferred_element_type=jnp.float32
            )
            scores = jnp.where(valid, scores * scale, -1e30)
            sink = sink_ref[0, head]
            peak = jnp.maximum(jnp.max(scores, axis=-1, keepdims=True), sink)
            terms = jnp.exp(scores - peak)
            total = jnp.sum(terms, axis=-1, keepdims=True) + jnp.exp(sink - peak)
            weights = (terms / total).astype(jnp.bfloat16)
            piece = jnp.dot(weights, values, preferred_element_type=jnp.float32)
            pieces.append(piece.astype(jnp.bfloat16))
        att[0, here, :] = jnp.concatenate(pieces, axis=1)
        return 0

    with jax.named_scope("attend"):
        lax.fori_loop(1, blocks, attend_block, 0)

    @pl.when(s > 0)
    def _():
        for at in range(2):
            halo[at].copy(kh.at[at], kh.at[at], {"sp": jnp.maximum(s - 1, 0)}).wait_recv()

    kn[0:window, :] = unit_norm(turn(kh[0]), kg_ref[...])
    vn[0:window, :] = turn(kh[1]).astype(jnp.bfloat16)
    with jax.named_scope("attend_first"):
        lax.fori_loop(0, 1, attend_block, 0)

    att_links = {flip: new_link() for flip in tp_flips}
    send(att_links[far_tp], att.at[0], att.at[far_tp], tp_dev(far_tp))
    send(att_links[core], att.at[0], att.at[core], tp_dev(core))

    with jax.named_scope("wait_att"):
        wait(att_links[far_tp], att.at[far_tp])
    send(att_links[far_tp ^ core], att.at[far_tp], att.at[far_tp ^ core], tp_dev(core))

    for flip in tp_flips:
        with jax.named_scope("wait_ow"):
            wait(ow_links[flip], ow.at[flip])
        wait(gain_links[flip], gains.at[flip])
    ow_load.wait()
    res_load.wait()
    wait(att_links[core], att.at[core])
    wait(att_links[far_tp ^ core], att.at[far_tp ^ core])

    def project(at, _):
        here = pl.ds(pl.multiple_of(at * window, window), window)
        mixed = jnp.zeros((window, width), jnp.float32)
        for flip in range(n_tp):
            product = jnp.dot(att[flip, here, :], ow[flip], preferred_element_type=jnp.float32)
            mixed = mixed + product.astype(jnp.bfloat16).astype(jnp.float32)
        mid[0, 0, here, :] = (res[here, :].astype(jnp.float32) + mixed).astype(jnp.bfloat16)
        return 0

    cuts = 2
    piece = rows // cuts
    mid_links = {
        (side, flip, cut): new_link()
        for side in range(2)
        for flip in range(n_tp)
        for cut in range(cuts)
        if side or flip
    }

    def part(side, flip, cut):
        return mid.at[side, flip, pl.ds(cut * piece, piece), :]

    mid_ends = {}

    def pass_mid(side, flip, cut, to_side, to_flip, device_of, hop):
        def make():
            return mid_links[to_side, to_flip, cut].copy(
                part(side, flip, cut), part(to_side, to_flip, cut), device_of(hop)
            )

        make().start()
        mid_ends[to_side, to_flip, cut] = lambda: make().wait_send()

    @scoped("wait_mid")
    def wait_mid(side, flip, cut):
        wait(mid_links[side, flip, cut], part(side, flip, cut))

    with jax.named_scope("project"):
        lax.fori_loop(0, blocks, project, 0)
    for cut in range(cuts):
        pass_mid(0, 0, cut, 1, 0, sp_dev, PAIR)
        pass_mid(0, 0, cut, 0, far_tp, tp_dev, far_tp)
        pass_mid(0, 0, cut, 0, core, tp_dev, core)

    norm_rows = 64

    @scoped("normalise")
    def normalise(side):
        def step(at, _):
            here = pl.ds(pl.multiple_of(at * norm_rows, norm_rows), norm_rows)
            total = jnp.zeros((norm_rows, 1), jnp.float32)
            for flip in range(n_tp):
                data = mid[side, flip, here, :].astype(jnp.float32)
                total = total + jnp.sum(data * data, axis=1, keepdims=True)
            factor = lax.rsqrt(total / (width * n_tp) + EPS)
            for flip in range(n_tp):
                data = mid[side, flip, here, :].astype(jnp.float32)
                nrm[side, flip, here, :] = (data * factor * gains[flip]).astype(jnp.bfloat16)
            return 0

        lax.fori_loop(0, rows // norm_rows, step, 0)

    pl.when(inner)(lambda: send_own("d", PAIR))

    @pl.when(outer)
    def _():
        for flip in far:
            for kind in "gu":
                send_own(kind, flip)
        for flip in far:
            send_own("d", flip)

    tile = 256
    tall = rows // 2
    wide_tile = rows // 2
    n_chunks = n_sp // 2
    z = s // 2

    @scoped("expand")
    def expand(chunk, side, first=False, flip=None, kinds="gu", last=False):
        at_slot = xor(xor(z, chunk, n_chunks), t, n_chunks)
        if flip is None:
            part = pl.ds(0, 2 * depth)
        else:
            part = pl.ds(pl.multiple_of(((y + flip) % 2) * depth, depth), depth)

        def step(at, _):
            here = pl.ds(pl.multiple_of(at * wide_tile, wide_tile), wide_tile)
            there = pl.ds(pl.multiple_of(side * rows + at * wide_tile, wide_tile), wide_tile)
            data = nrm[side, at_slot, here, part]
            for kind in kinds:
                weight, acc = (gt, acc_g) if kind == "g" else (ut, acc_u)
                acts = jnp.dot(data, weight[chunk, part, :], preferred_element_type=jnp.float32)
                if not first:
                    acts = acts + acc[there, :]
                if last:
                    gate = acc_g[there, :]
                    hid[there, :] = (gate / (1.0 + jnp.exp(-gate)) * acts).astype(jnp.bfloat16)
                else:
                    acc[there, :] = acts
            return 0

        lax.fori_loop(0, rows // wide_tile, step, 0)

    def wait_beside(flip):
        for kind in "gu":
            wait_weight(kind, flip + 1)

    def spread(cut):
        wait_mid(1, 0, cut)
        pass_mid(1, 0, cut, 1, far_tp, tp_dev, far_tp)
        pass_mid(1, 0, cut, 1, core, tp_dev, core)

    for kind in "gu":
        relay(kind, PAIR)
    for kind in "gu":
        relay(kind, soon)
    for cut in range(cuts):
        wait_mid(0, far_tp, cut)
        pass_mid(0, far_tp, cut, 0, far_tp ^ core, tp_dev, core)
    @pl.when(inner)
    def _():
        for cut in range(cuts):
            spread(cut)
        relay("d", PAIR)

    pl.when(outer)(lambda: relay("d", far[0]))
    for cut in range(cuts):
        wait_mid(0, core, cut)
        wait_mid(0, far_tp ^ core, cut)
    normalise(0)
    own_loads["g"]()
    own_loads["u"]()
    wait_beside(0)
    expand(0, 0, True)
    pl.when(outer)(lambda: spread(0))
    wait_beside(PAIR)
    expand(1, 0)
    pl.when(inner)(lambda: relay("g", late))
    pl.when(outer)(lambda: spread(1))
    wait_beside(soon)
    expand(soon // 2, 0)
    pl.when(inner)(lambda: relay("u", late))
    for cut in range(cuts):
        wait_mid(1, far_tp, cut)
        pass_mid(1, far_tp, cut, 1, far_tp ^ core, tp_dev, core)
        if cut == 0:
            pl.when(outer)(lambda: relay("g", late))
    for cut in range(cuts):
        wait_mid(1, core, cut)
        wait_mid(1, far_tp ^ core, cut)
    normalise(1)
    expand(0, 1, True)
    pl.when(outer)(lambda: relay("u", late))
    expand(1, 1)
    expand(soon // 2, 1)
    for side in range(2):
        expand(late // 2, side, flip=late)
    pl.when(outer)(lambda: relay("d", PAIR))
    wait_weight("g", late + 1)
    for side in range(2):
        expand(late // 2, side, flip=late + 1, kinds="g")
    wait_weight("u", late + 1)
    for side in range(2):
        expand(late // 2, side, flip=late + 1, kinds="u", last=True)

    core_links = counter[0]
    x_links = core_links + 2 * n_sp
    z_links = x_links + 4
    counter[0] += 2 * n_sp + 8
    by_tp = (z + t) % 2 == 0
    by_pair = jnp.logical_not(by_tp)

    def link(index):
        return Link((send_sems, recv_sems), index)

    def role_of(flip):
        return xor(xor(z, flip // 2, n_chunks), t, n_chunks)

    def side_rows(side):
        return pl.ds(side * rows, rows)

    def core_copy(flip, side):
        some = side_rows(side)
        return link(core_links + 2 * flip + side).copy(
            pb.at[flip, some, :], cb.at[flip, some, :], tp_dev(core)
        )

    def x_copy(flip, block, side):
        some = side_rows(side)
        return link(x_links + 2 * block + side).copy(
            pb.at[flip, some, :], xb.at[block, some, :], tp_dev(far_tp)
        )

    def z_copy(place, block):
        return link(z_links + 2 * place + block).copy(
            zs.at[place, block], zb.at[place, block], sp_dev(PAIR)
        )

    def over_rows(fn, size=tile):
        def step(at, _):
            fn(pl.multiple_of(at * size, size))
            return 0

        lax.fori_loop(0, rows // size, step, 0)

    def wide(ref, *index):
        return ref[index].astype(jnp.float32)

    def at_side(side, base, size=tile):
        return pl.ds(pl.multiple_of(side * rows + base, size), size)

    @scoped("shrink")
    def shrink(flip):
        for side in (1, 0):

            def step(base, side=side):
                here = at_side(side, base, tall)
                product = jnp.dot(hid[here, :], dn[flip], preferred_element_type=jnp.float32)
                pb[flip, here, :] = product.astype(jnp.bfloat16)

            step(0)
            step(tall)
            pl.when(role_of(flip) % 2 == 1)(lambda: core_copy(flip, side).start())

    def give_pair(place, flip, block, with_x):
        core_copy(flip, 1).wait_recv()
        if with_x:
            x_copy(flip, block, 1).wait_recv()

        def step(base):
            there = at_side(1, base)
            held = wide(pb, flip, there) + wide(cb, flip, there)
            if with_x:
                held = held + wide(xb, block, there)
            zs[place, block, pl.ds(base, tile), :] = held.astype(jnp.bfloat16)

        over_rows(step)
        z_copy(place, block).start()

    def give_tp(flip, block, side, with_z):
        if with_z:
            z_copy(1, block).wait_recv()
        core_copy(flip, side).wait_recv()

        def step(base):
            here = at_side(side, base)
            held = wide(pb, flip, here) + wide(cb, flip, here)
            if with_z:
                held = held + wide(zb, 1, block, pl.ds(base, tile))
            pb[flip, here, :] = held.astype(jnp.bfloat16)

        over_rows(step)
        x_copy(flip, block, side).start()

    @scoped("collect")
    def collect(flip, hold=False):
        role = role_of(flip)
        block = (y + flip) % 2
        second = flip % 2 == 1

        @pl.when(jnp.logical_and(role == far_tp, jnp.logical_or(by_tp, second)))
        def _():
            give_tp(flip, block, 1, False)

        if not second:
            pl.when(jnp.logical_and(role == far_tp, by_pair))(
                lambda: give_pair(1, flip, block, False)
            )
            pl.when(jnp.logical_and(role == 0, by_pair))(lambda: give_pair(0, flip, block, False))
        if not hold:
            rest(flip)

    def rest(flip):
        if flip % 2 == 1:
            pl.when(role_of(flip) == far_tp)(lambda: give_tp(flip, (y + 1) % 2, 0, False))
        else:
            pl.when(jnp.logical_and(role_of(flip) == far_tp, by_pair))(
                lambda: give_tp(flip, y, 0, False)
            )

    mine = xor(z, t, n_chunks)
    theirs = xor(mine, far_tp, n_chunks)

    def second_theirs():
        with jax.named_scope("theirs"):
            pl.when(by_tp)(lambda: give_tp(2 * theirs, y % 2, 0, True))

    def second_mine():
        with jax.named_scope("mine"):
            pl.when(by_tp)(lambda: give_pair(0, 2 * mine, y % 2, True))
            give_pair(0, 2 * mine + 1, (y + 1) % 2, True)

    def down(flip):
        if not (isinstance(flip, int) and flip in (0, PAIR)):
            wait_weight("d", flip)
        shrink(flip)

    def second_relay():
        pl.when(inner)(lambda: relay("d", far[1]))

    def both(one, other):
        return jnp.logical_and(one, other)

    own_loads["d"]()
    far_foreign = t // far_tp == z // far_tp
    here_first, there_first = far

    @pl.when(jnp.logical_not(far_foreign))
    def _():
        down(0)
        pl.when(inner)(lambda: relay("d", far[0]))
        down(1)
        collect(0)
        down(PAIR)
        collect(1)
        pl.when(outer)(lambda: relay("d", far[1]))
        down(PAIR + 1)
        collect(PAIR)
        shrink(here_first)
        collect(PAIR + 1)
        down(here_first + 1)
        collect(here_first)
        second_relay()
        shrink(there_first)
        collect(here_first + 1)
        collect(there_first)

        pl.when(both(inner, by_tp))(second_mine)
        down(there_first + 1)
        collect(there_first + 1)
        pl.when(jnp.logical_or(outer, by_pair))(second_mine)
        second_theirs()

    @pl.when(both(far_foreign, inner))
    def _():
        down(0)
        relay("d", here_first)
        shrink(here_first)
        collect(0)
        down(1)
        collect(here_first)
        down(PAIR)
        collect(1)
        down(PAIR + 1)
        collect(PAIR)
        down(here_first + 1)
        collect(PAIR + 1)
        collect(here_first + 1)
        second_relay()
        shrink(there_first)
        pl.when(by_tp)(second_mine)
        collect(there_first)
        down(there_first + 1)
        collect(there_first + 1)
        pl.when(by_pair)(second_mine)
        second_theirs()

    @pl.when(both(far_foreign, outer))
    def _():
        shrink(here_first)
        down(here_first + 1)
        collect(here_first)
        down(PAIR)
        collect(here_first + 1)
        relay("d", there_first)
        down(PAIR + 1)
        collect(PAIR)
        shrink(there_first)
        down(0)
        collect(there_first, True)
        down(1)
        collect(0)
        collect(1)
        down(there_first + 1)
        collect(there_first + 1, True)
        for flip in (there_first, there_first + 1):
            rest(flip)
        collect(PAIR + 1)
        second_mine()
        second_theirs()

    out_copies = []
    for beside in range(2):
        flip, block = 2 * mine + beside, (y + beside) % 2
        with jax.named_scope("wait_z"):
            core_copy(flip, 0).wait_recv()
            z_copy(0, block).wait_recv()
        with jax.named_scope("wait_x"):
            x_copy(flip, block, 0).wait_recv()
        columns = pl.ds(pl.multiple_of(block * depth, depth), depth)

        def finish(base, flip=flip, block=block, columns=columns):
            here = pl.ds(base, tile)
            feed = wide(pb, flip, here) + wide(cb, flip, here) + wide(zb, 0, block, here)
            feed = feed + wide(xb, block, here)
            out_ref[here, columns] = (wide(mid, 0, 0, here, columns) + 0.5 * feed).astype(jnp.bfloat16)

        over_rows(finish)
        out_copies.append(local(out_ref.at[:, columns], out_hbm.at[:, columns]))
        out_copies[-1].start()

    with jax.named_scope("ends"):
        for copy in out_copies:
            copy.wait()
        for end in [*ends, *mid_ends.values()]:
            end()
        for kind in kinds:
            for flip in [1, PAIR] + far:
                drain_own(kind, flip)
            for flip in [PAIR] + far:
                drain_relay(kind, flip)
        for flip in range(n_sp):
            for side in range(2):
                pl.when(role_of(flip) % 2 == 1)(lambda: core_copy(flip, side).wait_send())
        for beside in range(2):
            flip, block = 2 * theirs + beside, (y + beside) % 2
            x_copy(flip, block, 0).wait_send()
            z_copy(0, block).wait_send()
            pl.when(jnp.logical_or(by_tp, beside == 1))(lambda: x_copy(flip, block, 1).wait_send())
            if beside == 0:
                pl.when(by_pair)(lambda: z_copy(1, block).wait_send())

    @pl.when(s + 1 < n_sp)
    def _():
        for at, ref in enumerate((k_hbm, v_hbm)):
            halo_copy(at, ref).wait_send()


def kernel_device(
    queries,
    keys,
    values,
    query_gain,
    key_gain,
    sink_logits,
    out_weight,
    residual,
    norm_gain,
    gate_weight,
    up_weight,
    down_weight,
):
    n_sp, n_tp = lax.axis_size("sp"), lax.axis_size("tp")
    rows, width = residual.shape
    depth, units = gate_weight.shape
    big, _ = split_units(units)
    heads_width = queries.shape[1]
    head_width = query_gain.shape[0]
    bf16, f32 = jnp.bfloat16, jnp.float32
    vmem = pl.BlockSpec(memory_space=pltpu.VMEM)
    smem = pl.BlockSpec(memory_space=pltpu.SMEM)
    hbm = pl.BlockSpec(memory_space=pl.ANY)
    n_links = 97
    scratch = [
        pltpu.VMEM((n_sp // 2, 2 * depth, big), bf16),
        pltpu.VMEM((n_sp // 2, 2 * depth, big), bf16),
        pltpu.VMEM((n_sp, big, depth), bf16),
        pltpu.VMEM((2, n_tp, rows, width), bf16),
        pltpu.VMEM((2, n_tp, rows, width), bf16),
        pltpu.VMEM((2 * rows, big), f32),
        pltpu.VMEM((2 * rows, big), f32),
        pltpu.VMEM((2 * rows, big), bf16),
        pltpu.VMEM((n_sp, 2 * rows, depth), bf16),
        pltpu.VMEM((n_sp, 2 * rows, depth), bf16),
        pltpu.VMEM((2, 2 * rows, depth), bf16),
        pltpu.VMEM((2, 2, rows, depth), bf16),
        pltpu.VMEM((2, 2, rows, depth), bf16),
        pltpu.VMEM((n_tp, rows, heads_width), bf16),
        pltpu.VMEM((n_tp, heads_width, width), bf16),
        pltpu.VMEM((n_tp, 1, width), f32),
        pltpu.VMEM((rows, width), bf16),
        pltpu.VMEM((rows + WINDOW, head_width), bf16),
        pltpu.VMEM((rows + WINDOW, head_width), bf16),
        pltpu.VMEM((2, head_width, WINDOW), bf16),
        pltpu.VMEM((rows, heads_width), bf16),
        pltpu.VMEM((head_width, rows), bf16),
        pltpu.VMEM((head_width, rows), bf16),
        pltpu.VMEM((rows, width), bf16),
        pltpu.SemaphoreType.DMA((n_links,)),
        pltpu.SemaphoreType.DMA((n_links,)),
        pltpu.SemaphoreType.DMA((16,)),
    ]
    return pl.pallas_call(
        functools.partial(layer_kernel, n_sp, n_tp),
        out_shape=jax.ShapeDtypeStruct((rows, width), bf16),
        in_specs=[hbm, hbm, hbm, vmem, vmem, smem, hbm, hbm, vmem, hbm, hbm, hbm],
        out_specs=hbm,
        scratch_shapes=scratch,
        compiler_params=pltpu.CompilerParams(
            collective_id=0, has_side_effects=True, vmem_limit_bytes=66 * 1000 * 1000
        ),
    )(
        queries,
        keys.T,
        values.T,
        query_gain[None],
        key_gain[None],
        sink_logits[None],
        out_weight,
        residual,
        norm_gain[None],
        gate_weight,
        up_weight,
        down_weight,
    )


def per_device(*args):
    queries, keys, query_gain, residual, gate_weight = args[0], args[1], args[3], args[7], args[9]
    n_sp, n_tp = lax.axis_size("sp"), lax.axis_size("tp")
    depth, units = gate_weight.shape
    rows, width = residual.shape
    fits = (
        depth % LANES == 0
        and units % LANES == 0
        and rows % (2 * LANES) == 0
        and width == 2 * depth
        and n_sp == 2 * n_tp
        and n_tp // 2 == PAIR
        and n_sp % (2 * PAIR) == 0
        and keys.shape[1] == query_gain.shape[0]
    )
    return kernel_device(*args) if fits else permute_device(*args)


def solution(mesh):
    in_specs = (
        P("sp", "tp"),
        P("sp", "tp"),
        P("sp", "tp"),
        P(),
        P(),
        P("tp"),
        P("tp", None),
        P("sp", "tp"),
        P("tp"),
        P("sp", "tp"),
        P("sp", "tp"),
        P("tp", "sp"),
    )
    out_specs = P("sp", "tp")
    return jax.shard_map(
        per_device, mesh=mesh, in_specs=in_specs, out_specs=out_specs, check_vma=False
    )
```

```python
import functools

import jax
import jax.numpy as jnp
from jax import lax
from jax.experimental import pallas as pl
from jax.experimental.pallas import tpu as pltpu
from jax.sharding import PartitionSpec as P

WINDOW = 128
PAIR = 2
LANES = 128
PARTS = 2
EPS = 1e-06
MESH = pl.DeviceIdType.MESH


def swap(block, axis, flip):
    return lax.ppermute(block, axis, [(i, i ^ flip) for i in range(lax.axis_size(axis))])


def from_behind(block, axis, distance):
    devices = range(lax.axis_size(axis))
    route = [(i - distance, i) for i in devices if i - distance in devices]
    return lax.ppermute(block, axis, route)


def gather_flips(block, axis):
    found = {0: block}
    flip = lax.axis_size(axis) // 2
    while flip:
        for at, held in list(found.items()):
            found[at ^ flip] = swap(held, axis, flip)
        flip //= 2
    return [found[at] for at in range(lax.axis_size(axis))]


def norm_heads(flat, gain, heads):
    row_count = flat.shape[0]
    head_width = gain.shape[0]
    data = flat.astype(jnp.float32).reshape(row_count, heads, head_width)
    scaled = data * lax.rsqrt(jnp.mean(data * data, axis=-1, keepdims=True) + 1e-06) * gain
    return scaled.astype(jnp.bfloat16)


def attend(queries, keys, values, edge, query_gain, key_gain, sink_logits):
    head_width = query_gain.shape[0]
    row_count = queries.shape[0]
    q_heads = queries.shape[1] // head_width
    k_heads = keys.shape[1] // head_width
    group_size = q_heads // k_heads
    window_len = WINDOW
    block_count = row_count // window_len
    query_norm = norm_heads(queries, query_gain, q_heads)
    key_raw = jnp.concatenate([edge[:, : keys.shape[1]], keys], axis=0)
    key_all = norm_heads(key_raw, key_gain, k_heads).reshape(key_raw.shape)
    value_all = jnp.concatenate([edge[:, keys.shape[1] :], values], axis=0)

    def windows(flat):
        return jnp.concatenate(
            [
                flat[:row_count].reshape(block_count, window_len, k_heads, head_width),
                flat[window_len:].reshape(block_count, window_len, k_heads, head_width),
            ],
            axis=1,
        )

    key_blocks, value_blocks = windows(key_all), windows(value_all)
    query_blocks = query_norm.reshape(block_count, window_len, k_heads, group_size, head_width)
    scores = jnp.einsum(
        "nqhgd,nkhd->nhgqk", query_blocks, key_blocks, preferred_element_type=jnp.float32
    ) * head_width ** (-0.5)
    query_index = jnp.arange(window_len)[:, None]
    key_index = jnp.arange(2 * window_len)[None, :]
    offset_lag = window_len + query_index - key_index
    inband = (offset_lag >= 0) & (offset_lag < window_len)
    leading = (
        (jnp.arange(block_count)[:, None, None] > 0)
        | (key_index[None] >= window_len)
        | (lax.axis_index("sp") > 0)
    )
    valid = inband[None] & leading
    scores = jnp.where(valid[:, None, None], scores, -1e30)
    sink_rows = sink_logits.reshape(k_heads, group_size)[None, :, :, None]
    row_peak = jnp.maximum(jnp.max(scores, axis=-1), sink_rows)
    exp_terms = jnp.exp(scores - row_peak[..., None])
    denom_sum = jnp.sum(exp_terms, axis=-1) + jnp.exp(sink_rows - row_peak)
    weights = (exp_terms / denom_sum[..., None]).astype(jnp.bfloat16)
    attended = jnp.einsum(
        "nhgqk,nkhd->nqhgd", weights, value_blocks, preferred_element_type=jnp.float32
    ).astype(jnp.bfloat16)
    return attended.reshape(row_count, q_heads * head_width)


def permute_device(
    queries,
    keys,
    values,
    query_gain,
    key_gain,
    sink_logits,
    out_weight,
    residual,
    norm_gain,
    gate_weight,
    up_weight,
    down_weight,
):
    n_sp, n_tp = lax.axis_size("sp"), lax.axis_size("tp")
    sp, tp = lax.axis_index("sp"), lax.axis_index("tp")
    half = (sp // PAIR) % 2
    row_count, width = residual.shape
    depth, units = gate_weight.shape
    units //= 2

    def part(array, axis, flip):
        return lax.dynamic_slice_in_dim(array, (half ^ flip) * units, units, axis)

    far = list(range(2 * PAIR, n_sp, 2))

    def send(first, second, flips):
        found = {}
        for flip in flips:
            other = (flip // PAIR) % 2
            if second is None:
                piece = part(first, 0, other)
            else:
                piece = jnp.concatenate([part(first, 1, other), part(second, 1, other)], axis=1)
            found[flip] = swap(piece, "sp", flip) if flip else piece
        return found

    def relay(found, flips):
        for flip in flips:
            found[flip ^ 1] = swap(found[flip], "sp", 1)

    edge = jnp.concatenate([keys, values], axis=1)[row_count - WINDOW :]
    edge = from_behind(edge, "sp", 1)
    gate_weight, up_weight, residual, out_weight, edge = lax.optimization_barrier(
        (gate_weight, up_weight, residual, out_weight, edge)
    )
    near = [0, PAIR]
    first = far[: len(far) // 2]
    residual_pair = swap(residual, "sp", PAIR)
    both = send(gate_weight, up_weight, first)
    both.update(send(gate_weight, up_weight, near))
    attended = attend(queries, keys, values, edge, query_gain, key_gain, sink_logits)
    attended_pair = swap(attended, "sp", PAIR)

    gate_weight, up_weight, down_weight, attended_pair = lax.optimization_barrier(
        (gate_weight, up_weight, down_weight, attended_pair)
    )
    both.update(send(gate_weight, up_weight, far[len(far) // 2 :]))
    early = {flip: both[flip] for flip in first}
    down_weight, early = lax.optimization_barrier((down_weight, early))
    both.update(early)
    down = send(down_weight, None, far)
    down.update(send(down_weight, None, near))
    relay(both, near + far)
    relay(down, near)

    gains = jnp.concatenate(gather_flips(norm_gain, "tp"))
    projections = gather_flips(out_weight, "tp")
    stream = jnp.concatenate([residual, residual_pair], axis=0)
    stream = jnp.concatenate(gather_flips(stream, "tp"), axis=1).astype(jnp.float32)
    heads = gather_flips(jnp.concatenate([attended, attended_pair], axis=0), "tp")

    def own_first(columns):
        pieces = [
            lax.dynamic_slice_in_dim(columns, (tp ^ flip) * width, width, 1)
            for flip in range(n_tp)
        ]
        return jnp.concatenate(pieces, axis=1)

    projection = jnp.concatenate([own_first(piece) for piece in projections], axis=0)
    head = jnp.concatenate(heads, axis=1)
    mixed = jnp.dot(head, projection, preferred_element_type=jnp.float32)
    middle = (stream + mixed).astype(jnp.bfloat16)
    middle = lax.optimization_barrier(middle)
    middle_wide = middle.astype(jnp.float32)
    mean = jnp.mean(middle_wide * middle_wide, axis=1, keepdims=True)
    normed = (middle_wide * lax.rsqrt(mean + 1e-06) * gains).astype(jnp.bfloat16)

    late = {flip: down[flip] for flip in far}
    normed, late = lax.optimization_barrier((normed, late))
    down.update(late)
    relay(down, far)

    per_part = width // depth

    def place(flip):
        block = sp ^ flip
        return (((block // per_part) ^ tp) * per_part + block % per_part) * depth

    flips = range(n_sp)
    normed_in = jnp.concatenate(
        [lax.dynamic_slice_in_dim(normed, place(flip), depth, 1) for flip in flips], axis=1
    )
    gate_full = jnp.concatenate([both[flip][:, :units] for flip in flips], axis=0)
    up_full = jnp.concatenate([both[flip][:, units:] for flip in flips], axis=0)
    gate_acts = jnp.dot(normed_in, gate_full, preferred_element_type=jnp.float32)
    up_acts = jnp.dot(normed_in, up_full, preferred_element_type=jnp.float32)
    hidden = (jax.nn.silu(gate_acts) * up_acts).astype(jnp.bfloat16)

    down_full = jnp.zeros((units, width * n_tp), jnp.bfloat16)
    for flip in flips:
        down_full = lax.dynamic_update_slice_in_dim(down_full, down[flip], place(flip), 1)
    terms = [
        jnp.dot(
            hidden, down_full[:, at * width : (at + 1) * width], preferred_element_type=jnp.float32
        ).astype(jnp.bfloat16)
        for at in range(n_tp)
    ]

    def add(one, other):
        return one.astype(jnp.float32) + other.astype(jnp.float32)

    flip = 1
    held = dict(enumerate(terms))
    while flip < n_tp // 2:
        held = {
            at: add(held[at], swap(held[at ^ flip], "tp", flip)).astype(jnp.bfloat16)
            for at in held
            if not at & flip
        }
        flip *= 2
    own, other = held[0], held[flip]
    cut = width // 2
    across = add(own[:, :cut], swap(other[:, :cut], "tp", flip)).astype(jnp.bfloat16)
    left = add(across[:row_count], swap(across[row_count:], "sp", PAIR))
    pair = jnp.concatenate([own[:, cut:], other[:, cut:]], axis=1)
    pair = add(pair[:row_count], swap(pair[row_count:], "sp", PAIR)).astype(jnp.bfloat16)
    right = add(pair[:, : width - cut], swap(pair[:, width - cut :], "tp", flip))
    feed = jnp.concatenate([left, right], axis=1)
    return (middle_wide[:row_count, :width] + 0.5 * feed).astype(jnp.bfloat16)


def split_units(units):
    tiles = units // LANES
    small = (tiles // 2) * LANES
    return units - small, small


def scoped(name):
    def wrap(fn):
        def run(*args, **options):
            tags = [str(arg) for arg in args if isinstance(arg, (int, str))]
            with jax.named_scope("_".join([name, *tags])):
                return fn(*args, **options)

        return run

    return wrap


class Link:
    def __init__(self, sems, index):
        self.send, self.recv = sems[0].at[index], sems[1].at[index]

    def copy(self, src, dst, device):
        return pltpu.make_async_remote_copy(
            src_ref=src,
            dst_ref=dst,
            send_sem=self.send,
            recv_sem=self.recv,
            device_id=device,
            device_id_type=MESH,
        )


def layer_kernel(
    n_sp,
    n_tp,
    q_hbm,
    k_hbm,
    v_hbm,
    qg_ref,
    kg_ref,
    sink_ref,
    ow_hbm,
    res_hbm,
    ng_ref,
    gate_hbm,
    up_hbm,
    down_hbm,
    out_hbm,
    gt,
    ut,
    dn,
    mid,
    nrm,
    acc_g,
    acc_u,
    hid,
    pb,
    cb,
    xb,
    zs,
    zb,
    att,
    ow,
    gains,
    res,
    kn,
    vn,
    kh,
    q_ref,
    k_ref,
    v_ref,
    out_ref,
    send_sems,
    recv_sems,
    local_sems,
):
    s, t = lax.axis_index("sp"), lax.axis_index("tp")
    rows, width = res_hbm.shape
    depth, units = gate_hbm.shape
    big_units, small_units = split_units(units)
    window = WINDOW
    y = s % 2
    half = (s // PAIR) % 2
    is_big = (half + t) % 2 == 0
    core, far_tp = 1, n_tp // 2
    far = list(range(2 * PAIR, n_sp, PAIR))
    inner = (half + s // far[0]) % 2 == 1
    outer = jnp.logical_not(inner)
    soon = jnp.where(inner, far[1], far[0])
    late = jnp.where(inner, far[0], far[1])

    def flip_of(index, flip):
        out, bit = index, 1
        while bit <= flip:
            if flip & bit:
                out = out + bit - 2 * bit * ((index // bit) % 2)
            bit *= 2
        return out

    def xor(one, other, size):
        out, bit = 0, 1
        while bit < size:
            a, b = (one // bit) % 2, (other // bit) % 2
            out = out + bit * ((a + b) % 2)
            bit *= 2
        return out

    def sp_dev(flip):
        return {"sp": flip_of(s, flip)}

    def tp_dev(flip):
        return {"tp": flip_of(t, flip)}

    def sized(large, fn):
        if big_units == small_units:
            fn(big_units)
        else:
            pl.when(large)(lambda: fn(big_units))
            pl.when(jnp.logical_not(large))(lambda: fn(small_units))

    counter = [0]

    def new_link():
        counter[0] += 1
        return Link((send_sems, recv_sems), counter[0] - 1)

    ends = []

    locals_used = [0]

    def local(src, dst):
        locals_used[0] += 1
        return pltpu.make_async_copy(src, dst, local_sems.at[locals_used[0] - 1])

    kinds = {"g": (gate_hbm, gt), "u": (up_hbm, ut), "d": (down_hbm, dn)}
    counter[0] = len(kinds) * n_sp * PARTS
    step_depth = depth // PARTS

    def weight_link(kind, flip, cut):
        index = ("gud".index(kind) * n_sp + flip) * PARTS + cut
        return Link((send_sems, recv_sems), index)

    def slot(kind, flip, size, cut=None, seen_y=y):
        buf = kinds[kind][1]
        first, count = (0, depth) if cut is None else (cut * step_depth, step_depth)
        if kind == "d":
            return buf.at[flip, pl.ds(0, size), pl.ds(first, count)]
        start = ((seen_y + flip) % 2) * depth + first
        return buf.at[flip // 2, pl.ds(start, count), pl.ds(0, size)]

    def origin(kind, side, size, cut=None):
        ref = kinds[kind][0]
        first, count = (0, depth) if cut is None else (cut * step_depth, step_depth)
        start = pl.multiple_of(side * (units - size), LANES)
        if kind == "d":
            return ref.at[pl.ds(start, size), pl.ds(first, count)]
        return ref.at[pl.ds(first, count), pl.ds(start, size)]

    def own_copies(kind, flip):
        other = (flip // PAIR) % 2
        side = (half + other) % 2
        large = is_big if other == 0 else jnp.logical_not(is_big)

        def make(size, cut):
            return weight_link(kind, flip, cut).copy(
                origin(kind, side, size, cut),
                slot(kind, flip, size, cut, (y + flip) % 2),
                sp_dev(flip),
            )

        return large, make

    def send_own(kind, flip):
        large, make = own_copies(kind, flip)
        for cut in range(PARTS):
            sized(large, lambda size: make(size, cut).start())

    def drain_own(kind, flip):
        large, make = own_copies(kind, flip)
        for cut in range(PARTS):
            sized(large, lambda size: make(size, cut).wait_send())

    def wait_part(kind, flip, cut):
        def wait(size):
            at = slot(kind, flip, size, cut)
            weight_link(kind, flip, cut).copy(at, at, sp_dev(1)).wait_recv()

        sized(is_big, wait)

    @scoped("wait_weight")
    def wait_weight(kind, flip):
        for cut in range(PARTS):
            wait_part(kind, flip, cut)

    def relay_copy(kind, flip, size, cut):
        return weight_link(kind, flip + 1, cut).copy(
            slot(kind, flip, size, cut), slot(kind, flip + 1, size, cut, (y + 1) % 2), sp_dev(1)
        )

    @scoped("relay")
    def relay(kind, flip):
        for cut in range(PARTS):
            wait_part(kind, flip, cut)
            sized(is_big, lambda size: relay_copy(kind, flip, size, cut).start())

    def drain_relay(kind, flip):
        for cut in range(PARTS):
            sized(is_big, lambda size: relay_copy(kind, flip, size, cut).wait_send())

    def send(link, src, dst, device):
        copy = link.copy(src, dst, device)
        copy.start()
        ends.append(copy.wait_send)

    def wait(link, at):
        link.copy(at, at, tp_dev(core)).wait_recv()

    barrier = pltpu.get_barrier_semaphore()
    sp_flips = [1, PAIR] + far
    tp_flips = list(range(1, n_tp))
    for flip in sp_flips:
        pl.semaphore_signal(barrier, inc=1, device_id=sp_dev(flip), device_id_type=MESH)
    for flip in tp_flips:
        pl.semaphore_signal(barrier, inc=1, device_id=tp_dev(flip), device_id_type=MESH)

    @pl.when(s + 1 < n_sp)
    def _():
        pl.semaphore_signal(barrier, inc=1, device_id={"sp": s + 1}, device_id_type=MESH)

    @pl.when(s > 0)
    def _():
        pl.semaphore_signal(barrier, inc=1, device_id={"sp": s - 1}, device_id_type=MESH)

    if big_units != small_units:

        @pl.when(jnp.logical_not(is_big))
        def _():
            pad = big_units - small_units
            zero = jnp.zeros((gt.shape[1], pad), jnp.bfloat16)
            for chunk in range(gt.shape[0]):
                gt[chunk, :, small_units:] = zero
                ut[chunk, :, small_units:] = zero
            for flip in range(n_sp):
                dn[flip, small_units:, :] = jnp.zeros((pad, depth), jnp.bfloat16)

    @pl.when(s == 0)
    def _():
        kh[...] = jnp.zeros_like(kh)

    qkv_loads = [local(q_hbm, q_ref), local(k_hbm, k_ref), local(v_hbm, v_ref)]
    for load in qkv_loads:
        load.start()

    greeted = len(sp_flips) + len(tp_flips)
    edges = jnp.where(s > 0, 1, 0) + jnp.where(s + 1 < n_sp, 1, 0)
    with jax.named_scope("barrier"):
        pl.semaphore_wait(barrier, greeted + edges)

    halo = [new_link(), new_link()]
    last = pl.ds(rows - window, window)

    def halo_copy(at, ref):
        return halo[at].copy(ref.at[:, last], kh.at[at], {"sp": jnp.minimum(s + 1, n_sp - 1)})

    @pl.when(s + 1 < n_sp)
    def _():
        for at, ref in enumerate((k_hbm, v_hbm)):
            halo_copy(at, ref).start()

    own_loads = {}
    for kind in kinds:

        def load(kind=kind):
            index = locals_used[0]
            locals_used[0] += 1

            def make(size):
                return pltpu.make_async_copy(
                    origin(kind, half, size), slot(kind, 0, size), local_sems.at[index]
                )

            sized(is_big, lambda size: make(size).start())
            return lambda: sized(is_big, lambda size: make(size).wait())

        own_loads[kind] = load()
    for kind in kinds:
        send_own(kind, 1)
    for kind in "gu":
        send_own(kind, PAIR)
    pl.when(outer)(lambda: send_own("d", PAIR))

    @pl.when(inner)
    def _():
        for flip in reversed(far):
            for kind in "gu":
                send_own(kind, flip)
        for flip in far:
            send_own("d", flip)

    res_load = local(res_hbm, res)
    res_load.start()
    ow_links = {flip: new_link() for flip in tp_flips}
    gain_links = {flip: new_link() for flip in tp_flips}
    for flip in tp_flips:
        start = pl.multiple_of(flip_of(t, flip) * width, LANES)
        send(ow_links[flip], ow_hbm.at[:, pl.ds(start, width)], ow.at[flip], tp_dev(flip))
        send(gain_links[flip], ng_ref, gains.at[flip], tp_dev(flip))
    ow_load = local(ow_hbm.at[:, pl.ds(pl.multiple_of(t * width, LANES), width)], ow.at[0])
    ow_load.start()
    gains[0] = ng_ref[...]

    head_width = qg_ref.shape[1]
    heads = q_ref.shape[1] // head_width
    blocks = rows // window
    scale = head_width ** (-0.5)

    def unit_norm(data, gain):
        data = data.astype(jnp.float32)
        mean = jnp.mean(data * data, axis=-1, keepdims=True)
        return (data * lax.rsqrt(mean + EPS) * gain).astype(jnp.bfloat16)

    def turn(block):
        return block.astype(jnp.float32).T

    for load in qkv_loads:
        load.wait()

    def norm_keys(at, _):
        here = pl.ds(pl.multiple_of(at * window, window), window)
        there = pl.ds(pl.multiple_of((at + 1) * window, window), window)
        kn[there, :] = unit_norm(turn(k_ref[:, here]), kg_ref[...])
        vn[there, :] = turn(v_ref[:, here]).astype(jnp.bfloat16)
        return 0

    lax.fori_loop(0, blocks, norm_keys, 0)

    def attend_block(at, _):
        here = pl.ds(pl.multiple_of(at * window, window), window)
        both = pl.ds(pl.multiple_of(at * window, window), 2 * window)
        keys, values = kn[both, :], vn[both, :]
        raw = q_ref[here, :]
        query_index = lax.broadcasted_iota(jnp.int32, (window, 2 * window), 0)
        key_index = lax.broadcasted_iota(jnp.int32, (window, 2 * window), 1)
        lag = window + query_index - key_index
        first = jnp.where(s * blocks + at > 0, 0, window)
        valid = (lag >= 0) & (lag < window) & (key_index >= first)
        pieces = []
        for head in range(heads):
            query = unit_norm(raw[:, head * head_width : (head + 1) * head_width], qg_ref[...])
            scores = lax.dot_general(
                query, keys, (((1,), (1,)), ((), ())), preferred_element_type=jnp.float32
            )
            scores = jnp.where(valid, scores * scale, -1e30)
            sink = sink_ref[0, head]
            peak = jnp.maximum(jnp.max(scores, axis=-1, keepdims=True), sink)
            terms = jnp.exp(scores - peak)
            total = jnp.sum(terms, axis=-1, keepdims=True) + jnp.exp(sink - peak)
            weights = (terms / total).astype(jnp.bfloat16)
            piece = jnp.dot(weights, values, preferred_element_type=jnp.float32)
            pieces.append(piece.astype(jnp.bfloat16))
        att[0, here, :] = jnp.concatenate(pieces, axis=1)
        return 0

    with jax.named_scope("attend"):
        lax.fori_loop(1, blocks, attend_block, 0)

    @pl.when(s > 0)
    def _():
        for at in range(2):
            halo[at].copy(kh.at[at], kh.at[at], {"sp": jnp.maximum(s - 1, 0)}).wait_recv()

    kn[0:window, :] = unit_norm(turn(kh[0]), kg_ref[...])
    vn[0:window, :] = turn(kh[1]).astype(jnp.bfloat16)
    with jax.named_scope("attend_first"):
        lax.fori_loop(0, 1, attend_block, 0)

    att_links = {flip: new_link() for flip in tp_flips}
    send(att_links[far_tp], att.at[0], att.at[far_tp], tp_dev(far_tp))
    send(att_links[core], att.at[0], att.at[core], tp_dev(core))

    with jax.named_scope("wait_att"):
        wait(att_links[far_tp], att.at[far_tp])
    send(att_links[far_tp ^ core], att.at[far_tp], att.at[far_tp ^ core], tp_dev(core))

    for flip in tp_flips:
        with jax.named_scope("wait_ow"):
            wait(ow_links[flip], ow.at[flip])
        wait(gain_links[flip], gains.at[flip])
    ow_load.wait()
    res_load.wait()
    wait(att_links[core], att.at[core])
    wait(att_links[far_tp ^ core], att.at[far_tp ^ core])

    def project(at, _):
        here = pl.ds(pl.multiple_of(at * window, window), window)
        mixed = jnp.zeros((window, width), jnp.float32)
        for flip in range(n_tp):
            product = jnp.dot(att[flip, here, :], ow[flip], preferred_element_type=jnp.float32)
            mixed = mixed + product.astype(jnp.bfloat16).astype(jnp.float32)
        mid[0, 0, here, :] = (res[here, :].astype(jnp.float32) + mixed).astype(jnp.bfloat16)
        return 0

    cuts = 2
    piece = rows // cuts
    mid_links = {
        (side, flip, cut): new_link()
        for side in range(2)
        for flip in range(n_tp)
        for cut in range(cuts)
        if side or flip
    }

    def part(side, flip, cut):
        return mid.at[side, flip, pl.ds(cut * piece, piece), :]

    mid_ends = {}

    def pass_mid(side, flip, cut, to_side, to_flip, device_of, hop):
        def make():
            return mid_links[to_side, to_flip, cut].copy(
                part(side, flip, cut), part(to_side, to_flip, cut), device_of(hop)
            )

        make().start()
        mid_ends[to_side, to_flip, cut] = lambda: make().wait_send()

    @scoped("wait_mid")
    def wait_mid(side, flip, cut):
        wait(mid_links[side, flip, cut], part(side, flip, cut))

    with jax.named_scope("project"):
        lax.fori_loop(0, blocks, project, 0)
    for cut in range(cuts):
        pass_mid(0, 0, cut, 1, 0, sp_dev, PAIR)
        pass_mid(0, 0, cut, 0, far_tp, tp_dev, far_tp)
        pass_mid(0, 0, cut, 0, core, tp_dev, core)

    norm_rows = 64

    @scoped("normalise")
    def normalise(side):
        def step(at, _):
            here = pl.ds(pl.multiple_of(at * norm_rows, norm_rows), norm_rows)
            total = jnp.zeros((norm_rows, 1), jnp.float32)
            for flip in range(n_tp):
                data = mid[side, flip, here, :].astype(jnp.float32)
                total = total + jnp.sum(data * data, axis=1, keepdims=True)
            factor = lax.rsqrt(total / (width * n_tp) + EPS)
            for flip in range(n_tp):
                data = mid[side, flip, here, :].astype(jnp.float32)
                nrm[side, flip, here, :] = (data * factor * gains[flip]).astype(jnp.bfloat16)
            return 0

        lax.fori_loop(0, rows // norm_rows, step, 0)

    pl.when(inner)(lambda: send_own("d", PAIR))

    @pl.when(outer)
    def _():
        for flip in far:
            for kind in "gu":
                send_own(kind, flip)
        for flip in far:
            send_own("d", flip)

    tile = 256
    tall = rows // 2
    wide_tile = rows // 2
    n_chunks = n_sp // 2
    z = s // 2

    @scoped("expand")
    def expand(chunk, side, first=False, flip=None, kinds="gu", last=False):
        at_slot = xor(xor(z, chunk, n_chunks), t, n_chunks)
        if flip is None:
            part = pl.ds(0, 2 * depth)
        else:
            part = pl.ds(pl.multiple_of(((y + flip) % 2) * depth, depth), depth)

        def step(at, _):
            here = pl.ds(pl.multiple_of(at * wide_tile, wide_tile), wide_tile)
            there = pl.ds(pl.multiple_of(side * rows + at * wide_tile, wide_tile), wide_tile)
            data = nrm[side, at_slot, here, part]
            for kind in kinds:
                weight, acc = (gt, acc_g) if kind == "g" else (ut, acc_u)
                acts = jnp.dot(data, weight[chunk, part, :], preferred_element_type=jnp.float32)
                if not first:
                    acts = acts + acc[there, :]
                if last:
                    gate = acc_g[there, :]
                    hid[there, :] = (gate / (1.0 + jnp.exp(-gate)) * acts).astype(jnp.bfloat16)
                else:
                    acc[there, :] = acts
            return 0

        lax.fori_loop(0, rows // wide_tile, step, 0)

    def wait_beside(flip):
        for kind in "gu":
            wait_weight(kind, flip + 1)

    def spread(cut):
        wait_mid(1, 0, cut)
        pass_mid(1, 0, cut, 1, far_tp, tp_dev, far_tp)
        pass_mid(1, 0, cut, 1, core, tp_dev, core)

    for kind in "gu":
        relay(kind, PAIR)
    for kind in "gu":
        relay(kind, soon)
    for cut in range(cuts):
        wait_mid(0, far_tp, cut)
        pass_mid(0, far_tp, cut, 0, far_tp ^ core, tp_dev, core)
    @pl.when(inner)
    def _():
        for cut in range(cuts):
            spread(cut)
        relay("d", PAIR)

    pl.when(outer)(lambda: relay("d", far[0]))
    for cut in range(cuts):
        wait_mid(0, core, cut)
        wait_mid(0, far_tp ^ core, cut)
    normalise(0)
    own_loads["g"]()
    own_loads["u"]()
    wait_beside(0)
    expand(0, 0, True)
    pl.when(outer)(lambda: spread(0))
    wait_beside(PAIR)
    expand(1, 0)
    pl.when(inner)(lambda: relay("g", late))
    pl.when(outer)(lambda: spread(1))
    wait_beside(soon)
    expand(soon // 2, 0)
    pl.when(inner)(lambda: relay("u", late))
    for cut in range(cuts):
        wait_mid(1, far_tp, cut)
        pass_mid(1, far_tp, cut, 1, far_tp ^ core, tp_dev, core)
        if cut == 0:
            pl.when(outer)(lambda: relay("g", late))
    for cut in range(cuts):
        wait_mid(1, core, cut)
        wait_mid(1, far_tp ^ core, cut)
    normalise(1)
    expand(0, 1, True)
    pl.when(outer)(lambda: relay("u", late))
    expand(1, 1)
    expand(soon // 2, 1)
    for side in range(2):
        expand(late // 2, side, flip=late)
    pl.when(outer)(lambda: relay("d", PAIR))
    wait_weight("g", late + 1)
    for side in range(2):
        expand(late // 2, side, flip=late + 1, kinds="g")
    wait_weight("u", late + 1)
    for side in range(2):
        expand(late // 2, side, flip=late + 1, kinds="u", last=True)

    core_links = counter[0]
    x_links = core_links + 2 * n_sp
    z_links = x_links + 4
    counter[0] += 2 * n_sp + 8
    by_tp = (z + t) % 2 == 0
    by_pair = jnp.logical_not(by_tp)

    def link(index):
        return Link((send_sems, recv_sems), index)

    def role_of(flip):
        return xor(xor(z, flip // 2, n_chunks), t, n_chunks)

    def side_rows(side):
        return pl.ds(side * rows, rows)

    def core_copy(flip, side):
        some = side_rows(side)
        return link(core_links + 2 * flip + side).copy(
            pb.at[flip, some, :], cb.at[flip, some, :], tp_dev(core)
        )

    def x_copy(flip, block, side):
        some = side_rows(side)
        return link(x_links + 2 * block + side).copy(
            pb.at[flip, some, :], xb.at[block, some, :], tp_dev(far_tp)
        )

    def z_copy(place, block):
        return link(z_links + 2 * place + block).copy(
            zs.at[place, block], zb.at[place, block], sp_dev(PAIR)
        )

    def over_rows(fn, size=tile):
        def step(at, _):
            fn(pl.multiple_of(at * size, size))
            return 0

        lax.fori_loop(0, rows // size, step, 0)

    def wide(ref, *index):
        return ref[index].astype(jnp.float32)

    def at_side(side, base, size=tile):
        return pl.ds(pl.multiple_of(side * rows + base, size), size)

    @scoped("shrink")
    def shrink(flip):
        for side in (1, 0):

            def step(base, side=side):
                here = at_side(side, base, tall)
                product = jnp.dot(hid[here, :], dn[flip], preferred_element_type=jnp.float32)
                pb[flip, here, :] = product.astype(jnp.bfloat16)

            step(0)
            step(tall)
            pl.when(role_of(flip) % 2 == 1)(lambda: core_copy(flip, side).start())

    def give_pair(place, flip, block, with_x):
        core_copy(flip, 1).wait_recv()
        if with_x:
            x_copy(flip, block, 1).wait_recv()

        def step(base):
            there = at_side(1, base)
            held = wide(pb, flip, there) + wide(cb, flip, there)
            if with_x:
                held = held + wide(xb, block, there)
            zs[place, block, pl.ds(base, tile), :] = held.astype(jnp.bfloat16)

        over_rows(step)
        z_copy(place, block).start()

    def give_tp(flip, block, side, with_z):
        if with_z:
            z_copy(1, block).wait_recv()
        core_copy(flip, side).wait_recv()

        def step(base):
            here = at_side(side, base)
            held = wide(pb, flip, here) + wide(cb, flip, here)
            if with_z:
                held = held + wide(zb, 1, block, pl.ds(base, tile))
            pb[flip, here, :] = held.astype(jnp.bfloat16)

        over_rows(step)
        x_copy(flip, block, side).start()

    @scoped("collect")
    def collect(flip, hold=False):
        role = role_of(flip)
        block = (y + flip) % 2
        second = flip % 2 == 1

        @pl.when(jnp.logical_and(role == far_tp, jnp.logical_or(by_tp, second)))
        def _():
            give_tp(flip, block, 1, False)

        if not second:
            pl.when(jnp.logical_and(role == far_tp, by_pair))(
                lambda: give_pair(1, flip, block, False)
            )
            pl.when(jnp.logical_and(role == 0, by_pair))(lambda: give_pair(0, flip, block, False))
        if not hold:
            rest(flip)

    def rest(flip):
        if flip % 2 == 1:
            pl.when(role_of(flip) == far_tp)(lambda: give_tp(flip, (y + 1) % 2, 0, False))
        else:
            pl.when(jnp.logical_and(role_of(flip) == far_tp, by_pair))(
                lambda: give_tp(flip, y, 0, False)
            )

    mine = xor(z, t, n_chunks)
    theirs = xor(mine, far_tp, n_chunks)

    def second_theirs():
        with jax.named_scope("theirs"):
            pl.when(by_tp)(lambda: give_tp(2 * theirs, y % 2, 0, True))

    def second_mine():
        with jax.named_scope("mine"):
            pl.when(by_tp)(lambda: give_pair(0, 2 * mine, y % 2, True))
            give_pair(0, 2 * mine + 1, (y + 1) % 2, True)

    def down(flip):
        if not (isinstance(flip, int) and flip in (0, PAIR)):
            wait_weight("d", flip)
        shrink(flip)

    def second_relay():
        pl.when(inner)(lambda: relay("d", far[1]))

    def both(one, other):
        return jnp.logical_and(one, other)

    own_loads["d"]()
    far_foreign = t // far_tp == z // far_tp
    here_first, there_first = far

    @pl.when(jnp.logical_not(far_foreign))
    def _():
        down(0)
        pl.when(inner)(lambda: relay("d", far[0]))
        down(1)
        collect(0)
        down(PAIR)
        collect(1)
        pl.when(outer)(lambda: relay("d", far[1]))
        down(PAIR + 1)
        collect(PAIR)
        shrink(here_first)
        collect(PAIR + 1)
        down(here_first + 1)
        collect(here_first)
        second_relay()
        shrink(there_first)
        collect(here_first + 1)
        collect(there_first)

        pl.when(both(inner, by_tp))(second_mine)
        down(there_first + 1)
        collect(there_first + 1)
        pl.when(jnp.logical_or(outer, by_pair))(second_mine)
        second_theirs()

    @pl.when(both(far_foreign, inner))
    def _():
        down(0)
        relay("d", here_first)
        shrink(here_first)
        collect(0)
        down(1)
        collect(here_first)
        down(PAIR)
        collect(1)
        down(PAIR + 1)
        collect(PAIR)
        down(here_first + 1)
        collect(PAIR + 1)
        collect(here_first + 1)
        second_relay()
        shrink(there_first)
        pl.when(by_tp)(second_mine)
        collect(there_first)
        down(there_first + 1)
        collect(there_first + 1)
        pl.when(by_pair)(second_mine)
        second_theirs()

    @pl.when(both(far_foreign, outer))
    def _():
        shrink(here_first)
        down(here_first + 1)
        collect(here_first)
        down(PAIR)
        collect(here_first + 1)
        relay("d", there_first)
        down(PAIR + 1)
        collect(PAIR)
        shrink(there_first)
        down(0)
        collect(there_first, True)
        down(1)
        collect(0)
        collect(1)
        down(there_first + 1)
        collect(there_first + 1, True)
        for flip in (there_first, there_first + 1):
            rest(flip)
        collect(PAIR + 1)
        second_mine()
        second_theirs()

    with jax.named_scope("drain"):
        for end in [*ends, *mid_ends.values()]:
            end()
        for kind in kinds:
            for flip in [1, PAIR] + far:
                drain_own(kind, flip)
            for flip in [PAIR] + far:
                drain_relay(kind, flip)

    out_copies = []
    for beside in range(2):
        flip, block = 2 * mine + beside, (y + beside) % 2
        with jax.named_scope("wait_z"):
            core_copy(flip, 0).wait_recv()
            z_copy(0, block).wait_recv()
        with jax.named_scope("wait_x"):
            x_copy(flip, block, 0).wait_recv()
        columns = pl.ds(pl.multiple_of(block * depth, depth), depth)

        def finish(base, flip=flip, block=block, columns=columns):
            here = pl.ds(base, tile)
            feed = wide(pb, flip, here) + wide(cb, flip, here) + wide(zb, 0, block, here)
            feed = feed + wide(xb, block, here)
            out_ref[here, columns] = (wide(mid, 0, 0, here, columns) + 0.5 * feed).astype(jnp.bfloat16)

        over_rows(finish)
        out_copies.append(local(out_ref.at[:, columns], out_hbm.at[:, columns]))
        out_copies[-1].start()

    with jax.named_scope("ends"):
        for copy in out_copies:
            copy.wait()
        for flip in range(n_sp):
            for side in range(2):
                pl.when(role_of(flip) % 2 == 1)(lambda: core_copy(flip, side).wait_send())
        for beside in range(2):
            flip, block = 2 * theirs + beside, (y + beside) % 2
            x_copy(flip, block, 0).wait_send()
            z_copy(0, block).wait_send()
            pl.when(jnp.logical_or(by_tp, beside == 1))(lambda: x_copy(flip, block, 1).wait_send())
            if beside == 0:
                pl.when(by_pair)(lambda: z_copy(1, block).wait_send())

    @pl.when(s + 1 < n_sp)
    def _():
        for at, ref in enumerate((k_hbm, v_hbm)):
            halo_copy(at, ref).wait_send()


def kernel_device(
    queries,
    keys,
    values,
    query_gain,
    key_gain,
    sink_logits,
    out_weight,
    residual,
    norm_gain,
    gate_weight,
    up_weight,
    down_weight,
):
    n_sp, n_tp = lax.axis_size("sp"), lax.axis_size("tp")
    rows, width = residual.shape
    depth, units = gate_weight.shape
    big, _ = split_units(units)
    heads_width = queries.shape[1]
    head_width = query_gain.shape[0]
    bf16, f32 = jnp.bfloat16, jnp.float32
    vmem = pl.BlockSpec(memory_space=pltpu.VMEM)
    smem = pl.BlockSpec(memory_space=pltpu.SMEM)
    hbm = pl.BlockSpec(memory_space=pl.ANY)
    n_links = 97
    scratch = [
        pltpu.VMEM((n_sp // 2, 2 * depth, big), bf16),
        pltpu.VMEM((n_sp // 2, 2 * depth, big), bf16),
        pltpu.VMEM((n_sp, big, depth), bf16),
        pltpu.VMEM((2, n_tp, rows, width), bf16),
        pltpu.VMEM((2, n_tp, rows, width), bf16),
        pltpu.VMEM((2 * rows, big), f32),
        pltpu.VMEM((2 * rows, big), f32),
        pltpu.VMEM((2 * rows, big), bf16),
        pltpu.VMEM((n_sp, 2 * rows, depth), bf16),
        pltpu.VMEM((n_sp, 2 * rows, depth), bf16),
        pltpu.VMEM((2, 2 * rows, depth), bf16),
        pltpu.VMEM((2, 2, rows, depth), bf16),
        pltpu.VMEM((2, 2, rows, depth), bf16),
        pltpu.VMEM((n_tp, rows, heads_width), bf16),
        pltpu.VMEM((n_tp, heads_width, width), bf16),
        pltpu.VMEM((n_tp, 1, width), f32),
        pltpu.VMEM((rows, width), bf16),
        pltpu.VMEM((rows + WINDOW, head_width), bf16),
        pltpu.VMEM((rows + WINDOW, head_width), bf16),
        pltpu.VMEM((2, head_width, WINDOW), bf16),
        pltpu.VMEM((rows, heads_width), bf16),
        pltpu.VMEM((head_width, rows), bf16),
        pltpu.VMEM((head_width, rows), bf16),
        pltpu.VMEM((rows, width), bf16),
        pltpu.SemaphoreType.DMA((n_links,)),
        pltpu.SemaphoreType.DMA((n_links,)),
        pltpu.SemaphoreType.DMA((16,)),
    ]
    return pl.pallas_call(
        functools.partial(layer_kernel, n_sp, n_tp),
        out_shape=jax.ShapeDtypeStruct((rows, width), bf16),
        in_specs=[hbm, hbm, hbm, vmem, vmem, smem, hbm, hbm, vmem, hbm, hbm, hbm],
        out_specs=hbm,
        scratch_shapes=scratch,
        compiler_params=pltpu.CompilerParams(
            collective_id=0, has_side_effects=True, vmem_limit_bytes=66 * 1000 * 1000
        ),
    )(
        queries,
        keys.T,
        values.T,
        query_gain[None],
        key_gain[None],
        sink_logits[None],
        out_weight,
        residual,
        norm_gain[None],
        gate_weight,
        up_weight,
        down_weight,
    )


def per_device(*args):
    queries, keys, query_gain, residual, gate_weight = args[0], args[1], args[3], args[7], args[9]
    n_sp, n_tp = lax.axis_size("sp"), lax.axis_size("tp")
    depth, units = gate_weight.shape
    rows, width = residual.shape
    fits = (
        depth % LANES == 0
        and units % LANES == 0
        and rows % (2 * LANES) == 0
        and width == 2 * depth
        and n_sp == 2 * n_tp
        and n_tp // 2 == PAIR
        and n_sp % (2 * PAIR) == 0
        and keys.shape[1] == query_gain.shape[0]
    )
    return kernel_device(*args) if fits else permute_device(*args)


def solution(mesh):
    in_specs = (
        P("sp", "tp"),
        P("sp", "tp"),
        P("sp", "tp"),
        P(),
        P(),
        P("tp"),
        P("tp", None),
        P("sp", "tp"),
        P("tp"),
        P("sp", "tp"),
        P("sp", "tp"),
        P("tp", "sp"),
    )
    out_specs = P("sp", "tp")
    return jax.shard_map(
        per_device, mesh=mesh, in_specs=in_specs, out_specs=out_specs, check_vma=False
    )
```
